32 devices in a mesh: sp: 8 (over z, y), tp: 4 (over x, core).
Axes of the slice: x: 2, y: 2, z: 4, core: 2. Of those that a mesh axis runs over, the one named last changes fastest.
Arguments:
- tokens: bfloat16 [8192, 2048], P('sp', 'tp'), may hold values from -600 to 600, as said below
- norm_gain: float32 [2048], replicated, may hold values from 0.1 to 1.9
- w_query: bfloat16 [2048, 1024], P(None, 'tp'), may hold values from -0.125 to 0.125
- w_forget_fwd: bfloat16 [2048, 1024], P(None, 'tp'), may hold values from -0.125 to 0.125
- w_forget_bwd: bfloat16 [2048, 1024], P(None, 'tp'), may hold values from -0.125 to 0.125
- w_value: bfloat16 [2048, 1024], P(None, 'tp'), may hold values from -0.125 to 0.125
- w_gate: bfloat16 [2048, 1024], P(None, 'tp'), may hold values from -0.125 to 0.125
- w_pool_in: bfloat16 [2048, 1024], P(None, 'tp'), may hold values from -0.125 to 0.125
- forget_gap: float32 [2, 1024], P(None, 'tp'), may hold values from 0 to 0.06
- added_log_retention: float32 [8192, 8], P('sp', 'tp'), may hold values from -2.1 to 0
- initial_state: float32 [2, 8, 128, 128], P(None, 'tp'), may hold values from -0.18 to 0.18
- head_gain: float32 [1024], P('tp'), may hold values from 0.1 to 1.9
- pool_mix: bfloat16 [4, 256, 256], P('tp'), may hold values from -0.375 to 0.375
- pool_gain: float32 [1024], P('tp'), may hold values from 0.1 to 1.9
- w_out_recur: bfloat16 [1024, 2048], P('tp'), may hold values from -0.125 to 0.125
- w_out_pool: bfloat16 [1024, 2048], P('tp'), may hold values from -0.125 to 0.125
Outputs:
- mixed_out: bfloat16 [8192, 2048], P(('sp', 'tp'))
The draws below stay inside these ranges and needn't reach their ends.
Inputs may be any that keep to these rules, and one draw needn't show every extreme that they name: `tokens`: layer input with scales that differ between rows and between columns.
All inputs are finite; a program needn't handle non-finite values.
Results may differ from the reference program's by a relative error of at most 0.013.
Values may be sent and summed in bfloat16 or wider, within the bound.
A program may use at most 128 MiB of HBM per device.

```python
import jax
import jax.numpy as jnp
from jax import lax

D = 2048
HEADS = 8
HEAD_DIM = 128
EXPAND = 128
POOL_GROUPS = 4
POOL_GROUP = 256
BLOCK = 64
TOK_DEV = 1024
SEQ = 8192
HG_WIDTH = 1024
KDIM = 1024
POOL_WIDTH = 1024
N_TP = 4


def draw_tokens(key, part):
    first, second, third = jax.random.split(key, 3)
    base = jnp.clip(jax.random.normal(first, (SEQ, D), jnp.float32), -6.0, 6.0)
    row_scale = 10.0 ** jax.random.uniform(second, (SEQ, 1), jnp.float32, 0.0, 1.0)
    rising = jnp.arange(D, dtype=jnp.float32) / D
    column_scale = 10.0 ** (0.8 * rising + jax.random.uniform(third, (1, D), jnp.float32, 0.0, 0.2))
    return (base * row_scale * column_scale).astype(jnp.bfloat16)


def draw_forget_gap(key, part):
    pick_key, fast_key, slow_key = jax.random.split(key, 3)
    share = 0.5
    fast_heads = jax.random.uniform(pick_key, (2, HEADS, 1), jnp.float32) < share
    fast_gap = jax.random.uniform(fast_key, (2, HEADS, EXPAND), jnp.float32, 0.02, 0.06)
    lowest = jnp.log(jnp.float32(0.3 / SEQ))
    highest = jnp.log(jnp.float32(min(30.0 / SEQ, 0.06)))
    slow_gap = jnp.exp(jax.random.uniform(slow_key, (2, HEADS, EXPAND), jnp.float32, lowest, highest))
    return jnp.where(fast_heads, fast_gap, slow_gap).reshape(2, HEADS * EXPAND)


def draw_added_log_retention(key, part):
    level_key, where_key, size_key = jax.random.split(key, 3)
    span = max(TOK_DEV // 4, 1)
    pieces = SEQ // span
    lowest = jnp.log(jnp.float32(0.1 / SEQ))
    highest = jnp.log(jnp.float32(1.0 / SEQ))
    level = jnp.exp(jax.random.uniform(level_key, (pieces, 1, HEADS), jnp.float32, lowest, highest))
    backdrop_term = -jnp.broadcast_to(level, (pieces, span, HEADS)).reshape(SEQ, HEADS)
    spots = jax.random.randint(where_key, (3, HEADS), 0, SEQ)
    layer_depth = jax.random.uniform(size_key, (3, HEADS), jnp.float32, 0.22, 0.69)
    location_list = jnp.arange(SEQ, dtype=jnp.int32)[:, None, None] == spots[None, :, :]
    token_groups = -jnp.sum(jnp.where(location_list, layer_depth[None, :, :], 0.0), axis=1)
    return backdrop_term + token_groups


def steps_of(rng, shape, cuts, low, largest):
    loudness = 1.0
    for dim, parts in cuts:
        heights = jax.random.uniform(jax.random.fold_in(jax.random.fold_in(rng, 6), dim), (parts,), jnp.float32, low / len(cuts), largest / len(cuts))
        loudness = loudness * jnp.repeat(jnp.exp(heights), shape[dim] // parts).reshape((-1,) + (1,) * (len(shape) - 1 - dim))
    return loudness


def normal_values(rng, dims, deviation, most, shards=(), kind=jnp.bfloat16):
    factor_of = steps_of(rng, dims, shards, -0.22, 0.18) if shards else 1.0
    values = jax.random.normal(rng, dims, jnp.float32) * deviation * factor_of
    return jnp.minimum(jnp.maximum(values, -most), most).astype(kind)


def setup_inputs(seed: int = 0) -> dict:
    streams_of = jax.random.split(jax.random.key(seed), 17)
    return {
        "tokens": draw_tokens(jax.random.fold_in(streams_of[16], 71), 0),
        "norm_gain": jnp.clip(1.0 + 0.18 * jax.random.normal(streams_of[1], (D,), jnp.float32), 0.1, 1.9),
        "w_query": normal_values(streams_of[2], (D, KDIM), D ** -0.5, 0.125, ((1, 4),)),
        "w_forget_fwd": normal_values(streams_of[3], (D, KDIM), D ** -0.5, 0.125, ((1, 4),)),
        "w_forget_bwd": normal_values(streams_of[4], (D, KDIM), D ** -0.5, 0.125, ((1, 4),)),
        "w_value": normal_values(streams_of[5], (D, HG_WIDTH), D ** -0.5, 0.125, ((1, 4),)),
        "w_gate": normal_values(streams_of[6], (D, HG_WIDTH), D ** -0.5, 0.125, ((1, 4),)),
        "w_pool_in": normal_values(streams_of[7], (D, POOL_WIDTH), D ** -0.5, 0.125, ((1, 4),)),
        "forget_gap": draw_forget_gap(jax.random.fold_in(streams_of[16], 71), 0),
        "added_log_retention": draw_added_log_retention(jax.random.fold_in(streams_of[16], 71), 0),
        "initial_state": normal_values(streams_of[10], (2, HEADS, EXPAND, HEAD_DIM), 0.03, 0.18, ((1, 4),), jnp.float32),
        "head_gain": jnp.clip(1.0 + 0.18 * jax.random.normal(streams_of[11], (HG_WIDTH,), jnp.float32), 0.1, 1.9),
        "pool_mix": normal_values(streams_of[12], (POOL_GROUPS, POOL_GROUP, POOL_GROUP), POOL_GROUP ** -0.5, 0.375, ((0, 4),)),
        "pool_gain": jnp.clip(1.0 + 0.18 * jax.random.normal(streams_of[13], (POOL_WIDTH,), jnp.float32), 0.1, 1.9),
        "w_out_recur": normal_values(streams_of[14], (HG_WIDTH, D), (HG_WIDTH + POOL_WIDTH) ** -0.5, 0.125, ((0, 4),)),
        "w_out_pool": normal_values(streams_of[15], (POOL_WIDTH, D), (HG_WIDTH + POOL_WIDTH) ** -0.5, 0.125, ((0, 4),)),
    }


EPSILON = 1e-06
FULL_ACCURACY = lax.Precision.HIGHEST

def project(normed, scale, weight):
    return (jnp.dot(normed, weight, preferred_element_type=jnp.float32) * scale).astype(jnp.bfloat16)

def recurrence(query, block_entry, values, log_keep, start):
    length, heads, layer_depth = query.shape
    count = length // BLOCK

    def split(array):
        return array.reshape(count, BLOCK, heads, array.shape[2]).transpose(0, 2, 1, 3)
    lower = jnp.tril(jnp.ones((BLOCK, BLOCK), jnp.float32))

    def advance(hidden_state, inputs):
        query_block, entry_block, value_tile_rows, keep_block = inputs
        running = jnp.cumsum(keep_block, axis=1)
        query_retention = query_block * jnp.exp(running)
        entry_decay = entry_block * jnp.exp(-running)
        scores = jnp.einsum('hck,hsk->hcs', query_retention, entry_decay, precision=FULL_ACCURACY) * lower
        final_output = jnp.einsum('hcs,hsv->hcv', scores, value_tile_rows, precision=FULL_ACCURACY)
        final_output = final_output + jnp.einsum('rbl,rlm->rbm', query_retention, hidden_state, precision=FULL_ACCURACY)
        closing_value = running[:, -1:, :]
        final_block_entry = entry_block * jnp.exp(closing_value - running)
        hidden_state = jnp.exp(closing_value[:, 0, :, None]) * hidden_state + jnp.einsum('xnw,xnz->xwz', final_block_entry, value_tile_rows, precision=FULL_ACCURACY)
        return (hidden_state, final_output)
    hidden_state, final_output = lax.scan(advance, start, (split(query), split(block_entry), split(values), split(log_keep)))
    return final_output.transpose(0, 2, 1, 3).reshape(length, heads, values.shape[2])

def reference(tokens, norm_gain, w_query, w_forget_fwd, w_forget_bwd, w_value, w_gate, w_pool_in, forget_gap, added_log_retention, initial_state, head_gain, pool_mix, pool_gain, w_out_recur, w_out_pool):
    widened = tokens.astype(jnp.float32)
    scale = lax.rsqrt(lax.optimization_barrier(jnp.mean(widened * widened, axis=1, keepdims=True)) + EPSILON)
    normed = (widened * norm_gain).astype(jnp.bfloat16)
    query_pre = project(normed, scale, w_query)
    forget_fwd = project(normed, scale, w_forget_fwd)
    forget_bwd = project(normed, scale, w_forget_bwd)
    value_proj = project(normed, scale, w_value)
    gate_pre = project(normed, scale, w_gate)
    pool_in = project(normed, scale, w_pool_in)

    def split_heads(array, width):
        return array.astype(jnp.float32).reshape(SEQ, HEADS, width)
    query = jax.nn.silu(split_heads(query_pre, EXPAND))
    values = split_heads(value_proj, HEAD_DIM)
    token_group = added_log_retention[:, :, None]

    def gates(pre, gap):
        block_entry = gap.reshape(HEADS, EXPAND) * jax.nn.sigmoid(-split_heads(pre, EXPAND))
        return (block_entry, jnp.log1p(-block_entry) + token_group)
    entry_fwd, keep_fwd = gates(forget_fwd, forget_gap[0])
    entry_bwd, keep_bwd = gates(forget_bwd, forget_gap[1])
    out_fwd = recurrence(query, entry_fwd, values, keep_fwd, initial_state[0])
    output_backward = jnp.flip(recurrence(jnp.flip(query, 0), jnp.flip(entry_bwd, 0), jnp.flip(values, 0), jnp.flip(keep_bwd, 0), initial_state[1]), 0)
    both = out_fwd + output_backward
    both = both * lax.rsqrt(lax.optimization_barrier(jnp.mean(both * both, axis=2, keepdims=True)) + EPSILON)
    recur = (both.reshape(SEQ, HG_WIDTH) * head_gain * jax.nn.sigmoid(gate_pre.astype(jnp.float32))).astype(jnp.bfloat16)
    positions = jnp.arange(SEQ, dtype=jnp.int32)
    pooled = []
    for group in range(POOL_GROUPS):
        window = 2 ** (group + 1)
        current = pool_in[:, group * POOL_GROUP:(group + 1) * POOL_GROUP].astype(jnp.float32)
        sums = jnp.concatenate([jnp.zeros((1, POOL_GROUP), jnp.float32), jnp.cumsum(current, axis=0)], axis=0)
        low = jnp.clip(positions - window // 2, 0, SEQ)
        high = jnp.clip(positions - window // 2 + window, 0, SEQ)
        window_mean = (sums[high] - sums[low]) / (high - low).astype(jnp.float32)[:, None]
        diff = (window_mean - current).astype(jnp.bfloat16)
        pooled.append(jnp.dot(diff, pool_mix[group], preferred_element_type=jnp.float32))
    pool_out = (jnp.concatenate(pooled, axis=1) * pool_gain).astype(jnp.bfloat16)
    recur_share = HG_WIDTH // N_TP
    pool_share = POOL_WIDTH // N_TP
    total = jnp.zeros((SEQ, D), jnp.float32)
    for rank in range(N_TP):
        partial_sum = jnp.dot(recur[:, rank * recur_share:(rank + 1) * recur_share], w_out_recur[rank * recur_share:(rank + 1) * recur_share], preferred_element_type=jnp.float32)
        partial_sum = partial_sum + jnp.dot(pool_out[:, rank * pool_share:(rank + 1) * pool_share], w_out_pool[rank * pool_share:(rank + 1) * pool_share], preferred_element_type=jnp.float32)
        rounded = lax.optimization_barrier(partial_sum.astype(jnp.bfloat16))
        total = total + rounded.astype(jnp.float32)
    return total.astype(jnp.bfloat16)
```

```python
import functools

import jax
import jax.numpy as jnp
from jax import lax
from jax.experimental import pallas as pl
from jax.experimental.pallas import tpu as pltpu
from jax.sharding import PartitionSpec as P

DEPTH = 128
CHUNK = 128
EPSILON = 1e-06
RIM = 16
RING = 8
MESH = pl.DeviceIdType.MESH
F32 = jnp.float32
BF16 = jnp.bfloat16
VMEM_LIMIT = 62 * 1024 * 1024
ANY = pl.BlockSpec(memory_space=pl.ANY)
VM = pl.BlockSpec(memory_space=pltpu.VMEM)
EXACT = lax.Precision.HIGHEST


def dot(a, b, precision=None):
    return jnp.dot(a, b, preferred_element_type=F32, precision=precision)


def dot_t(a, b, precision=None):
    return lax.dot_general(
        a, b, (((1,), (1,)), ((), ())), preferred_element_type=F32, precision=precision
    )


def t_dot(a, b):
    return lax.dot_general(a, b, (((0,), (0,)), ((), ())), preferred_element_type=F32)


def peers():
    me = lax.axis_index("tp")
    sibling = me + 1 - 2 * lax.rem(me, 2)
    across = lax.rem(me + 2, 4)
    return me, sibling, across, lax.rem(sibling + 2, 4)


def strides():
    count = lax.axis_size("sp")
    return [1 << k for k in range(count.bit_length()) if 1 << k < count]


def partner(d, stride):
    me, count = lax.axis_index("sp"), lax.axis_size("sp")
    above, below = me + stride < count, me >= stride
    return (above, me + stride, below) if d == 0 else (below, me - stride, above)


def ring_size():
    return min(RING, lax.axis_size("sp"))


def ring_place():
    size = ring_size()
    me = lax.axis_index("sp")
    base, mine = me - lax.rem(me, size), lax.rem(me, size)
    place = jnp.where(lax.rem(mine, 2) == 0, mine // 2, size - 1 - mine // 2)

    def index(spot):
        spot = lax.rem(spot + size, size)
        return base + jnp.where(spot < size // 2, 2 * spot, 2 * (size - 1 - spot) + 1)

    return place, index(place + 1), index(place - 1)


def greet():
    barrier = pltpu.get_barrier_semaphore()
    _, sibling, across, opposite = peers()
    _, right, left = ring_place()
    for device in (sibling, across, opposite):
        pl.semaphore_signal(barrier, inc=1, device_id={"tp": device}, device_id_type=MESH)
    for device in (right, left):
        pl.semaphore_signal(barrier, inc=1, device_id={"sp": device}, device_id_type=MESH)
    number = jnp.int32(5)
    for stride in strides():
        for d in range(2):
            exists, target, _ = partner(d, stride)

            @pl.when(exists)
            def _():
                pl.semaphore_signal(
                    barrier, inc=1, device_id={"sp": target}, device_id_type=MESH
                )

            number = number + jnp.where(exists, 1, 0)
    pl.semaphore_wait(barrier, number)


def edge_copy(d, length, padded, e_send, e_recv):
    _, target, _ = partner(d, 1)
    begin, there = (length, 0) if d == 0 else (RIM, RIM + length)
    return pltpu.make_async_remote_copy(
        padded.at[pl.ds(begin, RIM)], padded.at[pl.ds(there, RIM)], e_send.at[d], e_recv.at[d],
        device_id={"sp": target}, device_id_type=MESH,
    )


def edge_start(d, length, padded, e_send, e_recv):
    exists, _, _ = partner(d, 1)

    @pl.when(exists)
    def _():
        edge_copy(d, length, padded, e_send, e_recv).start()


def edges_wait(length, padded, e_send, e_recv):
    for d in range(2):
        _, _, source = partner(d, 1)

        @pl.when(source)
        def _():
            edge_copy(d, length, padded, e_send, e_recv).wait_recv()


def scan_copy(k, d, stride, sent, landed, p_send, p_recv):
    _, target, _ = partner(d, stride)
    return pltpu.make_async_remote_copy(
        sent.at[k, d], landed.at[k, d], p_send.at[k, d], p_recv.at[k, d],
        device_id={"sp": target}, device_id_type=MESH,
    )


def scan_start(k, d, state, offset, sent, landed, before, before_keep, p_send, p_recv):
    stride, heads = strides()[k], state.shape[1]
    exists, _, _ = partner(d, stride)

    @pl.when(exists)
    def _():
        for h in range(heads):
            lanes = slice(h * DEPTH, (h + 1) * DEPTH)
            keep = jnp.exp(offset[d, :, lanes])
            sent[k, d, h, :DEPTH, :] = (keep * before[d, h] + state[d, h]).astype(BF16)
            sent[k, d, h, DEPTH:, :] = jnp.broadcast_to(
                keep * before_keep[d, :, lanes], (16, DEPTH)
            ).astype(BF16)
        scan_copy(k, d, stride, sent, landed, p_send, p_recv).start()


def scan_close(k, d, state, sent, landed, before, before_keep, p_send, p_recv):
    stride, heads = strides()[k], state.shape[1]
    _, _, source = partner(d, stride)

    @pl.when(source)
    def _():
        scan_copy(k, d, stride, sent, landed, p_send, p_recv).wait_recv()
        for h in range(heads):
            lanes = slice(h * DEPTH, (h + 1) * DEPTH)
            keep = before_keep[d, :, lanes]
            early = landed[k, d, h].astype(F32)
            before[d, h] = keep * early[:DEPTH] + before[d, h]
            before_keep[d, :, lanes] = keep * early[DEPTH : DEPTH + 1]


def mixer_kernel(groups, *refs):
    (h_tokens, h_gain, *h_weights) = refs[:8]
    (h_gap, h_added, h_initial, h_head, h_mix, h_scale, h_recur, h_pool) = refs[8:16]
    out = refs[16]
    (
        held, gain, wide, gap, added, initial, head_gain, mix, pool_gain, wfull,
        acc, square, cols, rows_of, turned, query_pre, value, gated, ent, runs, inner, reach,
        starts, offsets, chunk_state, chunk_keep, state, offset, padded,
        sent, landed, before, before_keep, given, taken, passed, brought, total,
        l_sem, s_sem, x_send, x_recv, f_send, f_recv, w_sem, b_sem, r_sem,
        rr_send, rr_recv, rl_send, rl_recv, p_send, p_recv, e_send, e_recv,
        a_send, a_recv, c_send, c_recv,
    ) = refs[17:]
    me, sibling, across, opposite = peers()
    length, width = held.shape[1:]
    columns = wide.shape[2]
    heads = columns // DEPTH
    count = length // CHUNK
    share = length // 4
    subs = share // CHUNK
    features = 4 * width
    depth = wfull.shape[1] // 2
    steps = len(strides())

    own_w = [
        pltpu.make_async_copy(h_recur, wfull.at[me, pl.ds(0, depth)], l_sem.at[0]),
        pltpu.make_async_copy(h_pool, wfull.at[me, pl.ds(depth, depth)], l_sem.at[1]),
    ]
    own_t = pltpu.make_async_copy(h_tokens, held.at[me], l_sem.at[2])
    small = [
        pltpu.make_async_copy(a, b, l_sem.at[3 + i])
        for i, (a, b) in enumerate((
            (h_gain, gain), (h_gap, gap), (h_added, added), (h_initial, initial),
            (h_head, head_gain), (h_mix, mix), (h_scale, pool_gain),
        ))
    ]
    loads = [
        pltpu.make_async_copy(w, wide.at[i], l_sem.at[10 + i]) for i, w in enumerate(h_weights)
    ]
    for copy in own_w + [own_t] + small + loads:
        copy.start()
    greet()

    size = ring_size()
    slab = 2 * depth // size
    half = slab // 2
    place, right, left = ring_place()
    rights, lefts = 2 * (size // 2), 2 * (size - 1 - size // 2)

    mine = pl.ds(pl.multiple_of(place * slab, slab), slab)
    w_across = pltpu.make_async_remote_copy(
        wfull.at[me, mine], wfull.at[me, mine], w_sem.at[0], w_sem.at[1],
        device_id={"tp": across}, device_id_type=MESH,
    )
    w_beside = pltpu.make_async_remote_copy(
        wfull.at[me], wfull.at[me], b_sem.at[0], b_sem.at[1],
        device_id={"tp": sibling}, device_id_type=MESH,
    )
    w_relay = pltpu.make_async_remote_copy(
        wfull.at[across], wfull.at[across], r_sem.at[0], r_sem.at[1],
        device_id={"tp": sibling}, device_id_type=MESH,
    )

    def ring_right(e):
        spot = lax.rem(place - e // 2 + size, size)
        at = pl.ds(pl.multiple_of(spot * slab + lax.rem(e, 2) * half, half), half)
        return pltpu.make_async_remote_copy(
            wfull.at[across, at], wfull.at[across, at], rr_send.at[e], rr_recv.at[e],
            device_id={"sp": right}, device_id_type=MESH,
        )

    def ring_left(e):
        spot = lax.rem(place + e // 2, size)
        at = pl.ds(pl.multiple_of(spot * slab + lax.rem(e, 2) * half, half), half)
        return pltpu.make_async_remote_copy(
            wfull.at[across, at], wfull.at[across, at], rl_send.at[e], rl_recv.at[e],
            device_id={"sp": left}, device_id_type=MESH,
        )

    def ring_turn(e):
        @pl.when(e < rights)
        def _():
            ring_right(e).wait_recv()

        @pl.when(e + 2 < rights)
        def _():
            ring_right(e + 2).start()

        @pl.when(e < lefts)
        def _():
            ring_left(e).wait_recv()

        @pl.when(e + 2 < lefts)
        def _():
            ring_left(e + 2).start()

    beside = pltpu.make_async_remote_copy(
        held.at[me], held.at[me], s_sem.at[0], s_sem.at[1],
        device_id={"tp": sibling}, device_id_type=MESH,
    )

    def piece(i):
        return pl.ds(pl.multiple_of(i * CHUNK, CHUNK), CHUNK)

    def crossing(i):
        return pltpu.make_async_remote_copy(
            held.at[me, piece(i)], held.at[me, piece(i)], x_send.at[i], x_recv.at[i],
            device_id={"tp": across}, device_id_type=MESH,
        )

    def relay(i):
        return pltpu.make_async_remote_copy(
            held.at[across, piece(i)], held.at[across, piece(i)], f_send.at[i], f_recv.at[i],
            device_id={"tp": sibling}, device_id_type=MESH,
        )

    for copy in own_w:
        copy.wait()
    w_across.start()
    own_t.wait()
    beside.start()
    for i in range(count):
        crossing(i).start()
    w_beside.start()
    for copy in small:
        copy.wait()

    row = lax.broadcasted_iota(jnp.int32, (CHUNK, CHUNK), 0)
    col = lax.broadcasted_iota(jnp.int32, (CHUNK, CHUNK), 1)
    lower, upper = row >= col, row <= col
    lower_f, upper_f = lower.astype(F32), upper.astype(F32)
    lower_2 = jnp.concatenate([lower_f, lower_f], axis=1).astype(BF16)
    upper_2 = jnp.concatenate([upper_f, upper_f], axis=1).astype(BF16)

    def sums(c, _):
        add = added[:, piece(c)]
        cols[0, c] = dot_t(lower_f, add, EXACT)
        cols[1, c] = dot_t(upper_f, add, EXACT)
        rows_of[0, c] = dot(add, upper_f, EXACT)
        rows_of[1, c] = dot(add, lower_f, EXACT)
        return 0

    lax.fori_loop(0, count, sums, 0)
    for h in range(heads):
        for d in range(2):
            turned[h, :, d * DEPTH : (d + 1) * DEPTH] = initial[d, h].T
    state[...] = jnp.zeros_like(state)
    offset[...] = jnp.zeros_like(offset)
    before[...] = jnp.zeros_like(before)
    before_keep[...] = jnp.ones_like(before_keep)
    for d in range(2):
        _, _, source = partner(d, 1)
        begin = 0 if d == 0 else RIM + length

        @pl.when(jnp.logical_not(source))
        def _():
            padded[pl.ds(begin, RIM), :] = jnp.zeros((RIM, columns), BF16)

    pair = me // 2
    near, far = 2 * pair, 2 - 2 * pair

    def normed(first, at):
        parts, squares = [], 0.0
        for o in range(2):
            x = held[first + o, at, :].astype(F32)
            squares = squares + jnp.sum(x * x, axis=1, keepdims=True)
            lanes = pl.ds(pl.multiple_of((first + o) * width, width), width)
            parts.append((x * gain[:, lanes]).astype(BF16))
        return jnp.concatenate(parts, axis=1), squares

    def depth_of(first):
        return pl.ds(pl.multiple_of(first * width, 2 * width), 2 * width)

    for copy in loads:
        copy.wait()
    beside.wait_recv()

    def own(i, _):
        at = pl.ds(pl.multiple_of(i * share, share), share)
        x, squares = normed(near, at)
        square[at, :] = squares
        for j in range(6):
            acc[j, at, :] = dot(x, wide[j, depth_of(near), :])
        return 0

    lax.fori_loop(0, 4, own, 0)
    w_across.wait_recv()
    for e in range(2):
        ring_right(e).start()
        ring_left(e).start()

    def gates(pre, gap_row, sums):
        enter = gap_row * (1.0 / (1.0 + jnp.exp(pre)))
        keep = jnp.log1p(-enter)
        high = keep.astype(BF16)
        low = (keep - high.astype(F32)).astype(BF16)
        return enter, dot(sums, jnp.concatenate([high, low], axis=0))

    def local(c):
        at = piece(c)
        x = query_pre[at, :].astype(F32)
        query = x / (1.0 + jnp.exp(-x))
        q_f, q_b = query * jnp.exp(runs[0, at, :]), query * jnp.exp(runs[1, at, :])
        e_f, e_b = ent[0, at, :], ent[1, at, :]
        values = value[at, :]
        col_f, col_b = cols[0, c], cols[1, c]
        row_f, row_b = rows_of[0, c], rows_of[1, c]
        for h in range(heads):
            lanes = slice(h * DEPTH, (h + 1) * DEPTH)
            a_col, b_col = col_f[:, h : h + 1], col_b[:, h : h + 1]
            fade = jnp.exp(
                jnp.where(lower, a_col - row_f[h : h + 1, :], b_col - row_b[h : h + 1, :])
            )
            w_f = dot_t(q_f[:, lanes].astype(BF16), e_f[:, lanes])
            w_b = dot_t(q_b[:, lanes].astype(BF16), e_b[:, lanes])
            weight = (jnp.where(lower, w_f, 0.0) + jnp.where(upper, w_b, 0.0)) * fade
            inner[at, lanes] = dot(weight.astype(BF16), values[:, lanes])
            reach[h, at, :DEPTH] = (q_f[:, lanes] * jnp.exp(a_col)).astype(BF16)
            reach[h, at, DEPTH:] = (q_b[:, lanes] * jnp.exp(b_col)).astype(BF16)

    def step(i, _):
        at = piece(i)
        crossing(i).wait_recv()
        relay(i).start()

        @pl.when(i > 0)
        def _():
            ring_turn(i - 1)
            local(i - 1)

        relay(i).wait_recv()
        x, squares = normed(far, at)
        scale = lax.rsqrt((square[at, :] + squares) / features + EPSILON)

        def project(j):
            return ((acc[j, at, :] + dot(x, wide[j, depth_of(far), :])) * scale).astype(BF16)

        pre_f, pre_b, values = project(1), project(2), project(3)
        padded[pl.ds(pl.multiple_of(i * CHUNK + RIM, RIM), CHUNK), :] = project(5)

        @pl.when(i == 0)
        def _():
            edge_start(1, length, padded, e_send, e_recv)

        @pl.when(i == count - 1)
        def _():
            edge_start(0, length, padded, e_send, e_recv)

        value[at, :] = values
        enter_f, run_f = gates(pre_f.astype(F32), gap[0:1, :], lower_2)
        enter_b, run_b = gates(pre_b.astype(F32), gap[1:2, :], upper_2)
        runs[0, at, :], runs[1, at, :] = run_f, run_b
        e_f, e_b = enter_f * jnp.exp(-run_f), enter_b * jnp.exp(-run_b)
        ent[0, at, :], ent[1, at, :] = e_f.astype(BF16), e_b.astype(BF16)
        close_f, close_b = run_f[CHUNK - 1 : CHUNK, :], run_b[0:1, :]
        last_f, last_b = e_f * jnp.exp(close_f), e_b * jnp.exp(close_b)
        offsets[0, i] = offset[0]
        col_f, col_b = cols[0, i], cols[1, i]
        for h in range(heads):
            lanes = slice(h * DEPTH, (h + 1) * DEPTH)
            a_col, b_col = col_f[:, h : h + 1], col_b[:, h : h + 1]
            a_end, b_end = a_col[CHUNK - 1 : CHUNK, :], b_col[0:1, :]
            total_f = close_f[:, lanes] + a_end
            ends_f = (last_f[:, lanes] * jnp.exp(a_end - a_col)).astype(BF16)
            ends_b = (last_b[:, lanes] * jnp.exp(b_end - b_col)).astype(BF16)
            ends = t_dot(values[:, lanes], jnp.concatenate([ends_f, ends_b], axis=1))
            starts[i, h, :, :DEPTH] = state[0, h]
            state[0, h] = jnp.exp(total_f) * state[0, h] + ends[:, :DEPTH]
            chunk_state[i, h] = ends[:, DEPTH:]
            chunk_keep[i, :, lanes] = close_b[:, lanes] + b_end
            offset[0, :, lanes] = offset[0, :, lanes] + total_f
        query_pre[at, :] = project(0)
        gate = project(4).astype(F32)
        gated[at, :] = head_gain[...] / (1.0 + jnp.exp(-gate))
        return 0

    lax.fori_loop(0, count, step, 0)

    def descend(i, _):
        c = count - 1 - i
        offsets[1, c] = offset[1]
        for h in range(heads):
            lanes = slice(h * DEPTH, (h + 1) * DEPTH)
            starts[c, h, :, DEPTH:] = state[1, h]
            keep = chunk_keep[c, :, lanes]
            state[1, h] = jnp.exp(keep) * state[1, h] + chunk_state[c, h]
            offset[1, :, lanes] = offset[1, :, lanes] + keep
        return 0

    window = jnp.left_shift(jnp.int32(2), lax.axis_index("tp") * groups)
    sequence, first_row = length * lax.axis_size("sp"), lax.axis_index("sp") * length

    def pooled(owner):
        begin = pl.multiple_of(owner * share, share)
        span = share + 2 * RIM
        near_rows = padded[pl.ds(begin, span), :]
        target = first_row + begin + lax.broadcasted_iota(jnp.int32, (share, span), 0)
        source = first_row + begin - RIM + lax.broadcasted_iota(jnp.int32, (share, span), 1)
        low = target - window // 2
        inside = (source >= low) & (source < low + window) & (source >= 0) & (source < sequence)
        start = first_row + begin + lax.broadcasted_iota(jnp.int32, (share, 1), 0) - window // 2
        number = jnp.minimum(start + window, sequence) - jnp.maximum(start, 0)
        mean = dot(inside.astype(F32).astype(BF16), near_rows) / number.astype(F32)
        here = padded[pl.ds(pl.multiple_of(begin + RIM, RIM), share), :].astype(F32)
        return (dot((mean - here).astype(BF16), mix[0]) * pool_gain[...]).astype(BF16)

    others = (across, opposite, sibling)

    def pool_copy(k):
        return pltpu.make_async_remote_copy(
            passed.at[k], brought.at[me], a_send.at[k], a_recv.at[k],
            device_id={"tp": others[k]}, device_id_type=MESH,
        )

    def pool_away(k):
        passed[k] = pooled(others[k])
        pool_copy(k).start()

    def pool_home():
        brought[me] = pooled(me)

    def pool_first():
        edges_wait(length, padded, e_send, e_recv)
        pool_away(0)

    def ring_end():
        for e in range(count - 1, max(rights, lefts)):
            ring_turn(e)
        w_relay.start()

    scan = (sent, landed, before, before_keep, p_send, p_recv)
    fillers = [
        lambda: local(count - 1), pool_first, lambda: pool_away(1), ring_end,
        lambda: pool_away(2), pool_home,
    ]
    if steps:
        scan_start(0, 0, state, offset, *scan)
    lax.fori_loop(0, count, descend, 0)
    for k in range(steps):
        for d in range(2):
            if k or d:
                scan_start(k, d, state, offset, *scan)
        for filler in fillers[k * len(fillers) // steps : (k + 1) * len(fillers) // steps]:
            filler()
        for d in range(2):
            scan_close(k, d, state, *scan)
    if not steps:
        for filler in fillers:
            filler()
    for h in range(heads):
        for d in range(2):
            lanes = slice(d * DEPTH, (d + 1) * DEPTH)
            keep = before_keep[d, :, h * DEPTH : (h + 1) * DEPTH]
            turned[h, :, lanes] = keep * turned[h, :, lanes] + before[d, h]

    def finished(c):
        at = piece(c)
        for h in range(heads):
            lanes = slice(h * DEPTH, (h + 1) * DEPTH)
            ages = jnp.exp(
                jnp.concatenate([offsets[0, c, :, lanes], offsets[1, c, :, lanes]], axis=1)
            )
            enter = (starts[c, h] + ages * turned[h]).astype(BF16)
            both = inner[at, lanes] + dot_t(reach[h, at, :], enter)
            both = both * lax.rsqrt(jnp.mean(both * both, axis=1, keepdims=True) + EPSILON)
            yield lanes, (both * gated[at, lanes]).astype(BF16)

    def recur_copy(t):
        outward = t < 2 * subs
        there = jnp.where(outward, jnp.where(lax.rem(t, 2) == 0, across, opposite), sibling)
        sub = jnp.where(outward, t // 2, t - 2 * subs)
        at = piece(there * subs + sub)
        return there * subs + sub, pltpu.make_async_remote_copy(
            given.at[at], taken.at[me, piece(sub)], c_send.at[t], c_recv.at[t],
            device_id={"tp": there}, device_id_type=MESH,
        )

    def away(t, _):
        c, copy = recur_copy(t)
        for lanes, value_of in finished(c):
            given[piece(c), lanes] = value_of
        copy.start()
        return 0

    lax.fori_loop(0, 3 * subs, away, 0)

    def home(s, _):
        for lanes, value_of in finished(me * subs + s):
            taken[me, piece(s), lanes] = value_of
        return 0

    lax.fori_loop(0, subs, home, 0)

    tile = 512
    tiles = out.shape[1] // tile
    w_beside.wait_recv()
    w_relay.wait_recv()
    for k in range(3):
        pool_copy(k).wait_recv()
    for t in range(2 * subs, 3 * subs):
        recur_copy(jnp.int32(t))[1].wait_recv()

    def wide_part(j, _):
        lanes = pl.ds(pl.multiple_of(j * tile, tile), tile)
        y = dot(taken[me], wfull[me, :depth, lanes])
        y = y + dot(taken[sibling], wfull[sibling, :depth, lanes])
        for r in range(4):
            y = y + dot(brought[r], wfull[r, depth:, lanes])
        total[:, lanes] = y
        return 0

    lax.fori_loop(0, tiles, wide_part, 0)
    for s in range(subs):
        recur_copy(jnp.int32(2 * s))[1].wait_recv()
        recur_copy(jnp.int32(2 * s + 1))[1].wait_recv()
        at = slice(s * CHUNK, (s + 1) * CHUNK)
        for j in range(tiles):
            lanes = slice(j * tile, (j + 1) * tile)
            y = total[at, lanes] + dot(taken[across, at, :], wfull[across, :depth, lanes])
            y = y + dot(taken[opposite, at, :], wfull[opposite, :depth, lanes])
            out[at, lanes] = y.astype(BF16)

    w_across.wait_send()
    beside.wait_send()
    w_beside.wait_send()
    w_relay.wait_send()

    def sent_pieces(i, _):
        crossing(i).wait_send()
        relay(i).wait_send()
        return 0

    lax.fori_loop(0, count, sent_pieces, 0)
    for e in range(rights):
        ring_right(e).wait_send()
    for e in range(lefts):
        ring_left(e).wait_send()
    for d in range(2):
        exists, _, _ = partner(d, 1)

        @pl.when(exists)
        def _():
            edge_copy(d, length, padded, e_send, e_recv).wait_send()

    for k in range(steps):
        for d in range(2):
            exists, _, _ = partner(d, strides()[k])

            @pl.when(exists)
            def _():
                scan_copy(k, d, strides()[k], sent, landed, p_send, p_recv).wait_send()

    for k in range(3):
        pool_copy(k).wait_send()
    for t in range(3 * subs):
        recur_copy(jnp.int32(t))[1].wait_send()


def shards(
    tokens, norm_gain, w_query, w_forget_fwd, w_forget_bwd, w_value, w_gate, w_pool_in,
    forget_gap, added_log_retention, initial_state, head_gain, pool_mix, pool_gain,
    w_out_recur, w_out_pool,
):
    weights = (w_query, w_forget_fwd, w_forget_bwd, w_value, w_gate, w_pool_in)
    length, width = tokens.shape
    features, columns = w_query.shape
    heads = columns // DEPTH
    count = length // CHUNK
    share = length // 4
    subs = share // CHUNK
    depth, out_width = w_out_recur.shape
    steps = len(strides())
    size = ring_size()
    rights, lefts = 2 * (size // 2), 2 * (size - 1 - size // 2)
    dma = pltpu.SemaphoreType.DMA
    operands = (
        tokens, norm_gain[None, :], *weights, forget_gap, added_log_retention.T, initial_state,
        head_gain[None, :], pool_mix, pool_gain[None, :], w_out_recur, w_out_pool,
    )

    def like(array):
        return pltpu.VMEM(array.shape, array.dtype)

    return pl.pallas_call(
        functools.partial(mixer_kernel, pool_mix.shape[0]),
        out_shape=jax.ShapeDtypeStruct((share, out_width), BF16),
        in_specs=[ANY] * len(operands),
        out_specs=VM,
        scratch_shapes=[
            pltpu.VMEM((4, length, width), BF16),
            like(operands[1]),
            pltpu.VMEM((6, features, columns), BF16),
            like(operands[8]), like(operands[9]), like(operands[10]), like(operands[11]),
            like(operands[12]), like(operands[13]),
            pltpu.VMEM((4, 2 * depth, out_width), BF16),
            pltpu.VMEM((6, length, columns), F32),
            pltpu.VMEM((length, 1), F32),
            pltpu.VMEM((2, count, CHUNK, heads), F32),
            pltpu.VMEM((2, count, heads, CHUNK), F32),
            pltpu.VMEM((heads, DEPTH, 2 * DEPTH), F32),
            pltpu.VMEM((length, columns), BF16),
            pltpu.VMEM((length, columns), BF16),
            pltpu.VMEM((length, columns), F32),
            pltpu.VMEM((2, length, columns), BF16),
            pltpu.VMEM((2, length, columns), F32),
            pltpu.VMEM((length, columns), F32),
            pltpu.VMEM((heads, length, 2 * DEPTH), BF16),
            pltpu.VMEM((count, heads, DEPTH, 2 * DEPTH), F32),
            pltpu.VMEM((2, count, 1, columns), F32),
            pltpu.VMEM((count, heads, DEPTH, DEPTH), F32),
            pltpu.VMEM((count, 1, columns), F32),
            pltpu.VMEM((2, heads, DEPTH, DEPTH), F32),
            pltpu.VMEM((2, 1, columns), F32),
            pltpu.VMEM((length + 2 * RIM, columns), BF16),
            pltpu.VMEM((steps, 2, heads, DEPTH + 16, DEPTH), BF16),
            pltpu.VMEM((steps, 2, heads, DEPTH + 16, DEPTH), BF16),
            pltpu.VMEM((2, heads, DEPTH, DEPTH), F32),
            pltpu.VMEM((2, 1, columns), F32),
            pltpu.VMEM((length, columns), BF16),
            pltpu.VMEM((4, share, columns), BF16),
            pltpu.VMEM((3, share, columns), BF16),
            pltpu.VMEM((4, share, columns), BF16),
            pltpu.VMEM((share, out_width), F32),
            dma((16,)), dma((2,)), dma((count,)), dma((count,)), dma((count,)), dma((count,)),
            dma((2,)), dma((2,)), dma((2,)),
            dma((rights,)), dma((rights,)), dma((lefts,)), dma((lefts,)),
            dma((steps, 2)), dma((steps, 2)), dma((2,)), dma((2,)),
            dma((3,)), dma((3,)), dma((3 * subs,)), dma((3 * subs,)),
        ],
        compiler_params=pltpu.CompilerParams(
            collective_id=0, has_side_effects=True, vmem_limit_bytes=VMEM_LIMIT
        ),
        name="mixer",
    )(*operands)


def solution(mesh):
    in_specs = (
        P("sp", "tp"), P(), P(None, "tp"), P(None, "tp"), P(None, "tp"), P(None, "tp"),
        P(None, "tp"), P(None, "tp"), P(None, "tp"), P("sp", "tp"), P(None, "tp", None, None),
        P("tp"), P("tp", None, None), P("tp"), P("tp", None), P("tp", None),
    )
    out_specs = P(("sp", "tp"), None)
    return jax.shard_map(shards, mesh=mesh, in_specs=in_specs, out_specs=out_specs, check_vma=False)
```

```python
import functools

import jax
import jax.numpy as jnp
from jax import lax
from jax.experimental import pallas as pl
from jax.experimental.pallas import tpu as pltpu
from jax.sharding import PartitionSpec as P

DEPTH = 128
CHUNK = 128
EPSILON = 1e-06
RIM = 16
RING = 8
MESH = pl.DeviceIdType.MESH
F32 = jnp.float32
BF16 = jnp.bfloat16
VMEM_LIMIT = 62 * 1024 * 1024
ANY = pl.BlockSpec(memory_space=pl.ANY)
VM = pl.BlockSpec(memory_space=pltpu.VMEM)
EXACT = lax.Precision.HIGHEST


def dot(a, b, precision=None):
    return jnp.dot(a, b, preferred_element_type=F32, precision=precision)


def dot_t(a, b, precision=None):
    return lax.dot_general(
        a, b, (((1,), (1,)), ((), ())), preferred_element_type=F32, precision=precision
    )


def t_dot(a, b):
    return lax.dot_general(a, b, (((0,), (0,)), ((), ())), preferred_element_type=F32)


def peers():
    me = lax.axis_index("tp")
    sibling = me + 1 - 2 * lax.rem(me, 2)
    across = lax.rem(me + 2, 4)
    return me, sibling, across, lax.rem(sibling + 2, 4)


def strides():
    count = lax.axis_size("sp")
    return [1 << k for k in range(count.bit_length()) if 1 << k < count]


def partner(d, stride):
    me, count = lax.axis_index("sp"), lax.axis_size("sp")
    above, below = me + stride < count, me >= stride
    return (above, me + stride, below) if d == 0 else (below, me - stride, above)


def ring_size():
    return min(RING, lax.axis_size("sp"))


def ring_place():
    size = ring_size()
    me = lax.axis_index("sp")
    base, mine = me - lax.rem(me, size), lax.rem(me, size)
    place = jnp.where(lax.rem(mine, 2) == 0, mine // 2, size - 1 - mine // 2)

    def index(spot):
        spot = lax.rem(spot + size, size)
        return base + jnp.where(spot < size // 2, 2 * spot, 2 * (size - 1 - spot) + 1)

    return place, index(place + 1), index(place - 1)


def greet():
    barrier = pltpu.get_barrier_semaphore()
    _, sibling, across, opposite = peers()
    _, right, left = ring_place()
    for device in (sibling, across, opposite):
        pl.semaphore_signal(barrier, inc=1, device_id={"tp": device}, device_id_type=MESH)
    for device in (right, left):
        pl.semaphore_signal(barrier, inc=1, device_id={"sp": device}, device_id_type=MESH)
    number = jnp.int32(5)
    for stride in strides():
        for d in range(2):
            exists, target, _ = partner(d, stride)

            @pl.when(exists)
            def _():
                pl.semaphore_signal(
                    barrier, inc=1, device_id={"sp": target}, device_id_type=MESH
                )

            number = number + jnp.where(exists, 1, 0)
    pl.semaphore_wait(barrier, number)


def edge_copy(d, length, padded, e_send, e_recv):
    _, target, _ = partner(d, 1)
    begin, there = (length, 0) if d == 0 else (RIM, RIM + length)
    return pltpu.make_async_remote_copy(
        padded.at[pl.ds(begin, RIM)], padded.at[pl.ds(there, RIM)], e_send.at[d], e_recv.at[d],
        device_id={"sp": target}, device_id_type=MESH,
    )


def edge_start(d, length, padded, e_send, e_recv):
    exists, _, _ = partner(d, 1)

    @pl.when(exists)
    def _():
        edge_copy(d, length, padded, e_send, e_recv).start()


def edges_wait(length, padded, e_send, e_recv):
    for d in range(2):
        _, _, source = partner(d, 1)

        @pl.when(source)
        def _():
            edge_copy(d, length, padded, e_send, e_recv).wait_recv()


def scan_copy(k, d, h, sent, landed, p_send, p_recv):
    _, target, _ = partner(d, strides()[k])
    return pltpu.make_async_remote_copy(
        sent.at[k, d, h], landed.at[k, d, h], p_send.at[k, d, h], p_recv.at[k, d, h],
        device_id={"sp": target}, device_id_type=MESH,
    )


def scan_start(k, d, h, state, offset, sent, landed, before, before_keep, p_send, p_recv):
    exists, _, _ = partner(d, strides()[k])

    @pl.when(exists)
    def _():
        lanes = slice(h * DEPTH, (h + 1) * DEPTH)
        keep = jnp.exp(offset[d, :, lanes])
        sent[k, d, h, :DEPTH, :] = (keep * before[d, h] + state[d, h]).astype(BF16)
        sent[k, d, h, DEPTH:, :] = jnp.broadcast_to(
            keep * before_keep[d, :, lanes], (16, DEPTH)
        ).astype(BF16)
        scan_copy(k, d, h, sent, landed, p_send, p_recv).start()


def scan_close(k, d, h, sent, landed, before, before_keep, p_send, p_recv):
    _, _, source = partner(d, strides()[k])

    @pl.when(source)
    def _():
        scan_copy(k, d, h, sent, landed, p_send, p_recv).wait_recv()
        lanes = slice(h * DEPTH, (h + 1) * DEPTH)
        keep = before_keep[d, :, lanes]
        early = landed[k, d, h].astype(F32)
        before[d, h] = keep * early[:DEPTH] + before[d, h]
        before_keep[d, :, lanes] = keep * early[DEPTH : DEPTH + 1]


def mixer_kernel(groups, *refs):
    (h_tokens, h_gain, *h_weights) = refs[:8]
    (h_gap, h_added, h_initial, h_head, h_mix, h_scale, h_recur, h_pool) = refs[8:16]
    out = refs[16]
    (
        held, gain, wide, gap, added, initial, head_gain, mix, pool_gain, wfull,
        acc, square, cols, rows_of, turned, query_pre, value, gated, ent, runs, inner, reach,
        starts, offsets, chunk_state, chunk_keep, state, offset, padded,
        sent, landed, before, before_keep, given, taken, passed, brought, total, kept_x, kept_scale,
        l_sem, s_sem, x_send, x_recv, f_send, f_recv, w_sem, b_sem, r_sem,
        rr_send, rr_recv, rl_send, rl_recv, p_send, p_recv, e_send, e_recv,
        a_send, a_recv, c_send, c_recv,
    ) = refs[17:]
    me, sibling, across, opposite = peers()
    length, width = held.shape[1:]
    columns = wide.shape[2]
    heads = columns // DEPTH
    count = length // CHUNK
    share = length // 4
    subs = share // CHUNK
    features = 4 * width
    depth = wfull.shape[1] // 2
    steps = len(strides())

    own_w = [
        pltpu.make_async_copy(h_recur, wfull.at[me, pl.ds(0, depth)], l_sem.at[0]),
        pltpu.make_async_copy(h_pool, wfull.at[me, pl.ds(depth, depth)], l_sem.at[1]),
    ]
    own_t = pltpu.make_async_copy(h_tokens, held.at[me], l_sem.at[2])
    small = [
        pltpu.make_async_copy(a, b, l_sem.at[3 + i])
        for i, (a, b) in enumerate((
            (h_gain, gain), (h_gap, gap), (h_added, added), (h_initial, initial),
            (h_head, head_gain), (h_mix, mix), (h_scale, pool_gain),
        ))
    ]
    loads = [
        pltpu.make_async_copy(w, wide.at[i], l_sem.at[10 + i]) for i, w in enumerate(h_weights)
    ]
    for copy in own_w + [own_t] + small + loads:
        copy.start()
    greet()

    size = ring_size()
    slab = 2 * depth // size
    half = slab // 2
    place, right, left = ring_place()
    rights, lefts = 2 * (size // 2), 2 * (size - 1 - size // 2)

    mine = pl.ds(pl.multiple_of(place * slab, slab), slab)
    w_across = pltpu.make_async_remote_copy(
        wfull.at[me, mine], wfull.at[me, mine], w_sem.at[0], w_sem.at[1],
        device_id={"tp": across}, device_id_type=MESH,
    )
    w_beside = pltpu.make_async_remote_copy(
        wfull.at[me], wfull.at[me], b_sem.at[0], b_sem.at[1],
        device_id={"tp": sibling}, device_id_type=MESH,
    )
    w_relay = pltpu.make_async_remote_copy(
        wfull.at[across], wfull.at[across], r_sem.at[0], r_sem.at[1],
        device_id={"tp": sibling}, device_id_type=MESH,
    )

    def ring_right(e):
        spot = lax.rem(place - e // 2 + size, size)
        at = pl.ds(pl.multiple_of(spot * slab + lax.rem(e, 2) * half, half), half)
        return pltpu.make_async_remote_copy(
            wfull.at[across, at], wfull.at[across, at], rr_send.at[e], rr_recv.at[e],
            device_id={"sp": right}, device_id_type=MESH,
        )

    def ring_left(e):
        spot = lax.rem(place + e // 2, size)
        at = pl.ds(pl.multiple_of(spot * slab + lax.rem(e, 2) * half, half), half)
        return pltpu.make_async_remote_copy(
            wfull.at[across, at], wfull.at[across, at], rl_send.at[e], rl_recv.at[e],
            device_id={"sp": left}, device_id_type=MESH,
        )

    def ring_turn(e):
        @pl.when(e < rights)
        def _():
            ring_right(e).wait_recv()

        @pl.when(e + 2 < rights)
        def _():
            ring_right(e + 2).start()

        @pl.when(e < lefts)
        def _():
            ring_left(e).wait_recv()

        @pl.when(e + 2 < lefts)
        def _():
            ring_left(e + 2).start()

    beside = pltpu.make_async_remote_copy(
        held.at[me], held.at[me], s_sem.at[0], s_sem.at[1],
        device_id={"tp": sibling}, device_id_type=MESH,
    )

    def piece(i):
        return pl.ds(pl.multiple_of(i * CHUNK, CHUNK), CHUNK)

    def crossing(i):
        return pltpu.make_async_remote_copy(
            held.at[me, piece(i)], held.at[me, piece(i)], x_send.at[i], x_recv.at[i],
            device_id={"tp": across}, device_id_type=MESH,
        )

    def relay(i):
        return pltpu.make_async_remote_copy(
            held.at[across, piece(i)], held.at[across, piece(i)], f_send.at[i], f_recv.at[i],
            device_id={"tp": sibling}, device_id_type=MESH,
        )

    for copy in own_w:
        copy.wait()
    w_across.start()
    own_t.wait()
    beside.start()
    for i in range(count):
        crossing(i).start()
    w_beside.start()
    for copy in small:
        copy.wait()

    row = lax.broadcasted_iota(jnp.int32, (CHUNK, CHUNK), 0)
    col = lax.broadcasted_iota(jnp.int32, (CHUNK, CHUNK), 1)
    lower, upper = row >= col, row <= col
    lower_f, upper_f = lower.astype(F32), upper.astype(F32)
    lower_2 = jnp.concatenate([lower_f, lower_f], axis=1).astype(BF16)
    upper_2 = jnp.concatenate([upper_f, upper_f], axis=1).astype(BF16)

    def sums(c, _):
        add = added[:, piece(c)]
        cols[0, c] = dot_t(lower_f, add, EXACT)
        cols[1, c] = dot_t(upper_f, add, EXACT)
        rows_of[0, c] = dot(add, upper_f, EXACT)
        rows_of[1, c] = dot(add, lower_f, EXACT)
        return 0

    lax.fori_loop(0, count, sums, 0)
    for h in range(heads):
        for d in range(2):
            turned[h, :, d * DEPTH : (d + 1) * DEPTH] = initial[d, h].T
    state[...] = jnp.zeros_like(state)
    offset[...] = jnp.zeros_like(offset)
    before[...] = jnp.zeros_like(before)
    before_keep[...] = jnp.ones_like(before_keep)
    for d in range(2):
        _, _, source = partner(d, 1)
        begin = 0 if d == 0 else RIM + length

        @pl.when(jnp.logical_not(source))
        def _():
            padded[pl.ds(begin, RIM), :] = jnp.zeros((RIM, columns), BF16)

    pair = me // 2
    near, far = 2 * pair, 2 - 2 * pair

    def normed(first, at):
        parts, squares = [], 0.0
        for o in range(2):
            x = held[first + o, at, :].astype(F32)
            squares = squares + jnp.sum(x * x, axis=1, keepdims=True)
            lanes = pl.ds(pl.multiple_of((first + o) * width, width), width)
            parts.append((x * gain[:, lanes]).astype(BF16))
        return jnp.concatenate(parts, axis=1), squares

    def depth_of(first):
        return pl.ds(pl.multiple_of(first * width, 2 * width), 2 * width)

    for copy in loads:
        copy.wait()
    beside.wait_recv()

    def own(i, _):
        at = pl.ds(pl.multiple_of(i * share, share), share)
        x, squares = normed(near, at)
        square[at, :] = squares
        for j in range(6):
            acc[j, at, :] = dot(x, wide[j, depth_of(near), :])
        return 0

    lax.fori_loop(0, 4, own, 0)
    w_across.wait_recv()
    for e in range(2):
        ring_right(e).start()
        ring_left(e).start()

    def gates(pre, gap_row, sums):
        enter = gap_row * (1.0 / (1.0 + jnp.exp(pre)))
        keep = jnp.log1p(-enter)
        high = keep.astype(BF16)
        low = (keep - high.astype(F32)).astype(BF16)
        return enter, dot(sums, jnp.concatenate([high, low], axis=0))

    def local(c):
        at = piece(c)
        x = query_pre[at, :].astype(F32)
        query = x / (1.0 + jnp.exp(-x))
        q_f, q_b = query * jnp.exp(runs[0, at, :]), query * jnp.exp(runs[1, at, :])
        e_f, e_b = ent[0, at, :], ent[1, at, :]
        values = value[at, :]
        col_f, col_b = cols[0, c], cols[1, c]
        row_f, row_b = rows_of[0, c], rows_of[1, c]
        for h in range(heads):
            lanes = slice(h * DEPTH, (h + 1) * DEPTH)
            a_col, b_col = col_f[:, h : h + 1], col_b[:, h : h + 1]
            fade = jnp.exp(
                jnp.where(lower, a_col - row_f[h : h + 1, :], b_col - row_b[h : h + 1, :])
            )
            w_f = dot_t(q_f[:, lanes].astype(BF16), e_f[:, lanes])
            w_b = dot_t(q_b[:, lanes].astype(BF16), e_b[:, lanes])
            weight = (jnp.where(lower, w_f, 0.0) + jnp.where(upper, w_b, 0.0)) * fade
            inner[at, lanes] = dot(weight.astype(BF16), values[:, lanes])
            reach[h, at, :DEPTH] = (q_f[:, lanes] * jnp.exp(a_col)).astype(BF16)
            reach[h, at, DEPTH:] = (q_b[:, lanes] * jnp.exp(b_col)).astype(BF16)

    def project(j, x, scale, at):
        return ((acc[j, at, :] + dot(x, wide[j, depth_of(far), :])) * scale).astype(BF16)

    def late(c):
        at, x, scale = piece(c), kept_x[...], kept_scale[...]
        padded[pl.ds(pl.multiple_of(c * CHUNK + RIM, RIM), CHUNK), :] = project(5, x, scale, at)
        query_pre[at, :] = project(0, x, scale, at)
        gate = project(4, x, scale, at).astype(F32)
        gated[at, :] = head_gain[...] / (1.0 + jnp.exp(-gate))

    def step(i, _):
        at = piece(i)
        crossing(i).wait_recv()
        relay(i).start()

        @pl.when(i > 0)
        def _():
            ring_turn(i - 1)
            late(i - 1)
            local(i - 1)

        @pl.when(i == 1)
        def _():
            edge_start(1, length, padded, e_send, e_recv)

        relay(i).wait_recv()
        x, squares = normed(far, at)
        scale = lax.rsqrt((square[at, :] + squares) / features + EPSILON)

        kept_x[...], kept_scale[...] = x, scale
        pre_f, pre_b, values = (project(j, x, scale, at) for j in (1, 2, 3))
        value[at, :] = values
        enter_f, run_f = gates(pre_f.astype(F32), gap[0:1, :], lower_2)
        enter_b, run_b = gates(pre_b.astype(F32), gap[1:2, :], upper_2)
        runs[0, at, :], runs[1, at, :] = run_f, run_b
        e_f, e_b = enter_f * jnp.exp(-run_f), enter_b * jnp.exp(-run_b)
        ent[0, at, :], ent[1, at, :] = e_f.astype(BF16), e_b.astype(BF16)
        close_f, close_b = run_f[CHUNK - 1 : CHUNK, :], run_b[0:1, :]
        last_f, last_b = e_f * jnp.exp(close_f), e_b * jnp.exp(close_b)
        offsets[0, i] = offset[0]
        col_f, col_b = cols[0, i], cols[1, i]
        for h in range(heads):
            lanes = slice(h * DEPTH, (h + 1) * DEPTH)
            a_col, b_col = col_f[:, h : h + 1], col_b[:, h : h + 1]
            a_end, b_end = a_col[CHUNK - 1 : CHUNK, :], b_col[0:1, :]
            total_f = close_f[:, lanes] + a_end
            ends_f = (last_f[:, lanes] * jnp.exp(a_end - a_col)).astype(BF16)
            ends_b = (last_b[:, lanes] * jnp.exp(b_end - b_col)).astype(BF16)
            ends = t_dot(values[:, lanes], jnp.concatenate([ends_f, ends_b], axis=1))
            starts[i, h, :, :DEPTH] = state[0, h]
            state[0, h] = jnp.exp(total_f) * state[0, h] + ends[:, :DEPTH]
            chunk_state[i, h] = ends[:, DEPTH:]
            chunk_keep[i, :, lanes] = close_b[:, lanes] + b_end
            offset[0, :, lanes] = offset[0, :, lanes] + total_f
        return 0

    lax.fori_loop(0, count, step, 0)

    def descend(i, _):
        c = count - 1 - i
        offsets[1, c] = offset[1]
        for h in range(heads):
            lanes = slice(h * DEPTH, (h + 1) * DEPTH)
            starts[c, h, :, DEPTH:] = state[1, h]
            keep = chunk_keep[c, :, lanes]
            state[1, h] = jnp.exp(keep) * state[1, h] + chunk_state[c, h]
            offset[1, :, lanes] = offset[1, :, lanes] + keep
        return 0

    window = jnp.left_shift(jnp.int32(2), lax.axis_index("tp") * groups)
    sequence, first_row = length * lax.axis_size("sp"), lax.axis_index("sp") * length

    def pooled(owner):
        begin = pl.multiple_of(owner * share, share)
        span = share + 2 * RIM
        near_rows = padded[pl.ds(begin, span), :]
        target = first_row + begin + lax.broadcasted_iota(jnp.int32, (share, span), 0)
        source = first_row + begin - RIM + lax.broadcasted_iota(jnp.int32, (share, span), 1)
        low = target - window // 2
        inside = (source >= low) & (source < low + window) & (source >= 0) & (source < sequence)
        start = first_row + begin + lax.broadcasted_iota(jnp.int32, (share, 1), 0) - window // 2
        number = jnp.minimum(start + window, sequence) - jnp.maximum(start, 0)
        mean = dot(inside.astype(F32).astype(BF16), near_rows) / number.astype(F32)
        here = padded[pl.ds(pl.multiple_of(begin + RIM, RIM), share), :].astype(F32)
        return (dot((mean - here).astype(BF16), mix[0]) * pool_gain[...]).astype(BF16)

    others = (across, opposite, sibling)

    def pool_copy(k):
        return pltpu.make_async_remote_copy(
            passed.at[k], brought.at[me], a_send.at[k], a_recv.at[k],
            device_id={"tp": others[k]}, device_id_type=MESH,
        )

    def pool_away(k):
        passed[k] = pooled(others[k])
        pool_copy(k).start()

    def pool_home():
        brought[me] = pooled(me)

    def pool_first():
        edges_wait(length, padded, e_send, e_recv)
        pool_away(0)

    def ring_end():
        for e in range(count - 1, max(rights, lefts)):
            ring_turn(e)
        w_relay.start()

    def late_last():
        late(count - 1)
        edge_start(0, length, padded, e_send, e_recv)
        local(count - 1)

    def finished(c, h):
        at, lanes = piece(c), slice(h * DEPTH, (h + 1) * DEPTH)
        ages = jnp.exp(jnp.concatenate([offsets[0, c, :, lanes], offsets[1, c, :, lanes]], axis=1))
        enter = (starts[c, h] + ages * turned[h]).astype(BF16)
        both = inner[at, lanes] + dot_t(reach[h, at, :], enter)
        both = both * lax.rsqrt(jnp.mean(both * both, axis=1, keepdims=True) + EPSILON)
        given[h, at, :] = (both * gated[at, lanes]).astype(BF16)

    def owner_of(k):
        return jnp.where(k < 2, jnp.where(k == 0, across, opposite), jnp.where(k == 2, sibling, me))

    def recur_copy(k, h):
        there = owner_of(k)
        at = pl.ds(pl.multiple_of(there * share, share), share)
        return pltpu.make_async_remote_copy(
            given.at[h, at], taken.at[me, h], c_send.at[h, k], c_recv.at[h, k],
            device_id={"tp": there}, device_id_type=MESH,
        )

    def finish(h):
        for d in range(2):
            lanes = slice(d * DEPTH, (d + 1) * DEPTH)
            keep = before_keep[d, :, h * DEPTH : (h + 1) * DEPTH]
            turned[h, :, lanes] = keep * turned[h, :, lanes] + before[d, h]

        def away(k, _):
            for sub in range(subs):
                finished(owner_of(k) * subs + sub, h)

            @pl.when(k < 3)
            def _():
                recur_copy(k, h).start()

            return 0

        lax.fori_loop(0, 4, away, 0)

    scan = (sent, landed, before, before_keep, p_send, p_recv)
    fillers = [late_last, pool_first, lambda: pool_away(1), ring_end, lambda: pool_away(2), pool_home]
    lax.fori_loop(0, count, descend, 0)
    for k in range(steps):
        for h in range(heads):
            for d in range(2):
                if k:
                    scan_close(k - 1, d, h, *scan)
                scan_start(k, d, h, state, offset, *scan)
        for filler in fillers[k * len(fillers) // steps : (k + 1) * len(fillers) // steps]:
            filler()
    if not steps:
        for filler in fillers:
            filler()
    for h in range(heads):
        for d in range(2):
            if steps:
                scan_close(steps - 1, d, h, *scan)
        finish(h)

    tile = 512
    tiles = out.shape[1] // tile
    w_beside.wait_recv()
    w_relay.wait_recv()
    for k in range(3):
        pool_copy(k).wait_recv()
    home = pl.ds(pl.multiple_of(me * share, share), share)

    def wide_pool(j, _):
        lanes = pl.ds(pl.multiple_of(j * tile, tile), tile)
        y = dot(brought[0], wfull[0, depth:, lanes])
        for r in range(1, 4):
            y = y + dot(brought[r], wfull[r, depth:, lanes])
        total[:, lanes] = y
        return 0

    lax.fori_loop(0, tiles, wide_pool, 0)
    for h in range(heads):
        recur_copy(2, h).wait_recv()
        if h < heads - 1:
            recur_copy(0, h).wait_recv()
            recur_copy(1, h).wait_recv()

    def wide_part(j, _):
        lanes = pl.ds(pl.multiple_of(j * tile, tile), tile)
        y = total[:, lanes]
        here = jnp.concatenate([given[h, home, :] for h in range(heads)], axis=1)
        y = y + dot(here, wfull[me, :depth, lanes])
        here = jnp.concatenate([taken[sibling, h] for h in range(heads)], axis=1)
        y = y + dot(here, wfull[sibling, :depth, lanes])
        for h in range(heads - 1):
            y = y + far_part(h, lanes)
        total[:, lanes] = y
        return 0

    def far_part(h, lanes):
        rows = slice(h * DEPTH, (h + 1) * DEPTH)
        return dot(
            jnp.concatenate([taken[across, h], taken[opposite, h]], axis=1),
            jnp.concatenate([wfull[across, rows, lanes], wfull[opposite, rows, lanes]], axis=0),
        )

    lax.fori_loop(0, tiles, wide_part, 0)
    for k in range(2):
        recur_copy(k, heads - 1).wait_recv()
    for j in range(tiles):
        lanes = slice(j * tile, (j + 1) * tile)
        out[:, lanes] = (total[:, lanes] + far_part(heads - 1, lanes)).astype(BF16)

    w_across.wait_send()
    beside.wait_send()
    w_beside.wait_send()
    w_relay.wait_send()

    def sent_pieces(i, _):
        crossing(i).wait_send()
        relay(i).wait_send()
        return 0

    lax.fori_loop(0, count, sent_pieces, 0)
    for e in range(rights):
        ring_right(e).wait_send()
    for e in range(lefts):
        ring_left(e).wait_send()
    for d in range(2):
        exists, _, _ = partner(d, 1)

        @pl.when(exists)
        def _():
            edge_copy(d, length, padded, e_send, e_recv).wait_send()

    for k in range(steps):
        for d in range(2):
            exists, _, _ = partner(d, strides()[k])

            @pl.when(exists)
            def _():
                for h in range(heads):
                    scan_copy(k, d, h, sent, landed, p_send, p_recv).wait_send()

    for k in range(3):
        pool_copy(k).wait_send()
        for h in range(heads):
            recur_copy(k, h).wait_send()


def shards(
    tokens, norm_gain, w_query, w_forget_fwd, w_forget_bwd, w_value, w_gate, w_pool_in,
    forget_gap, added_log_retention, initial_state, head_gain, pool_mix, pool_gain,
    w_out_recur, w_out_pool,
):
    weights = (w_query, w_forget_fwd, w_forget_bwd, w_value, w_gate, w_pool_in)
    length, width = tokens.shape
    features, columns = w_query.shape
    heads = columns // DEPTH
    count = length // CHUNK
    share = length // 4
    subs = share // CHUNK
    depth, out_width = w_out_recur.shape
    steps = len(strides())
    size = ring_size()
    rights, lefts = 2 * (size // 2), 2 * (size - 1 - size // 2)
    dma = pltpu.SemaphoreType.DMA
    operands = (
        tokens, norm_gain[None, :], *weights, forget_gap, added_log_retention.T, initial_state,
        head_gain[None, :], pool_mix, pool_gain[None, :], w_out_recur, w_out_pool,
    )

    def like(array):
        return pltpu.VMEM(array.shape, array.dtype)

    return pl.pallas_call(
        functools.partial(mixer_kernel, pool_mix.shape[0]),
        out_shape=jax.ShapeDtypeStruct((share, out_width), BF16),
        in_specs=[ANY] * len(operands),
        out_specs=VM,
        scratch_shapes=[
            pltpu.VMEM((4, length, width), BF16),
            like(operands[1]),
            pltpu.VMEM((6, features, columns), BF16),
            like(operands[8]), like(operands[9]), like(operands[10]), like(operands[11]),
            like(operands[12]), like(operands[13]),
            pltpu.VMEM((4, 2 * depth, out_width), BF16),
            pltpu.VMEM((6, length, columns), F32),
            pltpu.VMEM((length, 1), F32),
            pltpu.VMEM((2, count, CHUNK, heads), F32),
            pltpu.VMEM((2, count, heads, CHUNK), F32),
            pltpu.VMEM((heads, DEPTH, 2 * DEPTH), F32),
            pltpu.VMEM((length, columns), BF16),
            pltpu.VMEM((length, columns), BF16),
            pltpu.VMEM((length, columns), F32),
            pltpu.VMEM((2, length, columns), BF16),
            pltpu.VMEM((2, length, columns), F32),
            pltpu.VMEM((length, columns), F32),
            pltpu.VMEM((heads, length, 2 * DEPTH), BF16),
            pltpu.VMEM((count, heads, DEPTH, 2 * DEPTH), F32),
            pltpu.VMEM((2, count, 1, columns), F32),
            pltpu.VMEM((count, heads, DEPTH, DEPTH), F32),
            pltpu.VMEM((count, 1, columns), F32),
            pltpu.VMEM((2, heads, DEPTH, DEPTH), F32),
            pltpu.VMEM((2, 1, columns), F32),
            pltpu.VMEM((length + 2 * RIM, columns), BF16),
            pltpu.VMEM((steps, 2, heads, DEPTH + 16, DEPTH), BF16),
            pltpu.VMEM((steps, 2, heads, DEPTH + 16, DEPTH), BF16),
            pltpu.VMEM((2, heads, DEPTH, DEPTH), F32),
            pltpu.VMEM((2, 1, columns), F32),
            pltpu.VMEM((heads, length, DEPTH), BF16),
            pltpu.VMEM((4, heads, share, DEPTH), BF16),
            pltpu.VMEM((3, share, columns), BF16),
            pltpu.VMEM((4, share, columns), BF16),
            pltpu.VMEM((share, out_width), F32),
            pltpu.VMEM((CHUNK, 2 * width), BF16),
            pltpu.VMEM((CHUNK, 1), F32),
            dma((16,)), dma((2,)), dma((count,)), dma((count,)), dma((count,)), dma((count,)),
            dma((2,)), dma((2,)), dma((2,)),
            dma((rights,)), dma((rights,)), dma((lefts,)), dma((lefts,)),
            dma((steps, 2, heads)), dma((steps, 2, heads)), dma((2,)), dma((2,)),
            dma((3,)), dma((3,)), dma((heads, 3)), dma((heads, 3)),
        ],
        compiler_params=pltpu.CompilerParams(
            collective_id=0, has_side_effects=True, vmem_limit_bytes=VMEM_LIMIT
        ),
        name="mixer",
    )(*operands)


def solution(mesh):
    in_specs = (
        P("sp", "tp"), P(), P(None, "tp"), P(None, "tp"), P(None, "tp"), P(None, "tp"),
        P(None, "tp"), P(None, "tp"), P(None, "tp"), P("sp", "tp"), P(None, "tp", None, None),
        P("tp"), P("tp", None, None), P("tp"), P("tp", None), P("tp", None),
    )
    out_specs = P(("sp", "tp"), None)
    return jax.shard_map(shards, mesh=mesh, in_specs=in_specs, out_specs=out_specs, check_vma=False)
```

```python
import functools

import jax
import jax.numpy as jnp
from jax import lax
from jax.experimental import pallas as pl
from jax.experimental.pallas import tpu as pltpu
from jax.sharding import PartitionSpec as P

DEPTH = 128
CHUNK = 128
EPSILON = 1e-06
RIM = 16
RING = 8
MESH = pl.DeviceIdType.MESH
F32 = jnp.float32
BF16 = jnp.bfloat16
VMEM_LIMIT = 52 * 1024 * 1024
ANY = pl.BlockSpec(memory_space=pl.ANY)
VM = pl.BlockSpec(memory_space=pltpu.VMEM)
EXACT = lax.Precision.HIGHEST


def dot(a, b, precision=None):
    return jnp.dot(a, b, preferred_element_type=F32, precision=precision)


def dot_t(a, b, precision=None):
    return lax.dot_general(
        a, b, (((1,), (1,)), ((), ())), preferred_element_type=F32, precision=precision
    )


def t_dot(a, b):
    return lax.dot_general(a, b, (((0,), (0,)), ((), ())), preferred_element_type=F32)


def peers():
    me = lax.axis_index("tp")
    sibling = me + 1 - 2 * lax.rem(me, 2)
    across = lax.rem(me + 2, 4)
    return me, sibling, across, lax.rem(sibling + 2, 4)


def strides():
    count = lax.axis_size("sp")
    return [1 << k for k in range(count.bit_length()) if 1 << k < count]


def partner(d, stride):
    me, count = lax.axis_index("sp"), lax.axis_size("sp")
    above, below = me + stride < count, me >= stride
    return (above, me + stride, below) if d == 0 else (below, me - stride, above)


def ring_size():
    return min(RING, lax.axis_size("sp"))


def ring_place():
    size = ring_size()
    me = lax.axis_index("sp")
    base, mine = me - lax.rem(me, size), lax.rem(me, size)
    place = jnp.where(lax.rem(mine, 2) == 0, mine // 2, size - 1 - mine // 2)

    def index(spot):
        spot = lax.rem(spot + size, size)
        return base + jnp.where(spot < size // 2, 2 * spot, 2 * (size - 1 - spot) + 1)

    return place, index(place + 1), index(place - 1)


def greet():
    barrier = pltpu.get_barrier_semaphore()
    _, sibling, across, opposite = peers()
    _, right, left = ring_place()
    for device in (sibling, across, opposite):
        pl.semaphore_signal(barrier, inc=1, device_id={"tp": device}, device_id_type=MESH)
    for device in (right, left):
        pl.semaphore_signal(barrier, inc=1, device_id={"sp": device}, device_id_type=MESH)
    number = jnp.int32(5)
    for stride in strides():
        for d in range(2):
            exists, target, _ = partner(d, stride)

            @pl.when(exists)
            def _():
                pl.semaphore_signal(
                    barrier, inc=1, device_id={"sp": target}, device_id_type=MESH
                )

            number = number + jnp.where(exists, 1, 0)
    pl.semaphore_wait(barrier, number)


def edge_copy(d, length, padded, e_send, e_recv):
    _, target, _ = partner(d, 1)
    begin, there = (length, 0) if d == 0 else (RIM, RIM + length)
    return pltpu.make_async_remote_copy(
        padded.at[pl.ds(begin, RIM)], padded.at[pl.ds(there, RIM)], e_send.at[d], e_recv.at[d],
        device_id={"sp": target}, device_id_type=MESH,
    )


def edge_start(d, length, padded, e_send, e_recv):
    exists, _, _ = partner(d, 1)

    @pl.when(exists)
    def _():
        edge_copy(d, length, padded, e_send, e_recv).start()


def edge_wait(d, length, padded, e_send, e_recv):
    _, _, source = partner(d, 1)

    @pl.when(source)
    def _():
        edge_copy(d, length, padded, e_send, e_recv).wait_recv()


def scan_copy(k, d, h, sent, landed, p_send, p_recv):
    _, target, _ = partner(d, strides()[k])
    return pltpu.make_async_remote_copy(
        sent.at[k, d, h], landed.at[k, d, h], p_send.at[k, d, h], p_recv.at[k, d, h],
        device_id={"sp": target}, device_id_type=MESH,
    )


def scan_start(k, d, h, state, offset, sent, landed, before, before_keep, p_send, p_recv):
    exists, _, _ = partner(d, strides()[k])

    @pl.when(exists)
    def _():
        lanes = slice(h * DEPTH, (h + 1) * DEPTH)
        keep = jnp.exp(offset[d, :, lanes])
        sent[k, d, h, :DEPTH, :] = (keep * before[d, h] + state[d, h]).astype(BF16)
        sent[k, d, h, DEPTH:, :] = jnp.broadcast_to(
            keep * before_keep[d, :, lanes], (16, DEPTH)
        ).astype(BF16)
        scan_copy(k, d, h, sent, landed, p_send, p_recv).start()


def scan_close(k, d, h, sent, landed, before, before_keep, p_send, p_recv):
    _, _, source = partner(d, strides()[k])

    @pl.when(source)
    def _():
        scan_copy(k, d, h, sent, landed, p_send, p_recv).wait_recv()
        lanes = slice(h * DEPTH, (h + 1) * DEPTH)
        keep = before_keep[d, :, lanes]
        early = landed[k, d, h].astype(F32)
        before[d, h] = keep * early[:DEPTH] + before[d, h]
        before_keep[d, :, lanes] = keep * early[DEPTH : DEPTH + 1]


def mixer_kernel(groups, *refs):
    (h_tokens, h_gain, *h_weights) = refs[:8]
    (h_gap, h_added, h_initial, h_head, h_mix, h_scale, h_recur, h_pool) = refs[8:16]
    out = refs[16]
    (
        held, gain, wide, gap, added, initial, head_gain, mix, pool_gain, wfull,
        acc, square, cols, rows_of, turned, query_pre, value, gated, ent, runs, inner, reach,
        starts, offsets, chunk_state, chunk_keep, state, offset, padded,
        sent, landed, before, before_keep, given, taken, passed, brought, total, kept_x, kept_scale,
        l_sem, s_sem, x_send, x_recv, f_send, f_recv, w_sem, b_sem, r_sem,
        g_send, g_recv, q_send, q_recv, p_send, p_recv, e_send, e_recv,
        a_send, a_recv, c_send, c_recv,
    ) = refs[17:]
    me, sibling, across, opposite = peers()
    length, width = held.shape[1:]
    columns = wide.shape[2]
    heads = columns // DEPTH
    count = length // CHUNK
    share = length // 4
    subs = share // CHUNK
    features = 4 * width
    depth = wfull.shape[1] // 2
    steps = len(strides())

    own_w = [
        pltpu.make_async_copy(h_recur, wfull.at[me, pl.ds(0, depth)], l_sem.at[0]),
        pltpu.make_async_copy(h_pool, wfull.at[me, pl.ds(depth, depth)], l_sem.at[1]),
    ]
    own_t = pltpu.make_async_copy(h_tokens, held.at[me], l_sem.at[2])
    small = [
        pltpu.make_async_copy(a, b, l_sem.at[3 + i])
        for i, (a, b) in enumerate((
            (h_gain, gain), (h_gap, gap), (h_added, added), (h_initial, initial),
            (h_head, head_gain), (h_mix, mix), (h_scale, pool_gain),
        ))
    ]
    loads = [
        pltpu.make_async_copy(w, wide.at[i], l_sem.at[10 + i]) for i, w in enumerate(h_weights)
    ]
    for copy in own_w + [own_t] + small + loads:
        copy.start()
    greet()

    size = ring_size()
    slab = 2 * depth // size
    half = slab // 2
    place, right, left = ring_place()
    events = size - 1

    mine = pl.ds(pl.multiple_of(place * slab, slab), slab)
    w_across = pltpu.make_async_remote_copy(
        wfull.at[me, mine], wfull.at[me, mine], w_sem.at[0], w_sem.at[1],
        device_id={"tp": across}, device_id_type=MESH,
    )
    w_beside = pltpu.make_async_remote_copy(
        wfull.at[me], wfull.at[me], b_sem.at[0], b_sem.at[1],
        device_id={"tp": sibling}, device_id_type=MESH,
    )
    def w_pass(rows, send, recv):
        return pltpu.make_async_remote_copy(
            wfull.at[across, rows], wfull.at[across, rows], send, recv,
            device_id={"tp": sibling}, device_id_type=MESH,
        )

    def ring_rows(way, e):
        spot = lax.rem(place + (e // 2 if way else size - e // 2), size)
        side = 1 - lax.rem(e, 2) if way else lax.rem(e, 2)
        return pl.ds(pl.multiple_of(spot * slab + side * half, half), half)

    def ring_copy(way, e):
        at = ring_rows(way, e)
        return pltpu.make_async_remote_copy(
            wfull.at[across, at], wfull.at[across, at], g_send.at[way, e], g_recv.at[way, e],
            device_id={"sp": left if way else right}, device_id_type=MESH,
        )

    def ring_relay(way, e):
        return w_pass(ring_rows(way, e + 2), q_send.at[way, e], q_recv.at[way, e])

    def ring_turn(e):
        for way in range(2):
            ring_copy(way, e).wait_recv()

            @pl.when(e + 2 < events)
            def _():
                ring_copy(way, e + 2).start()

            ring_relay(way, e).start()

    beside = pltpu.make_async_remote_copy(
        held.at[me], held.at[me], s_sem.at[0], s_sem.at[1],
        device_id={"tp": sibling}, device_id_type=MESH,
    )

    def piece(i):
        return pl.ds(pl.multiple_of(i * CHUNK, CHUNK), CHUNK)

    def crossing(i):
        return pltpu.make_async_remote_copy(
            held.at[me, piece(i)], held.at[me, piece(i)], x_send.at[i], x_recv.at[i],
            device_id={"tp": across}, device_id_type=MESH,
        )

    def relay(i):
        return pltpu.make_async_remote_copy(
            held.at[across, piece(i)], held.at[across, piece(i)], f_send.at[i], f_recv.at[i],
            device_id={"tp": sibling}, device_id_type=MESH,
        )

    for copy in own_w:
        copy.wait()
    w_across.start()
    own_t.wait()
    beside.start()
    for i in range(count):
        crossing(i).start()
    w_beside.start()
    for copy in small:
        copy.wait()

    row = lax.broadcasted_iota(jnp.int32, (CHUNK, CHUNK), 0)
    col = lax.broadcasted_iota(jnp.int32, (CHUNK, CHUNK), 1)
    lower, upper = row >= col, row <= col
    lower_f, upper_f = lower.astype(F32), upper.astype(F32)
    lower_2 = jnp.concatenate([lower_f, lower_f], axis=1).astype(BF16)
    upper_2 = jnp.concatenate([upper_f, upper_f], axis=1).astype(BF16)

    def sums(c, _):
        add = added[:, piece(c)]
        cols[0, c] = dot_t(lower_f, add, EXACT)
        cols[1, c] = dot_t(upper_f, add, EXACT)
        rows_of[0, c] = dot(add, upper_f, EXACT)
        rows_of[1, c] = dot(add, lower_f, EXACT)
        return 0

    lax.fori_loop(0, count, sums, 0)
    for h in range(heads):
        for d in range(2):
            turned[h, :, d * DEPTH : (d + 1) * DEPTH] = initial[d, h].T
    state[...] = jnp.zeros_like(state)
    offset[...] = jnp.zeros_like(offset)
    before[...] = jnp.zeros_like(before)
    before_keep[...] = jnp.ones_like(before_keep)
    for d in range(2):
        _, _, source = partner(d, 1)
        begin = 0 if d == 0 else RIM + length

        @pl.when(jnp.logical_not(source))
        def _():
            padded[pl.ds(begin, RIM), :] = jnp.zeros((RIM, columns), BF16)

    pair = me // 2
    near, far = 2 * pair, 2 - 2 * pair

    def normed(first, at):
        parts, squares = [], 0.0
        for o in range(2):
            x = held[first + o, at, :].astype(F32)
            squares = squares + jnp.sum(x * x, axis=1, keepdims=True)
            lanes = pl.ds(pl.multiple_of((first + o) * width, width), width)
            parts.append((x * gain[:, lanes]).astype(BF16))
        return jnp.concatenate(parts, axis=1), squares

    def depth_of(first):
        return pl.ds(pl.multiple_of(first * width, 2 * width), 2 * width)

    for copy in loads:
        copy.wait()
    beside.wait_recv()

    def own(i, _):
        at = pl.ds(pl.multiple_of(i * share, share), share)
        x, squares = normed(near, at)
        square[at, :] = squares
        for j in range(6):
            acc[j, at, :] = dot(x, wide[j, depth_of(near), :])
        return 0

    lax.fori_loop(0, 4, own, 0)
    w_across.wait_recv()
    for e in range(min(2, events)):
        for way in range(2):
            ring_copy(way, e).start()
    w_pass(mine, r_sem.at[0], r_sem.at[1]).start()

    def gates(pre, gap_row, sums):
        enter = gap_row * (1.0 / (1.0 + jnp.exp(pre)))
        keep = jnp.log1p(-enter)
        high = keep.astype(BF16)
        low = (keep - high.astype(F32)).astype(BF16)
        return enter, dot(sums, jnp.concatenate([high, low], axis=0))

    def local(c):
        at = piece(c)
        x = query_pre[at, :].astype(F32)
        query = x / (1.0 + jnp.exp(-x))
        q_f, q_b = query * jnp.exp(runs[0, at, :]), query * jnp.exp(runs[1, at, :])
        e_f, e_b = ent[0, at, :], ent[1, at, :]
        values = value[at, :]
        col_f, col_b = cols[0, c], cols[1, c]
        row_f, row_b = rows_of[0, c], rows_of[1, c]
        for h in range(heads):
            lanes = slice(h * DEPTH, (h + 1) * DEPTH)
            a_col, b_col = col_f[:, h : h + 1], col_b[:, h : h + 1]
            fade = jnp.exp(
                jnp.where(lower, a_col - row_f[h : h + 1, :], b_col - row_b[h : h + 1, :])
            )
            w_f = dot_t(q_f[:, lanes].astype(BF16), e_f[:, lanes])
            w_b = dot_t(q_b[:, lanes].astype(BF16), e_b[:, lanes])
            weight = (jnp.where(lower, w_f, 0.0) + jnp.where(upper, w_b, 0.0)) * fade
            inner[at, lanes] = dot(weight.astype(BF16), values[:, lanes])
            reach[h, at, :DEPTH] = (q_f[:, lanes] * jnp.exp(a_col)).astype(BF16)
            reach[h, at, DEPTH:] = (q_b[:, lanes] * jnp.exp(b_col)).astype(BF16)

    def project(j, x, scale, at):
        return ((acc[j, at, :] + dot(x, wide[j, depth_of(far), :])) * scale).astype(BF16)

    def late(c):
        at, x, scale = piece(c), kept_x[...], kept_scale[...]
        padded[pl.ds(pl.multiple_of(c * CHUNK + RIM, RIM), CHUNK), :] = project(5, x, scale, at)
        query_pre[at, :] = project(0, x, scale, at)
        gate = project(4, x, scale, at).astype(F32)
        gated[at, :] = head_gain[...] / (1.0 + jnp.exp(-gate))

    def step(i, _):
        at = piece(i)
        crossing(i).wait_recv()
        relay(i).start()

        @pl.when(i > 0)
        def _():
            late(i - 1)
            local(i - 1)

        @pl.when((i > 0) & (i <= events))
        def _():
            ring_turn(i - 1)

        @pl.when(i == 1)
        def _():
            edge_start(1, length, padded, e_send, e_recv)

        relay(i).wait_recv()
        x, squares = normed(far, at)
        scale = lax.rsqrt((square[at, :] + squares) / features + EPSILON)

        kept_x[...], kept_scale[...] = x, scale
        pre_f, pre_b, values = (project(j, x, scale, at) for j in (1, 2, 3))
        value[at, :] = values
        enter_f, run_f = gates(pre_f.astype(F32), gap[0:1, :], lower_2)
        enter_b, run_b = gates(pre_b.astype(F32), gap[1:2, :], upper_2)
        runs[0, at, :], runs[1, at, :] = run_f, run_b
        e_f, e_b = enter_f * jnp.exp(-run_f), enter_b * jnp.exp(-run_b)
        ent[0, at, :], ent[1, at, :] = e_f.astype(BF16), e_b.astype(BF16)
        close_f, close_b = run_f[CHUNK - 1 : CHUNK, :], run_b[0:1, :]
        last_f, last_b = e_f * jnp.exp(close_f), e_b * jnp.exp(close_b)
        offsets[0, i] = offset[0]
        col_f, col_b = cols[0, i], cols[1, i]
        for h in range(heads):
            lanes = slice(h * DEPTH, (h + 1) * DEPTH)
            a_col, b_col = col_f[:, h : h + 1], col_b[:, h : h + 1]
            a_end, b_end = a_col[CHUNK - 1 : CHUNK, :], b_col[0:1, :]
            total_f = close_f[:, lanes] + a_end
            ends_f = (last_f[:, lanes] * jnp.exp(a_end - a_col)).astype(BF16)
            ends_b = (last_b[:, lanes] * jnp.exp(b_end - b_col)).astype(BF16)
            ends = t_dot(values[:, lanes], jnp.concatenate([ends_f, ends_b], axis=1))
            starts[i, h, :, :DEPTH] = state[0, h]
            state[0, h] = jnp.exp(total_f) * state[0, h] + ends[:, :DEPTH]
            chunk_state[i, h] = ends[:, DEPTH:]
            chunk_keep[i, :, lanes] = close_b[:, lanes] + b_end
            offset[0, :, lanes] = offset[0, :, lanes] + total_f
        return 0

    lax.fori_loop(0, count, step, 0)

    def descend(i, _):
        c = count - 1 - i
        offsets[1, c] = offset[1]
        for h in range(heads):
            lanes = slice(h * DEPTH, (h + 1) * DEPTH)
            starts[c, h, :, DEPTH:] = state[1, h]
            keep = chunk_keep[c, :, lanes]
            state[1, h] = jnp.exp(keep) * state[1, h] + chunk_state[c, h]
            offset[1, :, lanes] = offset[1, :, lanes] + keep
        return 0

    window = jnp.left_shift(jnp.int32(2), lax.axis_index("tp") * groups)
    sequence, first_row = length * lax.axis_size("sp"), lax.axis_index("sp") * length

    def pooled(owner):
        begin = pl.multiple_of(owner * share, share)
        span = share + 2 * RIM
        near_rows = padded[pl.ds(begin, span), :]
        target = first_row + begin + lax.broadcasted_iota(jnp.int32, (share, span), 0)
        source = first_row + begin - RIM + lax.broadcasted_iota(jnp.int32, (share, span), 1)
        low = target - window // 2
        inside = (source >= low) & (source < low + window) & (source >= 0) & (source < sequence)
        start = first_row + begin + lax.broadcasted_iota(jnp.int32, (share, 1), 0) - window // 2
        number = jnp.minimum(start + window, sequence) - jnp.maximum(start, 0)
        mean = dot(inside.astype(F32).astype(BF16), near_rows) / number.astype(F32)
        here = padded[pl.ds(pl.multiple_of(begin + RIM, RIM), share), :].astype(F32)
        return (dot((mean - here).astype(BF16), mix[0]) * pool_gain[...]).astype(BF16)

    def pool_copy(r, sender):
        return pltpu.make_async_remote_copy(
            passed.at[r], brought.at[me], a_send.at[r], a_recv.at[sender],
            device_id={"tp": jnp.int32(r)}, device_id_type=MESH,
        )

    def pool_away(r):
        if r == 3:
            edge_wait(1, length, padded, e_send, e_recv)
        if r == 0:
            edge_wait(0, length, padded, e_send, e_recv)
        passed[r] = pooled(r)

        @pl.when(me != r)
        def _():
            pool_copy(r, me).start()

    def ring_end():
        for e in range(count - 1, events):
            ring_turn(e)

    def late_last():
        late(count - 1)
        edge_start(0, length, padded, e_send, e_recv)
        local(count - 1)

    tile = 512
    tiles = out.shape[1] // tile

    def wide_pool():
        w_beside.wait_recv()
        w_pass(mine, r_sem.at[0], r_sem.at[1]).wait_recv()

        def landed_ring(e, _):
            for way in range(2):
                ring_relay(way, e).wait_recv()
            return 0

        lax.fori_loop(0, events, landed_ring, 0)
        for r in range(4):
            @pl.when(me != r)
            def _():
                pool_copy(r, r).wait_recv()

        def part(j, _):
            lanes = pl.ds(pl.multiple_of(j * tile, tile), tile)
            y = 0.0
            for r in range(4):
                x = jnp.where(me == r, passed[r], brought[r])
                y = y + dot(x, wfull[r, depth:, lanes])
            total[:, lanes] = y
            return 0

        lax.fori_loop(0, tiles, part, 0)

    def finished(c, h):
        at, lanes = piece(c), slice(h * DEPTH, (h + 1) * DEPTH)
        ages = jnp.exp(jnp.concatenate([offsets[0, c, :, lanes], offsets[1, c, :, lanes]], axis=1))
        enter = (starts[c, h] + ages * turned[h]).astype(BF16)
        both = inner[at, lanes] + dot_t(reach[h, at, :], enter)
        both = both * lax.rsqrt(jnp.mean(both * both, axis=1, keepdims=True) + EPSILON)
        given[h, at, :] = (both * gated[at, lanes]).astype(BF16)

    relations = (across, opposite, sibling, me)

    def recur_copy(k, h):
        there = relations[k]
        at = pl.ds(pl.multiple_of(there * share, share), share)
        return pltpu.make_async_remote_copy(
            given.at[h, at], taken.at[me, h], c_send.at[h, k], c_recv.at[h, k],
            device_id={"tp": there}, device_id_type=MESH,
        )

    def away(k, h):
        for sub in range(subs):
            finished(relations[k] * subs + sub, h)
        if k < 3:
            recur_copy(k, h).start()

    scan = (sent, landed, before, before_keep, p_send, p_recv)
    fillers = [
        (late_last, ring_end, lambda: pool_away(1), lambda: pool_away(2), lambda: pool_away(3)),
        (lambda: pool_away(0),),
        (wide_pool,),
    ]
    rounds = [[] for _ in range(max(steps, 1))]
    for i, group in enumerate(fillers):
        rounds[min(i, len(rounds) - 1)].extend(group)
    lax.fori_loop(0, count, descend, 0)
    for k in range(steps):
        for h in range(heads):
            for d in range(2):
                if k:
                    scan_close(k - 1, d, h, *scan)
                scan_start(k, d, h, state, offset, *scan)
        for filler in rounds[k]:
            filler()
    if not steps:
        for filler in rounds[0]:
            filler()
    for h in range(heads):
        for d in range(2):
            if steps:
                scan_close(steps - 1, d, h, *scan)
            lanes = slice(d * DEPTH, (d + 1) * DEPTH)
            keep = before_keep[d, :, h * DEPTH : (h + 1) * DEPTH]
            turned[h, :, lanes] = keep * turned[h, :, lanes] + before[d, h]
        for k in range(2):
            away(k, h)
    for k in (2, 3):
        for h in range(heads):
            away(k, h)

    def all_heads(rows):
        return jnp.concatenate([rows(h) for h in range(heads)], axis=1)

    def far_part(h, lanes):
        rows = slice(h * DEPTH, (h + 1) * DEPTH)
        return dot(
            jnp.concatenate([taken[across, h], taken[opposite, h]], axis=1),
            jnp.concatenate([wfull[across, rows, lanes], wfull[opposite, rows, lanes]], axis=0),
        )

    for h in range(heads):
        recur_copy(2, h).wait_recv()
    home = pl.ds(pl.multiple_of(me * share, share), share)
    for j in range(tiles):
        lanes = slice(j * tile, (j + 1) * tile)
        y = total[:, lanes] + dot(
            all_heads(lambda h: given[h, home, :]), wfull[me, :depth, lanes]
        )
        total[:, lanes] = y + dot(
            all_heads(lambda h: taken[sibling, h]), wfull[sibling, :depth, lanes]
        )
    for h in range(heads):
        for k in range(2):
            recur_copy(k, h).wait_recv()
        for j in range(tiles):
            lanes = slice(j * tile, (j + 1) * tile)
            y = total[:, lanes] + far_part(h, lanes)
            if h == heads - 1:
                out[:, lanes] = y.astype(BF16)
            else:
                total[:, lanes] = y

    w_across.wait_send()
    beside.wait_send()
    w_beside.wait_send()
    w_pass(mine, r_sem.at[0], r_sem.at[1]).wait_send()

    def sent_pieces(i, _):
        crossing(i).wait_send()
        relay(i).wait_send()
        return 0

    lax.fori_loop(0, count, sent_pieces, 0)

    def sent_ring(e, _):
        for way in range(2):
            ring_copy(way, e).wait_send()
            ring_relay(way, e).wait_send()
        return 0

    lax.fori_loop(0, events, sent_ring, 0)
    for d in range(2):
        exists, _, _ = partner(d, 1)

        @pl.when(exists)
        def _():
            edge_copy(d, length, padded, e_send, e_recv).wait_send()

    for k in range(steps):
        for d in range(2):
            exists, _, _ = partner(d, strides()[k])

            @pl.when(exists)
            def _():
                for h in range(heads):
                    scan_copy(k, d, h, sent, landed, p_send, p_recv).wait_send()

    for r in range(4):
        @pl.when(me != r)
        def _():
            pool_copy(r, me).wait_send()

    for h in range(heads):
        for k in range(3):
            recur_copy(k, h).wait_send()


def shards(
    tokens, norm_gain, w_query, w_forget_fwd, w_forget_bwd, w_value, w_gate, w_pool_in,
    forget_gap, added_log_retention, initial_state, head_gain, pool_mix, pool_gain,
    w_out_recur, w_out_pool,
):
    weights = (w_query, w_forget_fwd, w_forget_bwd, w_value, w_gate, w_pool_in)
    length, width = tokens.shape
    features, columns = w_query.shape
    heads = columns // DEPTH
    count = length // CHUNK
    share = length // 4
    subs = share // CHUNK
    depth, out_width = w_out_recur.shape
    steps = len(strides())
    size = ring_size()
    events = size - 1
    dma = pltpu.SemaphoreType.DMA
    operands = (
        tokens, norm_gain[None, :], *weights, forget_gap, added_log_retention.T, initial_state,
        head_gain[None, :], pool_mix, pool_gain[None, :], w_out_recur, w_out_pool,
    )

    def like(array):
        return pltpu.VMEM(array.shape, array.dtype)

    return pl.pallas_call(
        functools.partial(mixer_kernel, pool_mix.shape[0]),
        out_shape=pltpu.VMEM((share, out_width), BF16),
        in_specs=[ANY] * len(operands),
        out_specs=VM,
        scratch_shapes=[
            pltpu.VMEM((4, length, width), BF16),
            like(operands[1]),
            pltpu.VMEM((6, features, columns), BF16),
            like(operands[8]), like(operands[9]), like(operands[10]), like(operands[11]),
            like(operands[12]), like(operands[13]),
            pltpu.VMEM((4, 2 * depth, out_width), BF16),
            pltpu.VMEM((6, length, columns), F32),
            pltpu.VMEM((length, 1), F32),
            pltpu.VMEM((2, count, CHUNK, heads), F32),
            pltpu.VMEM((2, count, heads, CHUNK), F32),
            pltpu.VMEM((heads, DEPTH, 2 * DEPTH), F32),
            pltpu.VMEM((length, columns), BF16),
            pltpu.VMEM((length, columns), BF16),
            pltpu.VMEM((length, columns), F32),
            pltpu.VMEM((2, length, columns), BF16),
            pltpu.VMEM((2, length, columns), F32),
            pltpu.VMEM((length, columns), F32),
            pltpu.VMEM((heads, length, 2 * DEPTH), BF16),
            pltpu.VMEM((count, heads, DEPTH, 2 * DEPTH), F32),
            pltpu.VMEM((2, count, 1, columns), F32),
            pltpu.VMEM((count, heads, DEPTH, DEPTH), F32),
            pltpu.VMEM((count, 1, columns), F32),
            pltpu.VMEM((2, heads, DEPTH, DEPTH), F32),
            pltpu.VMEM((2, 1, columns), F32),
            pltpu.VMEM((length + 2 * RIM, columns), BF16),
            pltpu.VMEM((steps, 2, heads, DEPTH + 16, DEPTH), BF16),
            pltpu.VMEM((steps, 2, heads, DEPTH + 16, DEPTH), BF16),
            pltpu.VMEM((2, heads, DEPTH, DEPTH), F32),
            pltpu.VMEM((2, 1, columns), F32),
            pltpu.VMEM((heads, length, DEPTH), BF16),
            pltpu.VMEM((4, heads, share, DEPTH), BF16),
            pltpu.VMEM((4, share, columns), BF16),
            pltpu.VMEM((4, share, columns), BF16),
            pltpu.VMEM((share, out_width), F32),
            pltpu.VMEM((CHUNK, 2 * width), BF16),
            pltpu.VMEM((CHUNK, 1), F32),
            dma((16,)), dma((2,)), dma((count,)), dma((count,)), dma((count,)), dma((count,)),
            dma((2,)), dma((2,)), dma((2,)),
            dma((2, events)), dma((2, events)), dma((2, events)), dma((2, events)),
            dma((steps, 2, heads)), dma((steps, 2, heads)), dma((2,)), dma((2,)),
            dma((4,)), dma((4,)), dma((heads, 3)), dma((heads, 3)),
        ],
        compiler_params=pltpu.CompilerParams(
            collective_id=0, has_side_effects=True, vmem_limit_bytes=VMEM_LIMIT
        ),
        name="mixer",
    )(*(pltpu.with_memory_space_constraint(x, pltpu.HBM) for x in operands))


def solution(mesh):
    in_specs = (
        P("sp", "tp"), P(), P(None, "tp"), P(None, "tp"), P(None, "tp"), P(None, "tp"),
        P(None, "tp"), P(None, "tp"), P(None, "tp"), P("sp", "tp"), P(None, "tp", None, None),
        P("tp"), P("tp", None, None), P("tp"), P("tp", None), P("tp", None),
    )
    out_specs = P(("sp", "tp"), None)
    return jax.shard_map(shards, mesh=mesh, in_specs=in_specs, out_specs=out_specs, check_vma=False)
```

```python
import functools

import jax
import jax.numpy as jnp
from jax import lax
from jax.experimental import pallas as pl
from jax.experimental.pallas import tpu as pltpu
from jax.sharding import PartitionSpec as P

DEPTH = 128
CHUNK = 128
EPSILON = 1e-06
RIM = 16
RING = 8
MESH = pl.DeviceIdType.MESH
F32 = jnp.float32
BF16 = jnp.bfloat16
VMEM_LIMIT = 52 * 1024 * 1024
ANY = pl.BlockSpec(memory_space=pl.ANY)
VM = pl.BlockSpec(memory_space=pltpu.VMEM)
EXACT = lax.Precision.HIGHEST


def dot(a, b, precision=None):
    return jnp.dot(a, b, preferred_element_type=F32, precision=precision)


def dot_t(a, b, precision=None):
    return lax.dot_general(
        a, b, (((1,), (1,)), ((), ())), preferred_element_type=F32, precision=precision
    )


def t_dot(a, b):
    return lax.dot_general(a, b, (((0,), (0,)), ((), ())), preferred_element_type=F32)


def peers():
    me = lax.axis_index("tp")
    sibling = me + 1 - 2 * lax.rem(me, 2)
    across = lax.rem(me + 2, 4)
    return me, sibling, across, lax.rem(sibling + 2, 4)


def strides():
    count = lax.axis_size("sp")
    return [1 << k for k in range(count.bit_length()) if 1 << k < count]


def partner(d, stride):
    me, count = lax.axis_index("sp"), lax.axis_size("sp")
    above, below = me + stride < count, me >= stride
    if isinstance(d, int):
        return (above, me + stride, below) if d == 0 else (below, me - stride, above)
    target = jnp.where(d == 0, me + stride, me - stride)
    source = jnp.where(d == 0, me - stride, me + stride)
    return (target >= 0) & (target < count), target, (source >= 0) & (source < count)


def ring_size():
    return min(RING, lax.axis_size("sp"))


def ring_place():
    size = ring_size()
    me = lax.axis_index("sp")
    base, mine = me - lax.rem(me, size), lax.rem(me, size)
    place = jnp.where(lax.rem(mine, 2) == 0, mine // 2, size - 1 - mine // 2)

    def index(spot):
        spot = lax.rem(spot + size, size)
        return base + jnp.where(spot < size // 2, 2 * spot, 2 * (size - 1 - spot) + 1)

    return place, index(place + 1), index(place - 1)


def greet():
    barrier = pltpu.get_barrier_semaphore()
    _, sibling, across, opposite = peers()
    _, right, left = ring_place()
    for device in (sibling, across, opposite):
        pl.semaphore_signal(barrier, inc=1, device_id={"tp": device}, device_id_type=MESH)
    for device in (right, left):
        pl.semaphore_signal(barrier, inc=1, device_id={"sp": device}, device_id_type=MESH)
    number = jnp.int32(5)
    for stride in strides():
        for d in range(2):
            exists, target, _ = partner(d, stride)

            @pl.when(exists)
            def _():
                pl.semaphore_signal(
                    barrier, inc=1, device_id={"sp": target}, device_id_type=MESH
                )

            number = number + jnp.where(exists, 1, 0)
    pl.semaphore_wait(barrier, number)


def edge_copy(d, length, padded, e_send, e_recv):
    _, target, _ = partner(d, 1)
    there = 0 if d == 0 else RIM + length
    return pltpu.make_async_remote_copy(
        padded.at[pl.ds(length if d == 0 else RIM, RIM)], padded.at[pl.ds(there, RIM)],
        e_send.at[d], e_recv.at[d], device_id={"sp": target}, device_id_type=MESH,
    )


def edge_start(d, length, padded, e_send, e_recv):
    exists, _, _ = partner(d, 1)

    @pl.when(exists)
    def _():
        edge_copy(d, length, padded, e_send, e_recv).start()


def edge_wait(d, length, padded, e_send, e_recv):
    _, _, source = partner(d, 1)

    @pl.when(source)
    def _():
        edge_copy(d, length, padded, e_send, e_recv).wait_recv()


def scan_copy(k, d, h, sent, landed, p_send, p_recv):
    _, target, _ = partner(d, strides()[k])
    return pltpu.make_async_remote_copy(
        sent.at[k, d, h], landed.at[k, d, h], p_send.at[k, d], p_recv.at[k, d, h],
        device_id={"sp": target}, device_id_type=MESH,
    )


def scan_start(k, d, h, state, offset, sent, landed, before, before_keep, p_send, p_recv):
    exists, _, _ = partner(d, strides()[k])

    @pl.when(exists)
    def _():
        lanes = slice(h * DEPTH, (h + 1) * DEPTH)
        keep = jnp.exp(offset[d, :, lanes])
        sent[k, d, h, :DEPTH, :] = (keep * before[d, h] + state[d, h]).astype(BF16)
        sent[k, d, h, DEPTH:, :] = jnp.broadcast_to(
            keep * before_keep[d, :, lanes], (16, DEPTH)
        ).astype(BF16)
        scan_copy(k, d, h, sent, landed, p_send, p_recv).start()


def scan_close(k, d, h, sent, landed, before, before_keep, p_send, p_recv):
    _, _, source = partner(d, strides()[k])

    @pl.when(source)
    def _():
        scan_copy(k, d, h, sent, landed, p_send, p_recv).wait_recv()
        lanes = slice(h * DEPTH, (h + 1) * DEPTH)
        keep = before_keep[d, :, lanes]
        early = landed[k, d, h].astype(F32)
        before[d, h] = keep * early[:DEPTH] + before[d, h]
        before_keep[d, :, lanes] = keep * early[DEPTH : DEPTH + 1]


def mixer_kernel(groups, *refs):
    (h_tokens, h_gain, *h_weights) = refs[:8]
    (h_gap, h_added, h_initial, h_head, h_mix, h_scale, h_recur, h_pool) = refs[8:16]
    out = refs[16]
    (
        held, gain, wide, gap, added, initial, head_gain, mix, pool_gain, wfull,
        acc, square, cols, rows_of, turned, query_pre, value, gated, ent, runs, inner, reach,
        starts, offsets, chunk_state, chunk_keep, state, offset, padded,
        sent, landed, before, before_keep, given, taken, passed, brought, total, kept_x, kept_scale,
        l_sem, t_send, w_send, s_recv, x_recv, f_recv, w_recv, q_recv, g_recv,
        p_send, p_recv, e_send, e_recv, a_send, a_recv, c_send, c_recv,
    ) = refs[17:]
    me, sibling, across, opposite = peers()
    length, width = held.shape[1:]
    columns = wide.shape[2]
    heads = columns // DEPTH
    count = length // CHUNK
    share = length // 4
    subs = share // CHUNK
    features = 4 * width
    depth = wfull.shape[1] // 2
    steps = len(strides())

    own_w = [
        pltpu.make_async_copy(h_recur, wfull.at[me, pl.ds(0, depth)], l_sem.at[0]),
        pltpu.make_async_copy(h_pool, wfull.at[me, pl.ds(depth, depth)], l_sem.at[0]),
    ]
    own_t = pltpu.make_async_copy(h_tokens, held.at[me], l_sem.at[1])
    small = [
        pltpu.make_async_copy(a, b, l_sem.at[3 + i])
        for i, (a, b) in enumerate((
            (h_gain, gain), (h_gap, gap), (h_added, added), (h_initial, initial),
            (h_head, head_gain), (h_mix, mix), (h_scale, pool_gain),
        ))
    ]
    loads = [
        pltpu.make_async_copy(w, wide.at[i], l_sem.at[2]) for i, w in enumerate(h_weights)
    ]
    for copy in own_w + [own_t] + small + loads:
        copy.start()
    greet()

    size = ring_size()
    slab = 2 * depth // size
    half = slab // 2
    place, right, left = ring_place()
    events = size - 1

    mine = pl.ds(pl.multiple_of(place * slab, slab), slab)
    w_across = pltpu.make_async_remote_copy(
        wfull.at[me, mine], wfull.at[me, mine], w_send.at[0], w_recv.at[0],
        device_id={"tp": across}, device_id_type=MESH,
    )
    w_beside = pltpu.make_async_remote_copy(
        wfull.at[me], wfull.at[me], w_send.at[0], q_recv.at[0],
        device_id={"tp": sibling}, device_id_type=MESH,
    )
    def w_pass(rows):
        return pltpu.make_async_remote_copy(
            wfull.at[across, rows], wfull.at[across, rows], w_send.at[0], q_recv.at[0],
            device_id={"tp": sibling}, device_id_type=MESH,
        )

    def ring_rows(way, e):
        spot = lax.rem(place + (e // 2 if way else size - e // 2), size)
        side = 1 - lax.rem(e, 2) if way else lax.rem(e, 2)
        return pl.ds(pl.multiple_of(spot * slab + side * half, half), half)

    def ring_copy(way, e):
        at = ring_rows(way, e)
        return pltpu.make_async_remote_copy(
            wfull.at[across, at], wfull.at[across, at], w_send.at[0], g_recv.at[e],
            device_id={"sp": left if way else right}, device_id_type=MESH,
        )

    def ring_turn(e):
        landed_slab = wfull.at[across, pl.ds(0, slab)]
        pltpu.make_async_remote_copy(
            landed_slab, landed_slab, w_send.at[0], g_recv.at[e],
            device_id={"sp": right}, device_id_type=MESH,
        ).wait_recv()
        for way in range(2):
            @pl.when(e + 2 < events)
            def _():
                ring_copy(way, e + 2).start()

            w_pass(ring_rows(way, e + 2)).start()

    beside = pltpu.make_async_remote_copy(
        held.at[me], held.at[me], t_send.at[0], s_recv.at[0],
        device_id={"tp": sibling}, device_id_type=MESH,
    )

    def piece(i):
        return pl.ds(pl.multiple_of(i * CHUNK, CHUNK), CHUNK)

    def crossing(i):
        return pltpu.make_async_remote_copy(
            held.at[me, piece(i)], held.at[me, piece(i)], t_send.at[0], x_recv.at[i],
            device_id={"tp": across}, device_id_type=MESH,
        )

    def relay(i):
        return pltpu.make_async_remote_copy(
            held.at[across, piece(i)], held.at[across, piece(i)], t_send.at[0], f_recv.at[i],
            device_id={"tp": sibling}, device_id_type=MESH,
        )

    pltpu.make_async_copy(wfull.at[across], wfull.at[me], l_sem.at[0]).wait()
    w_across.start()
    own_t.wait()
    beside.start()
    for i in range(count):
        crossing(i).start()
    w_beside.start()
    for copy in small:
        copy.wait()

    row = lax.broadcasted_iota(jnp.int32, (CHUNK, CHUNK), 0)
    col = lax.broadcasted_iota(jnp.int32, (CHUNK, CHUNK), 1)
    lower, upper = row >= col, row <= col
    lower_f, upper_f = lower.astype(F32), upper.astype(F32)
    lower_2 = jnp.concatenate([lower_f, lower_f], axis=1).astype(BF16)
    upper_2 = jnp.concatenate([upper_f, upper_f], axis=1).astype(BF16)

    def sums(c, _):
        add = added[:, piece(c)]
        cols[0, c] = dot_t(lower_f, add, EXACT)
        cols[1, c] = dot_t(upper_f, add, EXACT)
        rows_of[0, c] = dot(add, upper_f, EXACT)
        rows_of[1, c] = dot(add, lower_f, EXACT)
        return 0

    lax.fori_loop(0, count, sums, 0)
    for h in range(heads):
        for d in range(2):
            turned[h, :, d * DEPTH : (d + 1) * DEPTH] = initial[d, h].T
    state[...] = jnp.zeros_like(state)
    offset[...] = jnp.zeros_like(offset)
    before[...] = jnp.zeros_like(before)
    before_keep[...] = jnp.ones_like(before_keep)
    for d in range(2):
        _, _, source = partner(d, 1)
        begin = 0 if d == 0 else RIM + length

        @pl.when(jnp.logical_not(source))
        def _():
            padded[pl.ds(begin, RIM), :] = jnp.zeros((RIM, columns), BF16)

    pair = me // 2
    near, far = 2 * pair, 2 - 2 * pair

    def normed(first, at):
        parts, squares = [], 0.0
        for o in range(2):
            x = held[first + o, at, :].astype(F32)
            squares = squares + jnp.sum(x * x, axis=1, keepdims=True)
            lanes = pl.ds(pl.multiple_of((first + o) * width, width), width)
            parts.append((x * gain[:, lanes]).astype(BF16))
        return jnp.concatenate(parts, axis=1), squares

    def depth_of(first):
        return pl.ds(pl.multiple_of(first * width, 2 * width), 2 * width)

    pltpu.make_async_copy(wide, wide, l_sem.at[2]).wait()
    beside.wait_recv()

    def own(i, _):
        at = pl.ds(pl.multiple_of(i * share, share), share)
        x, squares = normed(near, at)
        square[at, :] = squares
        for j in range(6):
            acc[j, at, :] = dot(x, wide[j, depth_of(near), :])
        return 0

    lax.fori_loop(0, 4, own, 0)
    w_across.wait_recv()
    for e in range(min(2, events)):
        for way in range(2):
            ring_copy(way, e).start()
    w_pass(mine).start()

    def gates(pre, gap_row, sums):
        enter = gap_row * (1.0 / (1.0 + jnp.exp(pre)))
        keep = jnp.log1p(-enter)
        high = keep.astype(BF16)
        low = (keep - high.astype(F32)).astype(BF16)
        return enter, dot(sums, jnp.concatenate([high, low], axis=0))

    def local(c):
        at = piece(c)
        x = query_pre[at, :].astype(F32)
        query = x / (1.0 + jnp.exp(-x))
        q_f, q_b = query * jnp.exp(runs[0, at, :]), query * jnp.exp(runs[1, at, :])
        e_f, e_b = ent[0, at, :], ent[1, at, :]
        values = value[at, :]
        col_f, col_b = cols[0, c], cols[1, c]
        row_f, row_b = rows_of[0, c], rows_of[1, c]
        for h in range(heads):
            lanes = slice(h * DEPTH, (h + 1) * DEPTH)
            a_col, b_col = col_f[:, h : h + 1], col_b[:, h : h + 1]
            fade = jnp.exp(
                jnp.where(lower, a_col - row_f[h : h + 1, :], b_col - row_b[h : h + 1, :])
            )
            w_f = dot_t(q_f[:, lanes].astype(BF16), e_f[:, lanes])
            w_b = dot_t(q_b[:, lanes].astype(BF16), e_b[:, lanes])
            weight = (jnp.where(lower, w_f, 0.0) + jnp.where(upper, w_b, 0.0)) * fade
            inner[at, lanes] = dot(weight.astype(BF16), values[:, lanes])
            reach[h, at, :DEPTH] = (q_f[:, lanes] * jnp.exp(a_col)).astype(BF16)
            reach[h, at, DEPTH:] = (q_b[:, lanes] * jnp.exp(b_col)).astype(BF16)

    def project(j, x, scale, at):
        return ((acc[j, at, :] + dot(x, wide[j, depth_of(far), :])) * scale).astype(BF16)

    def late_pool(c):
        rows = project(5, kept_x[...], kept_scale[...], piece(c))
        padded[pl.ds(pl.multiple_of(c * CHUNK + RIM, RIM), CHUNK), :] = rows

    def late(c):
        at, x, scale = piece(c), kept_x[...], kept_scale[...]
        query_pre[at, :] = project(0, x, scale, at)
        gate = project(4, x, scale, at).astype(F32)
        gated[at, :] = head_gain[...] / (1.0 + jnp.exp(-gate))

    def step(i, _):
        at = piece(i)
        crossing(i).wait_recv()
        relay(i).start()

        @pl.when(i > 0)
        def _():
            late_pool(i - 1)
            late(i - 1)
            local(i - 1)

        @pl.when((i > 0) & (i <= events))
        def _():
            ring_turn(i - 1)

        @pl.when(i == 1)
        def _():
            edge_start(1, length, padded, e_send, e_recv)

        relay(i).wait_recv()
        x, squares = normed(far, at)
        scale = lax.rsqrt((square[at, :] + squares) / features + EPSILON)

        kept_x[...], kept_scale[...] = x, scale
        pre_f, pre_b, values = (project(j, x, scale, at) for j in (1, 2, 3))
        value[at, :] = values
        enter_f, run_f = gates(pre_f.astype(F32), gap[0:1, :], lower_2)
        enter_b, run_b = gates(pre_b.astype(F32), gap[1:2, :], upper_2)
        runs[0, at, :], runs[1, at, :] = run_f, run_b
        e_f, e_b = enter_f * jnp.exp(-run_f), enter_b * jnp.exp(-run_b)
        ent[0, at, :], ent[1, at, :] = e_f.astype(BF16), e_b.astype(BF16)
        close_f, close_b = run_f[CHUNK - 1 : CHUNK, :], run_b[0:1, :]
        last_f, last_b = e_f * jnp.exp(close_f), e_b * jnp.exp(close_b)
        offsets[0, i] = offset[0]
        col_f, col_b = cols[0, i], cols[1, i]
        for h in range(heads):
            lanes = slice(h * DEPTH, (h + 1) * DEPTH)
            a_col, b_col = col_f[:, h : h + 1], col_b[:, h : h + 1]
            a_end, b_end = a_col[CHUNK - 1 : CHUNK, :], b_col[0:1, :]
            total_f = close_f[:, lanes] + a_end
            ends_f = (last_f[:, lanes] * jnp.exp(a_end - a_col)).astype(BF16)
            ends_b = (last_b[:, lanes] * jnp.exp(b_end - b_col)).astype(BF16)
            ends = t_dot(values[:, lanes], jnp.concatenate([ends_f, ends_b], axis=1))
            starts[i, h, :, :DEPTH] = state[0, h]
            state[0, h] = jnp.exp(total_f) * state[0, h] + ends[:, :DEPTH]
            chunk_state[i, h] = ends[:, DEPTH:]
            chunk_keep[i, :, lanes] = close_b[:, lanes] + b_end
            offset[0, :, lanes] = offset[0, :, lanes] + total_f
        return 0

    lax.fori_loop(0, count, step, 0)

    def descend(i, _):
        c = count - 1 - i
        offsets[1, c] = offset[1]
        for h in range(heads):
            lanes = slice(h * DEPTH, (h + 1) * DEPTH)
            starts[c, h, :, DEPTH:] = state[1, h]
            keep = chunk_keep[c, :, lanes]
            state[1, h] = jnp.exp(keep) * state[1, h] + chunk_state[c, h]
            offset[1, :, lanes] = offset[1, :, lanes] + keep
        return 0

    window = jnp.left_shift(jnp.int32(2), lax.axis_index("tp") * groups)
    sequence, first_row = length * lax.axis_size("sp"), lax.axis_index("sp") * length

    def pooled(owner):
        begin = pl.multiple_of(owner * share, share)
        span = share + 2 * RIM
        near_rows = padded[pl.ds(begin, span), :]
        target = first_row + begin + lax.broadcasted_iota(jnp.int32, (share, span), 0)
        source = first_row + begin - RIM + lax.broadcasted_iota(jnp.int32, (share, span), 1)
        low = target - window // 2
        inside = (source >= low) & (source < low + window) & (source >= 0) & (source < sequence)
        start = first_row + begin + lax.broadcasted_iota(jnp.int32, (share, 1), 0) - window // 2
        number = jnp.minimum(start + window, sequence) - jnp.maximum(start, 0)
        mean = dot(inside.astype(F32).astype(BF16), near_rows) / number.astype(F32)
        here = padded[pl.ds(pl.multiple_of(begin + RIM, RIM), share), :].astype(F32)
        return (dot((mean - here).astype(BF16), mix[0]) * pool_gain[...]).astype(BF16)

    def pool_copy(r):
        return pltpu.make_async_remote_copy(
            passed.at[r], brought.at[me], a_send.at[0], a_recv.at[0],
            device_id={"tp": jnp.int32(r)}, device_id_type=MESH,
        )

    pool_all = pltpu.make_async_remote_copy(
        passed.at[pl.ds(0, 3)], brought.at[pl.ds(0, 3)], a_send.at[0], a_recv.at[0],
        device_id={"tp": sibling}, device_id_type=MESH,
    )

    def pool_away(r):
        if r == 3:
            edge_wait(1, length, padded, e_send, e_recv)
        if r == 0:
            edge_wait(0, length, padded, e_send, e_recv)
        rows = pooled(r)
        passed[r] = rows

        @pl.when(me == r)
        def _():
            brought[r] = rows

        @pl.when(me != r)
        def _():
            pool_copy(r).start()

    def ring_end():
        for e in range(count - 1, events):
            ring_turn(e)

    def drain_gather():
        for block, sem in ((held, t_send), (wfull, w_send)):
            rows = block.at[pl.ds(0, 3)]
            pltpu.make_async_remote_copy(
                rows, rows, sem.at[0], s_recv.at[0],
                device_id={"tp": sibling}, device_id_type=MESH,
            ).wait_send()

    def drain_scan():
        for d in range(2):
            exists, _, _ = partner(d, 1)

            @pl.when(exists)
            def _():
                edge_copy(d, length, padded, e_send, e_recv).wait_send()

        for k in range(steps):
            for d in range(2):
                exists, _, _ = partner(d, strides()[k])

                @pl.when(exists)
                def _():
                    pltpu.make_async_remote_copy(
                        sent.at[k, d], sent.at[k, d], p_send.at[k, d], p_recv.at[k, d, 0],
                        device_id={"tp": sibling}, device_id_type=MESH,
                    ).wait_send()

        pool_all.wait_send()

    def late_last():
        late_pool(count - 1)
        edge_start(0, length, padded, e_send, e_recv)
        late(count - 1)
        local(count - 1)

    tile = 512
    tiles = out.shape[1] // tile

    def wide_pool():
        pltpu.make_async_remote_copy(
            wfull.at[pl.ds(0, 2)], wfull.at[pl.ds(0, 2)], w_send.at[0], q_recv.at[0],
            device_id={"tp": sibling}, device_id_type=MESH,
        ).wait_recv()
        pool_all.wait_recv()
        for j in range(tiles):
            lanes = slice(j * tile, (j + 1) * tile)
            y = dot(brought[0], wfull[0, depth:, lanes])
            for r in range(1, 4):
                y = y + dot(brought[r], wfull[r, depth:, lanes])
            total[:, lanes] = y

    def finished(c, h):
        at, lanes = piece(c), slice(h * DEPTH, (h + 1) * DEPTH)
        ages = jnp.exp(jnp.concatenate([offsets[0, c, :, lanes], offsets[1, c, :, lanes]], axis=1))
        enter = (starts[c, h] + ages * turned[h]).astype(BF16)
        both = inner[at, lanes] + dot_t(reach[h, at, :], enter)
        both = both * lax.rsqrt(jnp.mean(both * both, axis=1, keepdims=True) + EPSILON)
        given[h, at, :] = (both * gated[at, lanes]).astype(BF16)

    relations = (across, opposite, sibling, me)

    def recur_copy(k, h):
        there = relations[k]
        at = pl.ds(pl.multiple_of(there * share, share), share)
        return pltpu.make_async_remote_copy(
            given.at[h, at], taken.at[me, h], c_send.at[0], c_recv.at[heads if k == 2 else h],
            device_id={"tp": there}, device_id_type=MESH,
        )

    def recur_wait(owners, count, h):
        rows = taken.at[pl.ds(0, owners), pl.ds(0, count)]
        return pltpu.make_async_remote_copy(
            rows, rows, c_send.at[0], c_recv.at[h],
            device_id={"tp": sibling}, device_id_type=MESH,
        )

    def away(k, h):
        for sub in range(subs):
            finished(relations[k] * subs + sub, h)
        if k < 3:
            recur_copy(k, h).start()

    scan = (sent, landed, before, before_keep, p_send, p_recv)
    fillers = [
        [late_last, ring_end] + [functools.partial(pool_away, r) for r in (1, 2, 3)],
        [lambda: pool_away(0), drain_gather],
        [wide_pool],
    ]
    first = 1 - lax.rem(lax.axis_index("sp"), 2)
    rounds = [[] for _ in range(max(steps, 1))]
    for i, group in enumerate(fillers):
        rounds[min(i, len(rounds) - 1)].extend(group)
    for k in range(steps):
        if k == 0:
            for h in range(heads):
                scan_start(0, 0, h, state, offset, *scan)
            lax.fori_loop(0, count, descend, 0)
            for h in range(heads):
                scan_start(0, 1, h, state, offset, *scan)
        for h in range(heads if k else 0):
            for d in (first, 1 - first):
                scan_close(k - 1, d, h, *scan)
                scan_start(k, d, h, state, offset, *scan)
        for filler in rounds[k]:
            filler()
    if not steps:
        lax.fori_loop(0, count, descend, 0)
        for filler in rounds[0]:
            filler()
    for h in range(heads):
        for d in range(2):
            if steps:
                scan_close(steps - 1, d, h, *scan)
            lanes = slice(d * DEPTH, (d + 1) * DEPTH)
            keep = before_keep[d, :, h * DEPTH : (h + 1) * DEPTH]
            turned[h, :, lanes] = keep * turned[h, :, lanes] + before[d, h]
        for k in range(2):
            away(k, h)
    for k in (2, 3):
        for h in range(heads):
            away(k, h)

    def all_heads(rows):
        return jnp.concatenate([rows(h) for h in range(heads)], axis=1)

    def far_part(h, lanes):
        rows = slice(h * DEPTH, (h + 1) * DEPTH)
        return dot(
            jnp.concatenate([taken[across, h], taken[opposite, h]], axis=1),
            jnp.concatenate([wfull[across, rows, lanes], wfull[opposite, rows, lanes]], axis=0),
        )

    recur_wait(1, heads, heads).wait_recv()
    home = pl.ds(pl.multiple_of(me * share, share), share)
    for j in range(tiles):
        lanes = slice(j * tile, (j + 1) * tile)
        y = total[:, lanes] + dot(
            all_heads(lambda h: given[h, home, :]), wfull[me, :depth, lanes]
        )
        total[:, lanes] = y + dot(
            all_heads(lambda h: taken[sibling, h]), wfull[sibling, :depth, lanes]
        )
    drain_scan()
    for h in range(heads):
        recur_wait(1, 2, h).wait_recv()
        for j in range(tiles):
            lanes = slice(j * tile, (j + 1) * tile)
            y = total[:, lanes] + far_part(h, lanes)
            if h == heads - 1:
                out[:, lanes] = y.astype(BF16)
            else:
                total[:, lanes] = y

    recur_wait(3, heads, 0).wait_send()


def shards(
    tokens, norm_gain, w_query, w_forget_fwd, w_forget_bwd, w_value, w_gate, w_pool_in,
    forget_gap, added_log_retention, initial_state, head_gain, pool_mix, pool_gain,
    w_out_recur, w_out_pool,
):
    weights = (w_query, w_forget_fwd, w_forget_bwd, w_value, w_gate, w_pool_in)
    length, width = tokens.shape
    features, columns = w_query.shape
    heads = columns // DEPTH
    count = length // CHUNK
    share = length // 4
    subs = share // CHUNK
    depth, out_width = w_out_recur.shape
    steps = len(strides())
    size = ring_size()
    events = size - 1
    dma = pltpu.SemaphoreType.DMA
    operands = (
        tokens, norm_gain[None, :], *weights, forget_gap, added_log_retention.T, initial_state,
        head_gain[None, :], pool_mix, pool_gain[None, :], w_out_recur, w_out_pool,
    )

    def like(array):
        return pltpu.VMEM(array.shape, array.dtype)

    return pl.pallas_call(
        functools.partial(mixer_kernel, pool_mix.shape[0]),
        out_shape=pltpu.VMEM((share, out_width), BF16),
        in_specs=[ANY] * len(operands),
        out_specs=VM,
        scratch_shapes=[
            pltpu.VMEM((4, length, width), BF16),
            like(operands[1]),
            pltpu.VMEM((6, features, columns), BF16),
            like(operands[8]), like(operands[9]), like(operands[10]), like(operands[11]),
            like(operands[12]), like(operands[13]),
            pltpu.VMEM((4, 2 * depth, out_width), BF16),
            pltpu.VMEM((6, length, columns), F32),
            pltpu.VMEM((length, 1), F32),
            pltpu.VMEM((2, count, CHUNK, heads), F32),
            pltpu.VMEM((2, count, heads, CHUNK), F32),
            pltpu.VMEM((heads, DEPTH, 2 * DEPTH), F32),
            pltpu.VMEM((length, columns), BF16),
            pltpu.VMEM((length, columns), BF16),
            pltpu.VMEM((length, columns), F32),
            pltpu.VMEM((2, length, columns), BF16),
            pltpu.VMEM((2, length, columns), F32),
            pltpu.VMEM((length, columns), F32),
            pltpu.VMEM((heads, length, 2 * DEPTH), BF16),
            pltpu.VMEM((count, heads, DEPTH, 2 * DEPTH), F32),
            pltpu.VMEM((2, count, 1, columns), F32),
            pltpu.VMEM((count, heads, DEPTH, DEPTH), F32),
            pltpu.VMEM((count, 1, columns), F32),
            pltpu.VMEM((2, heads, DEPTH, DEPTH), F32),
            pltpu.VMEM((2, 1, columns), F32),
            pltpu.VMEM((length + 2 * RIM, columns), BF16),
            pltpu.VMEM((steps, 2, heads, DEPTH + 16, DEPTH), BF16),
            pltpu.VMEM((steps, 2, heads, DEPTH + 16, DEPTH), BF16),
            pltpu.VMEM((2, heads, DEPTH, DEPTH), F32),
            pltpu.VMEM((2, 1, columns), F32),
            pltpu.VMEM((heads, length, DEPTH), BF16),
            pltpu.VMEM((4, heads, share, DEPTH), BF16),
            pltpu.VMEM((4, share, columns), BF16),
            pltpu.VMEM((4, share, columns), BF16),
            pltpu.VMEM((share, out_width), F32),
            pltpu.VMEM((CHUNK, 2 * width), BF16),
            pltpu.VMEM((CHUNK, 1), F32),
            dma((10,)), dma((1,)), dma((1,)), dma((1,)), dma((count,)), dma((count,)),
            dma((1,)), dma((1,)), dma((events,)),
            dma((steps, 2)), dma((steps, 2, heads)), dma((2,)), dma((2,)),
            dma((1,)), dma((1,)), dma((1,)), dma((heads + 1,)),
        ],
        compiler_params=pltpu.CompilerParams(
            collective_id=0, has_side_effects=True, vmem_limit_bytes=VMEM_LIMIT
        ),
        name="mixer",
    )(*(pltpu.with_memory_space_constraint(x, pltpu.HBM) for x in operands))


def solution(mesh):
    in_specs = (
        P("sp", "tp"), P(), P(None, "tp"), P(None, "tp"), P(None, "tp"), P(None, "tp"),
        P(None, "tp"), P(None, "tp"), P(None, "tp"), P("sp", "tp"), P(None, "tp", None, None),
        P("tp"), P("tp", None, None), P("tp"), P("tp", None), P("tp", None),
    )
    out_specs = P(("sp", "tp"), None)
    return jax.shard_map(shards, mesh=mesh, in_specs=in_specs, out_specs=out_specs, check_vma=False)
```

```python
import functools

import jax
import jax.numpy as jnp
from jax import lax
from jax.experimental import pallas as pl
from jax.experimental.pallas import tpu as pltpu
from jax.sharding import PartitionSpec as P

DEPTH = 128
CHUNK = 128
EPSILON = 1e-06
RIM = 16
RING = 8
GROUP = 4
MESH = pl.DeviceIdType.MESH
F32 = jnp.float32
BF16 = jnp.bfloat16
VMEM_LIMIT = 52 * 1024 * 1024
ANY = pl.BlockSpec(memory_space=pl.ANY)
VM = pl.BlockSpec(memory_space=pltpu.VMEM)
EXACT = lax.Precision.HIGHEST


def dot(a, b, precision=None):
    return jnp.dot(a, b, preferred_element_type=F32, precision=precision)


def dot_t(a, b, precision=None):
    return lax.dot_general(
        a, b, (((1,), (1,)), ((), ())), preferred_element_type=F32, precision=precision
    )


def t_dot(a, b):
    return lax.dot_general(a, b, (((0,), (0,)), ((), ())), preferred_element_type=F32)


def peers():
    me = lax.axis_index("tp")
    sibling = me + 1 - 2 * lax.rem(me, 2)
    across = lax.rem(me + 2, 4)
    return me, sibling, across, lax.rem(sibling + 2, 4)


def partner(d, stride):
    me, count = lax.axis_index("sp"), lax.axis_size("sp")
    above, below = me + stride < count, me >= stride
    return (above, me + stride, below) if d == 0 else (below, me - stride, above)


def group_size():
    return min(GROUP, lax.axis_size("sp"))


def group_strides():
    count = lax.axis_size("sp") // group_size()
    return [1 << k for k in range(count.bit_length()) if 1 << k < count]


def group_place():
    me = lax.axis_index("sp")
    return me // group_size(), lax.rem(me, group_size())


def raw_partner(d, j):
    (_, place), me, size = group_place(), lax.axis_index("sp"), group_size()
    above, below = place + j < size, place >= j
    return (above, me + j, below) if d == 0 else (below, me - j, above)


def group_partner(d, stride):
    (group, place), size = group_place(), group_size()
    count = lax.axis_size("sp") // size
    above, below = group + stride < count, group >= stride
    if d == 0:
        return above & (place == size - 1), group + stride, below
    return below & (place == 0), group - stride, above


def ring_size():
    return min(RING, lax.axis_size("sp"))


def ring_place():
    size = ring_size()
    me = lax.axis_index("sp")
    base, mine = me - lax.rem(me, size), lax.rem(me, size)
    place = jnp.where(lax.rem(mine, 2) == 0, mine // 2, size - 1 - mine // 2)

    def index(spot):
        spot = lax.rem(spot + size, size)
        return base + jnp.where(spot < size // 2, 2 * spot, 2 * (size - 1 - spot) + 1)

    return place, index(place + 1), index(place - 1)


def greet():
    barrier = pltpu.get_barrier_semaphore()
    _, sibling, across, opposite = peers()
    _, right, left = ring_place()
    for device in (sibling, across, opposite):
        pl.semaphore_signal(barrier, inc=1, device_id={"tp": device}, device_id_type=MESH)
    for device in (right, left):
        pl.semaphore_signal(barrier, inc=1, device_id={"sp": device}, device_id_type=MESH)
    size, (group, place) = group_size(), group_place()
    for j in range(1, size):
        target = group * size + lax.rem(place + j, size)
        pl.semaphore_signal(barrier, inc=1, device_id={"sp": target}, device_id_type=MESH)
    number = jnp.int32(5 + size - 1)
    for stride in group_strides():
        for d in range(2):
            sends, _, gets = group_partner(d, stride)
            source = (group - stride) * size + size - 1 if d == 0 else (group + stride) * size

            @pl.when(gets)
            def _():
                pl.semaphore_signal(
                    barrier, inc=1, device_id={"sp": source}, device_id_type=MESH
                )

            number = number + jnp.where(sends, size, 0)
    pl.semaphore_wait(barrier, number)


def edge_copy(d, length, padded, e_send, e_recv):
    _, target, _ = partner(d, 1)
    there = 0 if d == 0 else RIM + length
    return pltpu.make_async_remote_copy(
        padded.at[pl.ds(length if d == 0 else RIM, RIM)], padded.at[pl.ds(there, RIM)],
        e_send.at[d], e_recv.at[d], device_id={"sp": target}, device_id_type=MESH,
    )


def edge_start(d, length, padded, e_send, e_recv):
    exists, _, _ = partner(d, 1)

    @pl.when(exists)
    def _():
        edge_copy(d, length, padded, e_send, e_recv).start()


def edge_wait(d, length, padded, e_send, e_recv):
    _, _, source = partner(d, 1)

    @pl.when(source)
    def _():
        edge_copy(d, length, padded, e_send, e_recv).wait_recv()


def scan_copy(slot, k, d, h, target, sent, landed, p_send, p_recv):
    return pltpu.make_async_remote_copy(
        sent.at[k, d, h], landed.at[slot, d, h], p_send.at[slot, d], p_recv.at[slot, d, h],
        device_id={"sp": target}, device_id_type=MESH,
    )


def scan_start(k, d, h, state, offset, sent, landed, before, before_keep, p_send, p_recv):
    size = group_size()
    if k == 0:
        sends, _, _ = raw_partner(d, 1)
    else:
        sends, group, _ = group_partner(d, group_strides()[k - 1])

    @pl.when(sends)
    def _():
        lanes = slice(h * DEPTH, (h + 1) * DEPTH)
        keep = jnp.exp(offset[d, :, lanes])
        sent[k, d, h, :DEPTH, :] = (keep * before[d, h] + state[d, h]).astype(BF16)
        sent[k, d, h, DEPTH:, :] = jnp.broadcast_to(
            keep * before_keep[d, :, lanes], (16, DEPTH)
        ).astype(BF16)
        if k == 0:
            for j in range(size - 1, 0, -1):
                exists, target, _ = raw_partner(d, j)

                @pl.when(exists)
                def _():
                    scan_copy(j - 1, k, d, h, target, sent, landed, p_send, p_recv).start()
        else:
            for place in range(size - 1, -1, -1) if d == 0 else range(size):
                target = group * size + place
                scan_copy(size + k - 2, k, d, h, target, sent, landed, p_send, p_recv).start()


def scan_close(k, d, h, sent, landed, before, before_keep, p_send, p_recv):
    size = group_size()
    if k == 0:
        arrivals = [(j - 1, *raw_partner(d, j)[1:]) for j in range(1, size)]
    else:
        arrivals = [(size + k - 2, 0, group_partner(d, group_strides()[k - 1])[2])]
    for slot, target, gets in arrivals:
        @pl.when(gets)
        def _():
            scan_copy(slot, k, d, h, target, sent, landed, p_send, p_recv).wait_recv()
            lanes = slice(h * DEPTH, (h + 1) * DEPTH)
            keep = before_keep[d, :, lanes]
            early = landed[slot, d, h].astype(F32)
            before[d, h] = keep * early[:DEPTH] + before[d, h]
            before_keep[d, :, lanes] = keep * early[DEPTH : DEPTH + 1]


def scan_drain(k, d, sent, landed, p_send, p_recv):
    size = group_size()
    if k == 0:
        leaving = [(j - 1, raw_partner(d, j)[0], sent.at[0, d]) for j in range(1, size)]
    else:
        sends = group_partner(d, group_strides()[k - 1])[0]
        leaving = [(size + k - 2, sends, landed.at[pl.ds(0, size // 2)])]
    for slot, sends, block in leaving:
        @pl.when(sends)
        def _():
            pltpu.make_async_remote_copy(
                block, block, p_send.at[slot, d], p_recv.at[slot, d, 0],
                device_id={"sp": 0}, device_id_type=MESH,
            ).wait_send()


def mixer_kernel(groups, *refs):
    (h_tokens, h_gain, *h_weights) = refs[:8]
    (h_gap, h_added, h_initial, h_head, h_mix, h_scale, h_recur, h_pool) = refs[8:16]
    out = refs[16]
    (
        held, gain, wide, gap, added, initial, head_gain, mix, pool_gain, wfull,
        acc, square, cols, rows_of, turned, query_pre, value, gated, ent, runs, inner, reach,
        starts, offsets, chunk_state, chunk_keep, state, offset, padded,
        sent, landed, before, before_keep, given, taken, passed, brought, total, kept_x, kept_scale,
        l_sem, t_send, w_send, s_recv, x_recv, f_recv, w_recv, q_recv, g_recv,
        p_send, p_recv, e_send, e_recv, a_send, a_recv, c_send, c_recv,
    ) = refs[17:]
    me, sibling, across, opposite = peers()
    length, width = held.shape[1:]
    columns = wide.shape[2]
    heads = columns // DEPTH
    count = length // CHUNK
    share = length // 4
    subs = share // CHUNK
    features = 4 * width
    depth = wfull.shape[1] // 2
    steps = 1 + len(group_strides())

    own_w = [
        pltpu.make_async_copy(h_recur, wfull.at[me, pl.ds(0, depth)], l_sem.at[0]),
        pltpu.make_async_copy(h_pool, wfull.at[me, pl.ds(depth, depth)], l_sem.at[0]),
    ]
    own_t = pltpu.make_async_copy(h_tokens, held.at[me], l_sem.at[1])
    small = [
        pltpu.make_async_copy(a, b, l_sem.at[3 + i])
        for i, (a, b) in enumerate((
            (h_gain, gain), (h_gap, gap), (h_added, added), (h_initial, initial),
            (h_head, head_gain), (h_mix, mix), (h_scale, pool_gain),
        ))
    ]
    loads = [
        pltpu.make_async_copy(w, wide.at[i], l_sem.at[2]) for i, w in enumerate(h_weights)
    ]
    for copy in own_w + [own_t] + small + loads:
        copy.start()
    greet()

    size = ring_size()
    slab = 2 * depth // size
    half = slab // 2
    place, right, left = ring_place()
    events = size - 1

    mine = pl.ds(pl.multiple_of(place * slab, slab), slab)
    w_across = pltpu.make_async_remote_copy(
        wfull.at[me, mine], wfull.at[me, mine], w_send.at[0], w_recv.at[0],
        device_id={"tp": across}, device_id_type=MESH,
    )
    w_beside = pltpu.make_async_remote_copy(
        wfull.at[me], wfull.at[me], w_send.at[0], q_recv.at[0],
        device_id={"tp": sibling}, device_id_type=MESH,
    )
    def w_pass(rows):
        return pltpu.make_async_remote_copy(
            wfull.at[across, rows], wfull.at[across, rows], w_send.at[0], q_recv.at[0],
            device_id={"tp": sibling}, device_id_type=MESH,
        )

    def ring_rows(way, e):
        spot = lax.rem(place + (e // 2 if way else size - e // 2), size)
        side = 1 - lax.rem(e, 2) if way else lax.rem(e, 2)
        return pl.ds(pl.multiple_of(spot * slab + side * half, half), half)

    def ring_copy(way, e):
        at = ring_rows(way, e)
        return pltpu.make_async_remote_copy(
            wfull.at[across, at], wfull.at[across, at], w_send.at[0], g_recv.at[e],
            device_id={"sp": left if way else right}, device_id_type=MESH,
        )

    def ring_turn(e):
        landed_slab = wfull.at[across, pl.ds(0, slab)]
        pltpu.make_async_remote_copy(
            landed_slab, landed_slab, w_send.at[0], g_recv.at[e],
            device_id={"sp": right}, device_id_type=MESH,
        ).wait_recv()
        for way in range(2):
            @pl.when(e + 2 < events)
            def _():
                ring_copy(way, e + 2).start()

            w_pass(ring_rows(way, e + 2)).start()

    beside = pltpu.make_async_remote_copy(
        held.at[me], held.at[me], t_send.at[0], s_recv.at[0],
        device_id={"tp": sibling}, device_id_type=MESH,
    )

    def piece(i):
        return pl.ds(pl.multiple_of(i * CHUNK, CHUNK), CHUNK)

    def crossing(i):
        return pltpu.make_async_remote_copy(
            held.at[me, piece(i)], held.at[me, piece(i)], t_send.at[0], x_recv.at[i],
            device_id={"tp": across}, device_id_type=MESH,
        )

    def relay(i):
        return pltpu.make_async_remote_copy(
            held.at[across, piece(i)], held.at[across, piece(i)], t_send.at[0], f_recv.at[i],
            device_id={"tp": sibling}, device_id_type=MESH,
        )

    pltpu.make_async_copy(wfull.at[across], wfull.at[me], l_sem.at[0]).wait()
    w_across.start()
    own_t.wait()
    beside.start()
    for i in range(count):
        crossing(i).start()
    w_beside.start()
    for copy in small:
        copy.wait()

    row = lax.broadcasted_iota(jnp.int32, (CHUNK, CHUNK), 0)
    col = lax.broadcasted_iota(jnp.int32, (CHUNK, CHUNK), 1)
    lower, upper = row >= col, row <= col
    lower_f, upper_f = lower.astype(F32), upper.astype(F32)
    lower_2 = jnp.concatenate([lower_f, lower_f], axis=1).astype(BF16)
    upper_2 = jnp.concatenate([upper_f, upper_f], axis=1).astype(BF16)

    def sums(c, _):
        add = added[:, piece(c)]
        cols[0, c] = dot_t(lower_f, add, EXACT)
        cols[1, c] = dot_t(upper_f, add, EXACT)
        rows_of[0, c] = dot(add, upper_f, EXACT)
        rows_of[1, c] = dot(add, lower_f, EXACT)
        return 0

    lax.fori_loop(0, count, sums, 0)
    for h in range(heads):
        for d in range(2):
            turned[h, :, d * DEPTH : (d + 1) * DEPTH] = initial[d, h].T
    state[...] = jnp.zeros_like(state)
    offset[...] = jnp.zeros_like(offset)
    before[...] = jnp.zeros_like(before)
    before_keep[...] = jnp.ones_like(before_keep)
    for d in range(2):
        _, _, source = partner(d, 1)
        begin = 0 if d == 0 else RIM + length

        @pl.when(jnp.logical_not(source))
        def _():
            padded[pl.ds(begin, RIM), :] = jnp.zeros((RIM, columns), BF16)

    pair = me // 2
    near, far = 2 * pair, 2 - 2 * pair

    def normed(first, at):
        parts, squares = [], 0.0
        for o in range(2):
            x = held[first + o, at, :].astype(F32)
            squares = squares + jnp.sum(x * x, axis=1, keepdims=True)
            lanes = pl.ds(pl.multiple_of((first + o) * width, width), width)
            parts.append((x * gain[:, lanes]).astype(BF16))
        return jnp.concatenate(parts, axis=1), squares

    def depth_of(first):
        return pl.ds(pl.multiple_of(first * width, 2 * width), 2 * width)

    pltpu.make_async_copy(wide, wide, l_sem.at[2]).wait()
    beside.wait_recv()

    def own(i, _):
        at = pl.ds(pl.multiple_of(i * share, share), share)
        x, squares = normed(near, at)
        square[at, :] = squares
        for j in range(6):
            acc[j, at, :] = dot(x, wide[j, depth_of(near), :])
        return 0

    lax.fori_loop(0, 4, own, 0)
    w_across.wait_recv()
    for e in range(min(2, events)):
        for way in range(2):
            ring_copy(way, e).start()
    w_pass(mine).start()

    def gates(pre, gap_row, sums):
        enter = gap_row * (1.0 / (1.0 + jnp.exp(pre)))
        keep = jnp.log1p(-enter)
        high = keep.astype(BF16)
        low = (keep - high.astype(F32)).astype(BF16)
        return enter, dot(sums, jnp.concatenate([high, low], axis=0))

    def local(c):
        at = piece(c)
        x = query_pre[at, :].astype(F32)
        query = x / (1.0 + jnp.exp(-x))
        q_f, q_b = query * jnp.exp(runs[0, at, :]), query * jnp.exp(runs[1, at, :])
        e_f, e_b = ent[0, at, :], ent[1, at, :]
        values = value[at, :]
        col_f, col_b = cols[0, c], cols[1, c]
        row_f, row_b = rows_of[0, c], rows_of[1, c]
        for h in range(heads):
            lanes = slice(h * DEPTH, (h + 1) * DEPTH)
            a_col, b_col = col_f[:, h : h + 1], col_b[:, h : h + 1]
            fade = jnp.exp(
                jnp.where(lower, a_col - row_f[h : h + 1, :], b_col - row_b[h : h + 1, :])
            )
            w_f = dot_t(q_f[:, lanes].astype(BF16), e_f[:, lanes])
            w_b = dot_t(q_b[:, lanes].astype(BF16), e_b[:, lanes])
            weight = (jnp.where(lower, w_f, 0.0) + jnp.where(upper, w_b, 0.0)) * fade
            inner[at, lanes] = dot(weight.astype(BF16), values[:, lanes])
            reach[h, at, :DEPTH] = (q_f[:, lanes] * jnp.exp(a_col)).astype(BF16)
            reach[h, at, DEPTH:] = (q_b[:, lanes] * jnp.exp(b_col)).astype(BF16)

    def project(j, x, scale, at):
        return ((acc[j, at, :] + dot(x, wide[j, depth_of(far), :])) * scale).astype(BF16)

    def late_pool(c):
        rows = project(5, kept_x[...], kept_scale[...], piece(c))
        padded[pl.ds(pl.multiple_of(c * CHUNK + RIM, RIM), CHUNK), :] = rows

    def late(c):
        at, x, scale = piece(c), kept_x[...], kept_scale[...]
        query_pre[at, :] = project(0, x, scale, at)
        gate = project(4, x, scale, at).astype(F32)
        gated[at, :] = head_gain[...] / (1.0 + jnp.exp(-gate))

    def step(i, _):
        at = piece(i)
        crossing(i).wait_recv()
        relay(i).start()

        @pl.when(i > 0)
        def _():
            late_pool(i - 1)
            late(i - 1)
            local(i - 1)

        @pl.when((i > 0) & (i <= events))
        def _():
            ring_turn(i - 1)

        @pl.when(i == 1)
        def _():
            edge_start(1, length, padded, e_send, e_recv)

        relay(i).wait_recv()
        x, squares = normed(far, at)
        scale = lax.rsqrt((square[at, :] + squares) / features + EPSILON)

        kept_x[...], kept_scale[...] = x, scale
        pre_f, pre_b, values = (project(j, x, scale, at) for j in (1, 2, 3))
        value[at, :] = values
        enter_f, run_f = gates(pre_f.astype(F32), gap[0:1, :], lower_2)
        enter_b, run_b = gates(pre_b.astype(F32), gap[1:2, :], upper_2)
        runs[0, at, :], runs[1, at, :] = run_f, run_b
        e_f, e_b = enter_f * jnp.exp(-run_f), enter_b * jnp.exp(-run_b)
        ent[0, at, :], ent[1, at, :] = e_f.astype(BF16), e_b.astype(BF16)
        close_f, close_b = run_f[CHUNK - 1 : CHUNK, :], run_b[0:1, :]
        last_f, last_b = e_f * jnp.exp(close_f), e_b * jnp.exp(close_b)
        offsets[0, i] = offset[0]
        col_f, col_b = cols[0, i], cols[1, i]
        for h in range(heads):
            lanes = slice(h * DEPTH, (h + 1) * DEPTH)
            a_col, b_col = col_f[:, h : h + 1], col_b[:, h : h + 1]
            a_end, b_end = a_col[CHUNK - 1 : CHUNK, :], b_col[0:1, :]
            total_f = close_f[:, lanes] + a_end
            ends_f = (last_f[:, lanes] * jnp.exp(a_end - a_col)).astype(BF16)
            ends_b = (last_b[:, lanes] * jnp.exp(b_end - b_col)).astype(BF16)
            ends = t_dot(values[:, lanes], jnp.concatenate([ends_f, ends_b], axis=1))
            starts[i, h, :, :DEPTH] = state[0, h]
            state[0, h] = jnp.exp(total_f) * state[0, h] + ends[:, :DEPTH]
            chunk_state[i, h] = ends[:, DEPTH:]
            chunk_keep[i, :, lanes] = close_b[:, lanes] + b_end
            offset[0, :, lanes] = offset[0, :, lanes] + total_f
        return 0

    lax.fori_loop(0, count, step, 0)

    def descend(i, _):
        c = count - 1 - i
        offsets[1, c] = offset[1]
        for h in range(heads):
            lanes = slice(h * DEPTH, (h + 1) * DEPTH)
            starts[c, h, :, DEPTH:] = state[1, h]
            keep = chunk_keep[c, :, lanes]
            state[1, h] = jnp.exp(keep) * state[1, h] + chunk_state[c, h]
            offset[1, :, lanes] = offset[1, :, lanes] + keep
        return 0

    window = jnp.left_shift(jnp.int32(2), lax.axis_index("tp") * groups)
    sequence, first_row = length * lax.axis_size("sp"), lax.axis_index("sp") * length

    def pooled(owner):
        begin = pl.multiple_of(owner * share, share)
        span = share + 2 * RIM
        near_rows = padded[pl.ds(begin, span), :]
        target = first_row + begin + lax.broadcasted_iota(jnp.int32, (share, span), 0)
        source = first_row + begin - RIM + lax.broadcasted_iota(jnp.int32, (share, span), 1)
        low = target - window // 2
        inside = (source >= low) & (source < low + window) & (source >= 0) & (source < sequence)
        start = first_row + begin + lax.broadcasted_iota(jnp.int32, (share, 1), 0) - window // 2
        number = jnp.minimum(start + window, sequence) - jnp.maximum(start, 0)
        mean = dot(inside.astype(F32).astype(BF16), near_rows) / number.astype(F32)
        here = padded[pl.ds(pl.multiple_of(begin + RIM, RIM), share), :].astype(F32)
        return (dot((mean - here).astype(BF16), mix[0]) * pool_gain[...]).astype(BF16)

    def pool_copy(r):
        return pltpu.make_async_remote_copy(
            passed.at[r], brought.at[me], a_send.at[0], a_recv.at[0],
            device_id={"tp": jnp.int32(r)}, device_id_type=MESH,
        )

    pool_all = pltpu.make_async_remote_copy(
        passed.at[pl.ds(0, 3)], brought.at[pl.ds(0, 3)], a_send.at[0], a_recv.at[0],
        device_id={"tp": sibling}, device_id_type=MESH,
    )

    def pool_away(r):
        if r == 3:
            edge_wait(1, length, padded, e_send, e_recv)
        if r == 0:
            edge_wait(0, length, padded, e_send, e_recv)
        rows = pooled(r)
        passed[r] = rows

        @pl.when(me == r)
        def _():
            brought[r] = rows

        @pl.when(me != r)
        def _():
            pool_copy(r).start()

    def ring_end():
        for e in range(count - 1, events):
            ring_turn(e)

    def drain_gather():
        for block, sem in ((held, t_send), (wfull, w_send)):
            rows = block.at[pl.ds(0, 3)]
            pltpu.make_async_remote_copy(
                rows, rows, sem.at[0], s_recv.at[0],
                device_id={"tp": sibling}, device_id_type=MESH,
            ).wait_send()

    def drain_scan():
        for d in range(2):
            exists, _, _ = partner(d, 1)

            @pl.when(exists)
            def _():
                edge_copy(d, length, padded, e_send, e_recv).wait_send()

        for k in range(steps):
            for d in range(2):
                scan_drain(k, d, sent, landed, p_send, p_recv)

        pool_all.wait_send()

    def late_last():
        late_pool(count - 1)
        edge_start(0, length, padded, e_send, e_recv)
        late(count - 1)
        local(count - 1)

    tile = 512
    tiles = out.shape[1] // tile

    def wide_pool():
        pltpu.make_async_remote_copy(
            wfull.at[pl.ds(0, 2)], wfull.at[pl.ds(0, 2)], w_send.at[0], q_recv.at[0],
            device_id={"tp": sibling}, device_id_type=MESH,
        ).wait_recv()
        pool_all.wait_recv()
        for j in range(tiles):
            lanes = slice(j * tile, (j + 1) * tile)
            y = dot(brought[0], wfull[0, depth:, lanes])
            for r in range(1, 4):
                y = y + dot(brought[r], wfull[r, depth:, lanes])
            total[:, lanes] = y

    def finished(c, h):
        at, lanes = piece(c), slice(h * DEPTH, (h + 1) * DEPTH)
        ages = jnp.exp(jnp.concatenate([offsets[0, c, :, lanes], offsets[1, c, :, lanes]], axis=1))
        enter = (starts[c, h] + ages * turned[h]).astype(BF16)
        both = inner[at, lanes] + dot_t(reach[h, at, :], enter)
        both = both * lax.rsqrt(jnp.mean(both * both, axis=1, keepdims=True) + EPSILON)
        given[h, at, :] = (both * gated[at, lanes]).astype(BF16)

    relations = (across, opposite, sibling, me)

    def recur_copy(k, h):
        there = relations[k]
        at = pl.ds(pl.multiple_of(there * share, share), share)
        return pltpu.make_async_remote_copy(
            given.at[h, at], taken.at[me, h], c_send.at[0], c_recv.at[heads if k == 2 else h],
            device_id={"tp": there}, device_id_type=MESH,
        )

    def recur_wait(owners, count, h):
        rows = taken.at[pl.ds(0, owners), pl.ds(0, count)]
        return pltpu.make_async_remote_copy(
            rows, rows, c_send.at[0], c_recv.at[h],
            device_id={"tp": sibling}, device_id_type=MESH,
        )

    def away(k, h):
        for sub in range(subs):
            finished(relations[k] * subs + sub, h)
        if k < 3:
            recur_copy(k, h).start()

    scan = (sent, landed, before, before_keep, p_send, p_recv)
    fillers = [
        [late_last, ring_end] + [functools.partial(pool_away, r) for r in (1, 2, 3)],
        [lambda: pool_away(0), drain_gather],
    ]
    rounds = [[] for _ in range(steps)]
    for i, group in enumerate(fillers):
        rounds[min(i, len(rounds) - 1)].extend(group)
    for k in range(steps):
        if k == 0:
            for h in range(heads):
                scan_start(0, 0, h, state, offset, *scan)
            lax.fori_loop(0, count, descend, 0)
            for h in range(heads):
                scan_start(0, 1, h, state, offset, *scan)
        for h in range(heads if k else 0):
            for d in range(2):
                scan_close(k - 1, d, h, *scan)
                scan_start(k, d, h, state, offset, *scan)
        for filler in rounds[k]:
            filler()
    for h in range(heads):
        for d in range(2):
            scan_close(steps - 1, d, h, *scan)
            lanes = slice(d * DEPTH, (d + 1) * DEPTH)
            keep = before_keep[d, :, h * DEPTH : (h + 1) * DEPTH]
            turned[h, :, lanes] = keep * turned[h, :, lanes] + before[d, h]
        for k in range(2):
            away(k, h)
    for k in (2, 3):
        for h in range(heads):
            away(k, h)

    def all_heads(rows):
        return jnp.concatenate([rows(h) for h in range(heads)], axis=1)

    def far_part(h, lanes):
        rows = slice(h * DEPTH, (h + 1) * DEPTH)
        return dot(
            jnp.concatenate([taken[across, h], taken[opposite, h]], axis=1),
            jnp.concatenate([wfull[across, rows, lanes], wfull[opposite, rows, lanes]], axis=0),
        )

    wide_pool()
    recur_wait(1, heads, heads).wait_recv()
    home = pl.ds(pl.multiple_of(me * share, share), share)
    for j in range(tiles):
        lanes = slice(j * tile, (j + 1) * tile)
        y = total[:, lanes] + dot(
            all_heads(lambda h: given[h, home, :]), wfull[me, :depth, lanes]
        )
        total[:, lanes] = y + dot(
            all_heads(lambda h: taken[sibling, h]), wfull[sibling, :depth, lanes]
        )
    drain_scan()
    for h in range(heads):
        recur_wait(1, 2, h).wait_recv()
        for j in range(tiles):
            lanes = slice(j * tile, (j + 1) * tile)
            y = total[:, lanes] + far_part(h, lanes)
            if h == heads - 1:
                out[:, lanes] = y.astype(BF16)
            else:
                total[:, lanes] = y

    recur_wait(3, heads, 0).wait_send()


def shards(
    tokens, norm_gain, w_query, w_forget_fwd, w_forget_bwd, w_value, w_gate, w_pool_in,
    forget_gap, added_log_retention, initial_state, head_gain, pool_mix, pool_gain,
    w_out_recur, w_out_pool,
):
    weights = (w_query, w_forget_fwd, w_forget_bwd, w_value, w_gate, w_pool_in)
    length, width = tokens.shape
    features, columns = w_query.shape
    heads = columns // DEPTH
    count = length // CHUNK
    share = length // 4
    subs = share // CHUNK
    depth, out_width = w_out_recur.shape
    steps = 1 + len(group_strides())
    size = ring_size()
    events = size - 1
    slots = group_size() - 1 + steps - 1
    dma = pltpu.SemaphoreType.DMA
    operands = (
        tokens, norm_gain[None, :], *weights, forget_gap, added_log_retention.T, initial_state,
        head_gain[None, :], pool_mix, pool_gain[None, :], w_out_recur, w_out_pool,
    )

    def like(array):
        return pltpu.VMEM(array.shape, array.dtype)

    return pl.pallas_call(
        functools.partial(mixer_kernel, pool_mix.shape[0]),
        out_shape=pltpu.VMEM((share, out_width), BF16),
        in_specs=[ANY] * len(operands),
        out_specs=VM,
        scratch_shapes=[
            pltpu.VMEM((4, length, width), BF16),
            like(operands[1]),
            pltpu.VMEM((6, features, columns), BF16),
            like(operands[8]), like(operands[9]), like(operands[10]), like(operands[11]),
            like(operands[12]), like(operands[13]),
            pltpu.VMEM((4, 2 * depth, out_width), BF16),
            pltpu.VMEM((6, length, columns), F32),
            pltpu.VMEM((length, 1), F32),
            pltpu.VMEM((2, count, CHUNK, heads), F32),
            pltpu.VMEM((2, count, heads, CHUNK), F32),
            pltpu.VMEM((heads, DEPTH, 2 * DEPTH), F32),
            pltpu.VMEM((length, columns), BF16),
            pltpu.VMEM((length, columns), BF16),
            pltpu.VMEM((length, columns), F32),
            pltpu.VMEM((2, length, columns), BF16),
            pltpu.VMEM((2, length, columns), F32),
            pltpu.VMEM((length, columns), F32),
            pltpu.VMEM((heads, length, 2 * DEPTH), BF16),
            pltpu.VMEM((count, heads, DEPTH, 2 * DEPTH), F32),
            pltpu.VMEM((2, count, 1, columns), F32),
            pltpu.VMEM((count, heads, DEPTH, DEPTH), F32),
            pltpu.VMEM((count, 1, columns), F32),
            pltpu.VMEM((2, heads, DEPTH, DEPTH), F32),
            pltpu.VMEM((2, 1, columns), F32),
            pltpu.VMEM((length + 2 * RIM, columns), BF16),
            pltpu.VMEM((steps, 2, heads, DEPTH + 16, DEPTH), BF16),
            pltpu.VMEM((slots, 2, heads, DEPTH + 16, DEPTH), BF16),
            pltpu.VMEM((2, heads, DEPTH, DEPTH), F32),
            pltpu.VMEM((2, 1, columns), F32),
            pltpu.VMEM((heads, length, DEPTH), BF16),
            pltpu.VMEM((4, heads, share, DEPTH), BF16),
            pltpu.VMEM((4, share, columns), BF16),
            pltpu.VMEM((4, share, columns), BF16),
            pltpu.VMEM((share, out_width), F32),
            pltpu.VMEM((CHUNK, 2 * width), BF16),
            pltpu.VMEM((CHUNK, 1), F32),
            dma((10,)), dma((1,)), dma((1,)), dma((1,)), dma((count,)), dma((count,)),
            dma((1,)), dma((1,)), dma((events,)),
            dma((slots, 2)), dma((slots, 2, heads)), dma((2,)), dma((2,)),
            dma((1,)), dma((1,)), dma((1,)), dma((heads + 1,)),
        ],
        compiler_params=pltpu.CompilerParams(
            collective_id=0, has_side_effects=True, vmem_limit_bytes=VMEM_LIMIT
        ),
        name="mixer",
    )(*(pltpu.with_memory_space_constraint(x, pltpu.HBM) for x in operands))


def solution(mesh):
    in_specs = (
        P("sp", "tp"), P(), P(None, "tp"), P(None, "tp"), P(None, "tp"), P(None, "tp"),
        P(None, "tp"), P(None, "tp"), P(None, "tp"), P("sp", "tp"), P(None, "tp", None, None),
        P("tp"), P("tp", None, None), P("tp"), P("tp", None), P("tp", None),
    )
    out_specs = P(("sp", "tp"), None)
    return jax.shard_map(shards, mesh=mesh, in_specs=in_specs, out_specs=out_specs, check_vma=False)
```

```python
import functools

import jax
import jax.numpy as jnp
from jax import lax
from jax.experimental import pallas as pl
from jax.experimental.pallas import tpu as pltpu
from jax.sharding import PartitionSpec as P

DEPTH = 128
CHUNK = 128
EPSILON = 1e-06
RIM = 16
RING = 8
GROUP = 4
MESH = pl.DeviceIdType.MESH
F32 = jnp.float32
BF16 = jnp.bfloat16
VMEM_LIMIT = 52 * 1024 * 1024
ANY = pl.BlockSpec(memory_space=pl.ANY)
VM = pl.BlockSpec(memory_space=pltpu.VMEM)
EXACT = lax.Precision.HIGHEST


def dot(a, b, precision=None):
    return jnp.dot(a, b, preferred_element_type=F32, precision=precision)


def dot_t(a, b, precision=None):
    return lax.dot_general(
        a, b, (((1,), (1,)), ((), ())), preferred_element_type=F32, precision=precision
    )


def t_dot(a, b):
    return lax.dot_general(a, b, (((0,), (0,)), ((), ())), preferred_element_type=F32)


def peers():
    me = lax.axis_index("tp")
    sibling = me + 1 - 2 * lax.rem(me, 2)
    across = lax.rem(me + 2, 4)
    return me, sibling, across, lax.rem(sibling + 2, 4)


def partner(d, stride):
    me, count = lax.axis_index("sp"), lax.axis_size("sp")
    above, below = me + stride < count, me >= stride
    return (above, me + stride, below) if d == 0 else (below, me - stride, above)


def group_size():
    return min(GROUP, lax.axis_size("sp"))


def group_strides():
    count = lax.axis_size("sp") // group_size()
    return [1 << k for k in range(count.bit_length()) if 1 << k < count]


def group_place():
    me = lax.axis_index("sp")
    return me // group_size(), lax.rem(me, group_size())


def raw_partner(d, j):
    (_, place), me, size = group_place(), lax.axis_index("sp"), group_size()
    above, below = place + j < size, place >= j
    return (above, me + j, below) if d == 0 else (below, me - j, above)


def group_partner(d, stride):
    (group, place), size = group_place(), group_size()
    count = lax.axis_size("sp") // size
    above, below = group + stride < count, group >= stride
    if d == 0:
        return above & (place >= size - 2), group + stride, below
    return below & (place < 2), group - stride, above


def ring_size():
    return min(RING, lax.axis_size("sp"))


def ring_place():
    size = ring_size()
    me = lax.axis_index("sp")
    base, mine = me - lax.rem(me, size), lax.rem(me, size)
    place = jnp.where(lax.rem(mine, 2) == 0, mine // 2, size - 1 - mine // 2)

    def index(spot):
        spot = lax.rem(spot + size, size)
        return base + jnp.where(spot < size // 2, 2 * spot, 2 * (size - 1 - spot) + 1)

    return place, index(place + 1), index(place - 1)


def greet():
    barrier = pltpu.get_barrier_semaphore()
    _, sibling, across, opposite = peers()
    _, right, left = ring_place()
    for device in (sibling, across, opposite):
        pl.semaphore_signal(barrier, inc=1, device_id={"tp": device}, device_id_type=MESH)
    for device in (right, left):
        pl.semaphore_signal(barrier, inc=1, device_id={"sp": device}, device_id_type=MESH)
    size, (group, place) = group_size(), group_place()
    for j in range(1, size):
        target = group * size + lax.rem(place + j, size)
        pl.semaphore_signal(barrier, inc=1, device_id={"sp": target}, device_id_type=MESH)
    number = jnp.int32(5 + size - 1)
    for stride in group_strides():
        for d in range(2):
            sends, _, gets = group_partner(d, stride)
            source = (group - stride) * size + size - 2 if d == 0 else (group + stride) * size
            source = source + lax.rem(place, 2)

            @pl.when(gets)
            def _():
                pl.semaphore_signal(
                    barrier, inc=1, device_id={"sp": source}, device_id_type=MESH
                )

            number = number + jnp.where(sends, size // 2, 0)
    for d in range(2):
        exists, target, _ = partner(d, 1)
        outside = exists & (place == (size - 1 if d == 0 else 0))

        @pl.when(outside)
        def _():
            pl.semaphore_signal(barrier, inc=1, device_id={"sp": target}, device_id_type=MESH)

        number = number + jnp.where(outside, 1, 0)
    pl.semaphore_wait(barrier, number)


def edge_copy(d, length, padded, e_send, e_recv):
    _, target, _ = partner(d, 1)
    there = 0 if d == 0 else RIM + length
    return pltpu.make_async_remote_copy(
        padded.at[pl.ds(length if d == 0 else RIM, RIM)], padded.at[pl.ds(there, RIM)],
        e_send.at[d], e_recv.at[d], device_id={"sp": target}, device_id_type=MESH,
    )


def edge_start(d, length, padded, e_send, e_recv):
    exists, _, _ = partner(d, 1)

    @pl.when(exists)
    def _():
        edge_copy(d, length, padded, e_send, e_recv).start()


def edge_wait(d, length, padded, e_send, e_recv):
    _, _, source = partner(d, 1)

    @pl.when(source)
    def _():
        edge_copy(d, length, padded, e_send, e_recv).wait_recv()


def scan_copy(slot, k, d, h, target, sent, landed, p_send, p_recv):
    return pltpu.make_async_remote_copy(
        sent.at[k, d, h], landed.at[slot, d, h], p_send.at[slot, d], p_recv.at[slot, d, h],
        device_id={"sp": target}, device_id_type=MESH,
    )


def raw_sends(d):
    size, (_, place), me = group_size(), group_place(), lax.axis_index("sp")
    rows = []
    for j in range(size - 1, 0, -1):
        exists, target, _ = raw_partner(d, j)
        rows.append((j - 1, exists, target, place + j >= size - 2 if d == 0 else place - j < 2))
    if d == 0:
        extra = (size - 1, place == size - 1, me - 1, place >= 0)
    else:
        extra = (size - 1, place == 0, me + 1, place >= 0)
    return [extra] + rows


def raw_start(d, h, state, offset, sent, landed, before, before_keep, p_send, p_recv):
    lanes = slice(h * DEPTH, (h + 1) * DEPTH)
    sent[0, d, h, :DEPTH, :] = state[d, h].astype(BF16)
    sent[0, d, h, DEPTH:, :] = jnp.broadcast_to(
        jnp.exp(offset[d, :, lanes]), (16, DEPTH)
    ).astype(BF16)
    for slot, exists, target, boundary in raw_sends(d):
        @pl.when(exists & boundary)
        def _():
            scan_copy(slot, 0, d, h, target, sent, landed, p_send, p_recv).start()


def raw_rest(d, h, sent, landed, before, before_keep, p_send, p_recv):
    for slot, exists, target, boundary in raw_sends(d):
        @pl.when(exists & jnp.logical_not(boundary))
        def _():
            scan_copy(slot, 0, d, h, target, sent, landed, p_send, p_recv).start()


def total_start(k, d, h, state, offset, sent, landed, before, before_keep, p_send, p_recv):
    size, (_, place) = group_size(), group_place()
    sends, group, _ = group_partner(d, group_strides()[k - 1])
    inner = place == (size - 2 if d == 0 else 1)
    lanes = slice(h * DEPTH, (h + 1) * DEPTH)

    def send(values, keep):
        sent[k, d, h, :DEPTH, :] = values.astype(BF16)
        sent[k, d, h, DEPTH:, :] = jnp.broadcast_to(keep, (16, DEPTH)).astype(BF16)
        for pair in range(size // 2 - 1, -1, -1) if d == 0 else range(size // 2):
            target = group * size + 2 * pair + lax.rem(place, 2)
            scan_copy(size + k - 1, k, d, h, target, sent, landed, p_send, p_recv).start()

    @pl.when(sends & jnp.logical_not(inner))
    def _():
        keep = jnp.exp(offset[d, :, lanes])
        send(keep * before[d, h] + state[d, h], keep * before_keep[d, :, lanes])

    @pl.when(sends & inner)
    def _():
        if k == 1:
            scan_copy(size - 1, 0, d, h, 0, sent, landed, p_send, p_recv).wait_recv()
        last = landed[size - 1, d, h].astype(F32)
        keep = jnp.exp(offset[d, :, lanes])
        last_keep = last[DEPTH : DEPTH + 1]
        send(
            last_keep * (keep * before[d, h] + state[d, h]) + last[:DEPTH],
            last_keep * (keep * before_keep[d, :, lanes]),
        )

    if k == 1:
        @pl.when(inner & jnp.logical_not(sends))
        def _():
            scan_copy(size - 1, 0, d, h, 0, sent, landed, p_send, p_recv).wait_recv()


def scan_close(k, d, h, only, sent, landed, before, before_keep, p_send, p_recv):
    size = group_size()
    if k == 0:
        arrivals = [(j - 1, raw_partner(d, j)[2]) for j in range(1, size)]
    else:
        arrivals = [(size + k - 1, group_partner(d, group_strides()[k - 1])[2])]
    for slot, gets in arrivals:
        @pl.when(gets & only)
        def _():
            scan_copy(slot, k, d, h, 0, sent, landed, p_send, p_recv).wait_recv()
            lanes = slice(h * DEPTH, (h + 1) * DEPTH)
            keep = before_keep[d, :, lanes]
            early = landed[slot, d, h].astype(F32)
            before[d, h] = keep * early[:DEPTH] + before[d, h]
            before_keep[d, :, lanes] = keep * early[DEPTH : DEPTH + 1]


def scan_drain(k, d, sent, landed, p_send, p_recv):
    size = group_size()
    if k == 0:
        leaving = [(slot, exists, sent.at[0, d]) for slot, exists, _, _ in raw_sends(d)]
    else:
        sends = group_partner(d, group_strides()[k - 1])[0]
        leaving = [(size + k - 1, sends, landed.at[pl.ds(0, size // 4)])]
    for slot, sends, block in leaving:
        @pl.when(sends)
        def _():
            pltpu.make_async_remote_copy(
                block, block, p_send.at[slot, d], p_recv.at[slot, d, 0],
                device_id={"sp": 0}, device_id_type=MESH,
            ).wait_send()


def mixer_kernel(groups, *refs):
    (h_tokens, h_gain, *h_weights) = refs[:8]
    (h_gap, h_added, h_initial, h_head, h_mix, h_scale, h_recur, h_pool) = refs[8:16]
    out = refs[16]
    (
        held, gain, wide, gap, added, initial, head_gain, mix, pool_gain, wfull,
        acc, square, cols, rows_of, turned, query_pre, value, gated, ent, runs, inner, reach,
        starts, offsets, chunk_state, chunk_keep, state, offset, padded,
        sent, landed, before, before_keep, given, taken, passed, brought, total, kept_x, kept_scale,
        l_sem, t_send, w_send, s_recv, x_recv, f_recv, w_recv, q_recv, g_recv,
        p_send, p_recv, e_send, e_recv, a_send, a_recv, c_send, c_recv,
    ) = refs[17:]
    me, sibling, across, opposite = peers()
    length, width = held.shape[1:]
    columns = wide.shape[2]
    heads = columns // DEPTH
    count = length // CHUNK
    share = length // 4
    subs = share // CHUNK
    features = 4 * width
    depth = wfull.shape[1] // 2
    steps = 1 + len(group_strides())

    own_w = [
        pltpu.make_async_copy(h_recur, wfull.at[me, pl.ds(0, depth)], l_sem.at[0]),
        pltpu.make_async_copy(h_pool, wfull.at[me, pl.ds(depth, depth)], l_sem.at[0]),
    ]
    own_t = pltpu.make_async_copy(h_tokens, held.at[me], l_sem.at[1])
    small = [
        pltpu.make_async_copy(a, b, l_sem.at[3 + i])
        for i, (a, b) in enumerate((
            (h_gain, gain), (h_gap, gap), (h_added, added), (h_initial, initial),
            (h_head, head_gain), (h_mix, mix), (h_scale, pool_gain),
        ))
    ]
    loads = [
        pltpu.make_async_copy(w, wide.at[i], l_sem.at[2]) for i, w in enumerate(h_weights)
    ]
    for copy in own_w + [own_t] + small + loads:
        copy.start()
    greet()

    size = ring_size()
    slab = 2 * depth // size
    half = slab // 2
    place, right, left = ring_place()
    events = size - 1

    mine = pl.ds(pl.multiple_of(place * slab, slab), slab)
    w_across = pltpu.make_async_remote_copy(
        wfull.at[me, mine], wfull.at[me, mine], w_send.at[0], w_recv.at[0],
        device_id={"tp": across}, device_id_type=MESH,
    )
    w_beside = pltpu.make_async_remote_copy(
        wfull.at[me], wfull.at[me], w_send.at[0], q_recv.at[0],
        device_id={"tp": sibling}, device_id_type=MESH,
    )
    def w_pass(rows):
        return pltpu.make_async_remote_copy(
            wfull.at[across, rows], wfull.at[across, rows], w_send.at[0], q_recv.at[0],
            device_id={"tp": sibling}, device_id_type=MESH,
        )

    def ring_rows(way, e):
        spot = lax.rem(place + (e // 2 if way else size - e // 2), size)
        side = 1 - lax.rem(e, 2) if way else lax.rem(e, 2)
        return pl.ds(pl.multiple_of(spot * slab + side * half, half), half)

    def ring_copy(way, e):
        at = ring_rows(way, e)
        return pltpu.make_async_remote_copy(
            wfull.at[across, at], wfull.at[across, at], w_send.at[0], g_recv.at[e],
            device_id={"sp": left if way else right}, device_id_type=MESH,
        )

    def ring_turn(e):
        landed_slab = wfull.at[across, pl.ds(0, slab)]
        pltpu.make_async_remote_copy(
            landed_slab, landed_slab, w_send.at[0], g_recv.at[e],
            device_id={"sp": right}, device_id_type=MESH,
        ).wait_recv()
        for way in range(2):
            @pl.when(e + 2 < events)
            def _():
                ring_copy(way, e + 2).start()

            w_pass(ring_rows(way, e + 2)).start()

    beside = pltpu.make_async_remote_copy(
        held.at[me], held.at[me], t_send.at[0], s_recv.at[0],
        device_id={"tp": sibling}, device_id_type=MESH,
    )

    def piece(i):
        return pl.ds(pl.multiple_of(i * CHUNK, CHUNK), CHUNK)

    def crossing(i):
        return pltpu.make_async_remote_copy(
            held.at[me, piece(i)], held.at[me, piece(i)], t_send.at[0], x_recv.at[i],
            device_id={"tp": across}, device_id_type=MESH,
        )

    def relay(i):
        return pltpu.make_async_remote_copy(
            held.at[across, piece(i)], held.at[across, piece(i)], t_send.at[0], f_recv.at[i],
            device_id={"tp": sibling}, device_id_type=MESH,
        )

    pltpu.make_async_copy(wfull.at[across], wfull.at[me], l_sem.at[0]).wait()
    w_across.start()
    own_t.wait()
    beside.start()
    for i in range(count):
        crossing(i).start()
    w_beside.start()
    for copy in small:
        copy.wait()

    row = lax.broadcasted_iota(jnp.int32, (CHUNK, CHUNK), 0)
    col = lax.broadcasted_iota(jnp.int32, (CHUNK, CHUNK), 1)
    lower, upper = row >= col, row <= col
    lower_f, upper_f = lower.astype(F32), upper.astype(F32)
    lower_2 = jnp.concatenate([lower_f, lower_f], axis=1).astype(BF16)
    upper_2 = jnp.concatenate([upper_f, upper_f], axis=1).astype(BF16)

    def sums(c, _):
        add = added[:, piece(c)]
        cols[0, c] = dot_t(lower_f, add, EXACT)
        cols[1, c] = dot_t(upper_f, add, EXACT)
        rows_of[0, c] = dot(add, upper_f, EXACT)
        rows_of[1, c] = dot(add, lower_f, EXACT)
        return 0

    lax.fori_loop(0, count, sums, 0)
    for h in range(heads):
        for d in range(2):
            turned[h, :, d * DEPTH : (d + 1) * DEPTH] = initial[d, h].T
    state[...] = jnp.zeros_like(state)
    offset[...] = jnp.zeros_like(offset)
    before[...] = jnp.zeros_like(before)
    before_keep[...] = jnp.ones_like(before_keep)
    for d in range(2):
        _, _, source = partner(d, 1)
        begin = 0 if d == 0 else RIM + length

        @pl.when(jnp.logical_not(source))
        def _():
            padded[pl.ds(begin, RIM), :] = jnp.zeros((RIM, columns), BF16)

    pair = me // 2
    near, far = 2 * pair, 2 - 2 * pair

    def normed(first, at):
        parts, squares = [], 0.0
        for o in range(2):
            x = held[first + o, at, :].astype(F32)
            squares = squares + jnp.sum(x * x, axis=1, keepdims=True)
            lanes = pl.ds(pl.multiple_of((first + o) * width, width), width)
            parts.append((x * gain[:, lanes]).astype(BF16))
        return jnp.concatenate(parts, axis=1), squares

    def depth_of(first):
        return pl.ds(pl.multiple_of(first * width, 2 * width), 2 * width)

    pltpu.make_async_copy(wide, wide, l_sem.at[2]).wait()
    beside.wait_recv()

    def own(i, _):
        at = pl.ds(pl.multiple_of(i * share, share), share)
        x, squares = normed(near, at)
        square[at, :] = squares
        for j in range(6):
            acc[j, at, :] = dot(x, wide[j, depth_of(near), :])
        return 0

    lax.fori_loop(0, 4, own, 0)
    w_across.wait_recv()
    for e in range(min(2, events)):
        for way in range(2):
            ring_copy(way, e).start()
    w_pass(mine).start()

    def gates(pre, gap_row, sums):
        enter = gap_row * (1.0 / (1.0 + jnp.exp(pre)))
        keep = jnp.log1p(-enter)
        high = keep.astype(BF16)
        low = (keep - high.astype(F32)).astype(BF16)
        return enter, dot(sums, jnp.concatenate([high, low], axis=0))

    def local(c):
        at = piece(c)
        x = query_pre[at, :].astype(F32)
        query = x / (1.0 + jnp.exp(-x))
        q_f, q_b = query * jnp.exp(runs[0, at, :]), query * jnp.exp(runs[1, at, :])
        e_f, e_b = ent[0, at, :], ent[1, at, :]
        values = value[at, :]
        col_f, col_b = cols[0, c], cols[1, c]
        row_f, row_b = rows_of[0, c], rows_of[1, c]
        for h in range(heads):
            lanes = slice(h * DEPTH, (h + 1) * DEPTH)
            a_col, b_col = col_f[:, h : h + 1], col_b[:, h : h + 1]
            fade = jnp.exp(
                jnp.where(lower, a_col - row_f[h : h + 1, :], b_col - row_b[h : h + 1, :])
            )
            w_f = dot_t(q_f[:, lanes].astype(BF16), e_f[:, lanes])
            w_b = dot_t(q_b[:, lanes].astype(BF16), e_b[:, lanes])
            weight = (jnp.where(lower, w_f, 0.0) + jnp.where(upper, w_b, 0.0)) * fade
            inner[at, lanes] = dot(weight.astype(BF16), values[:, lanes])
            reach[h, at, :DEPTH] = (q_f[:, lanes] * jnp.exp(a_col)).astype(BF16)
            reach[h, at, DEPTH:] = (q_b[:, lanes] * jnp.exp(b_col)).astype(BF16)

    def project(j, x, scale, at):
        return ((acc[j, at, :] + dot(x, wide[j, depth_of(far), :])) * scale).astype(BF16)

    def late_pool(c):
        rows = project(5, kept_x[...], kept_scale[...], piece(c))
        padded[pl.ds(pl.multiple_of(c * CHUNK + RIM, RIM), CHUNK), :] = rows

    def late(c):
        at, x, scale = piece(c), kept_x[...], kept_scale[...]
        query_pre[at, :] = project(0, x, scale, at)
        gate = project(4, x, scale, at).astype(F32)
        gated[at, :] = head_gain[...] / (1.0 + jnp.exp(-gate))

    def step(i, _):
        at = piece(i)
        crossing(i).wait_recv()
        relay(i).start()

        @pl.when(i > 0)
        def _():
            late_pool(i - 1)
            late(i - 1)
            local(i - 1)

        @pl.when((i > 0) & (i <= events))
        def _():
            ring_turn(i - 1)

        @pl.when(i == 1)
        def _():
            edge_start(1, length, padded, e_send, e_recv)

        relay(i).wait_recv()
        x, squares = normed(far, at)
        scale = lax.rsqrt((square[at, :] + squares) / features + EPSILON)

        kept_x[...], kept_scale[...] = x, scale
        pre_f, pre_b, values = (project(j, x, scale, at) for j in (1, 2, 3))
        value[at, :] = values
        enter_f, run_f = gates(pre_f.astype(F32), gap[0:1, :], lower_2)
        enter_b, run_b = gates(pre_b.astype(F32), gap[1:2, :], upper_2)
        runs[0, at, :], runs[1, at, :] = run_f, run_b
        e_f, e_b = enter_f * jnp.exp(-run_f), enter_b * jnp.exp(-run_b)
        ent[0, at, :], ent[1, at, :] = e_f.astype(BF16), e_b.astype(BF16)
        close_f, close_b = run_f[CHUNK - 1 : CHUNK, :], run_b[0:1, :]
        last_f, last_b = e_f * jnp.exp(close_f), e_b * jnp.exp(close_b)
        offsets[0, i] = offset[0]
        col_f, col_b = cols[0, i], cols[1, i]
        for h in range(heads):
            lanes = slice(h * DEPTH, (h + 1) * DEPTH)
            a_col, b_col = col_f[:, h : h + 1], col_b[:, h : h + 1]
            a_end, b_end = a_col[CHUNK - 1 : CHUNK, :], b_col[0:1, :]
            total_f = close_f[:, lanes] + a_end
            ends_f = (last_f[:, lanes] * jnp.exp(a_end - a_col)).astype(BF16)
            ends_b = (last_b[:, lanes] * jnp.exp(b_end - b_col)).astype(BF16)
            ends = t_dot(values[:, lanes], jnp.concatenate([ends_f, ends_b], axis=1))
            starts[i, h, :, :DEPTH] = state[0, h]
            state[0, h] = jnp.exp(total_f) * state[0, h] + ends[:, :DEPTH]
            chunk_state[i, h] = ends[:, DEPTH:]
            chunk_keep[i, :, lanes] = close_b[:, lanes] + b_end
            offset[0, :, lanes] = offset[0, :, lanes] + total_f
        return 0

    lax.fori_loop(0, count, step, 0)

    def descend(i, _):
        c = count - 1 - i
        offsets[1, c] = offset[1]
        for h in range(heads):
            lanes = slice(h * DEPTH, (h + 1) * DEPTH)
            starts[c, h, :, DEPTH:] = state[1, h]
            keep = chunk_keep[c, :, lanes]
            state[1, h] = jnp.exp(keep) * state[1, h] + chunk_state[c, h]
            offset[1, :, lanes] = offset[1, :, lanes] + keep
        return 0

    window = jnp.left_shift(jnp.int32(2), lax.axis_index("tp") * groups)
    sequence, first_row = length * lax.axis_size("sp"), lax.axis_index("sp") * length

    def pooled(owner):
        begin = pl.multiple_of(owner * share, share)
        span = share + 2 * RIM
        near_rows = padded[pl.ds(begin, span), :]
        target = first_row + begin + lax.broadcasted_iota(jnp.int32, (share, span), 0)
        source = first_row + begin - RIM + lax.broadcasted_iota(jnp.int32, (share, span), 1)
        low = target - window // 2
        inside = (source >= low) & (source < low + window) & (source >= 0) & (source < sequence)
        start = first_row + begin + lax.broadcasted_iota(jnp.int32, (share, 1), 0) - window // 2
        number = jnp.minimum(start + window, sequence) - jnp.maximum(start, 0)
        mean = dot(inside.astype(F32).astype(BF16), near_rows) / number.astype(F32)
        here = padded[pl.ds(pl.multiple_of(begin + RIM, RIM), share), :].astype(F32)
        return (dot((mean - here).astype(BF16), mix[0]) * pool_gain[...]).astype(BF16)

    def pool_copy(r):
        return pltpu.make_async_remote_copy(
            passed.at[r], brought.at[me], a_send.at[0], a_recv.at[0],
            device_id={"tp": jnp.int32(r)}, device_id_type=MESH,
        )

    pool_all = pltpu.make_async_remote_copy(
        passed.at[pl.ds(0, 3)], brought.at[pl.ds(0, 3)], a_send.at[0], a_recv.at[0],
        device_id={"tp": sibling}, device_id_type=MESH,
    )

    def pool_away(r):
        if r == 3:
            edge_wait(1, length, padded, e_send, e_recv)
        if r == 0:
            edge_wait(0, length, padded, e_send, e_recv)
        rows = pooled(r)
        passed[r] = rows

        @pl.when(me == r)
        def _():
            brought[r] = rows

        @pl.when(me != r)
        def _():
            pool_copy(r).start()

    def ring_end():
        for e in range(count - 1, events):
            ring_turn(e)

    def drain_gather():
        for block, sem in ((held, t_send), (wfull, w_send)):
            rows = block.at[pl.ds(0, 3)]
            pltpu.make_async_remote_copy(
                rows, rows, sem.at[0], s_recv.at[0],
                device_id={"tp": sibling}, device_id_type=MESH,
            ).wait_send()

    def drain_scan():
        for d in range(2):
            exists, _, _ = partner(d, 1)

            @pl.when(exists)
            def _():
                edge_copy(d, length, padded, e_send, e_recv).wait_send()

        for k in range(steps):
            for d in range(2):
                scan_drain(k, d, sent, landed, p_send, p_recv)

        pool_all.wait_send()

    def late_last():
        late(count - 1)
        local(count - 1)

    tile = 512
    tiles = out.shape[1] // tile

    def wide_pool():
        pltpu.make_async_remote_copy(
            wfull.at[pl.ds(0, 2)], wfull.at[pl.ds(0, 2)], w_send.at[0], q_recv.at[0],
            device_id={"tp": sibling}, device_id_type=MESH,
        ).wait_recv()
        pool_all.wait_recv()
        for j in range(tiles):
            lanes = slice(j * tile, (j + 1) * tile)
            y = dot(brought[0], wfull[0, depth:, lanes])
            for r in range(1, 4):
                y = y + dot(brought[r], wfull[r, depth:, lanes])
            total[:, lanes] = y

    def finished(c, h):
        at, lanes = piece(c), slice(h * DEPTH, (h + 1) * DEPTH)
        ages = jnp.exp(jnp.concatenate([offsets[0, c, :, lanes], offsets[1, c, :, lanes]], axis=1))
        enter = (starts[c, h] + ages * turned[h]).astype(BF16)
        both = inner[at, lanes] + dot_t(reach[h, at, :], enter)
        both = both * lax.rsqrt(jnp.mean(both * both, axis=1, keepdims=True) + EPSILON)
        given[h, at, :] = (both * gated[at, lanes]).astype(BF16)

    relations = (across, opposite, sibling, me)

    def recur_copy(k, h):
        there = relations[k]
        at = pl.ds(pl.multiple_of(there * share, share), share)
        return pltpu.make_async_remote_copy(
            given.at[h, at], taken.at[me, h], c_send.at[0], c_recv.at[heads if k == 2 else h],
            device_id={"tp": there}, device_id_type=MESH,
        )

    def recur_wait(owners, count, h):
        rows = taken.at[pl.ds(0, owners), pl.ds(0, count)]
        return pltpu.make_async_remote_copy(
            rows, rows, c_send.at[0], c_recv.at[h],
            device_id={"tp": sibling}, device_id_type=MESH,
        )

    def away(k, h):
        for sub in range(subs):
            finished(relations[k] * subs + sub, h)
        if k < 3:
            recur_copy(k, h).start()

    scan = (sent, landed, before, before_keep, p_send, p_recv)
    place_in_group = group_place()[1]
    always = place_in_group >= 0
    leads = (place_in_group >= group_size() // 2, place_in_group < group_size() // 2)

    def close_rest():
        for h in range(heads):
            for d in range(2):
                scan_close(0, d, h, leads[1 - d] if steps > 1 else always, *scan)

    fillers = [
        [late_last, ring_end] + [functools.partial(pool_away, r) for r in (1, 2, 3)]
        + ([] if steps > 1 else [lambda: pool_away(0), close_rest, drain_gather]),
        [close_rest, drain_gather] if steps > 1 else [],
    ]
    rounds = [[] for _ in range(steps)]
    for i, group in enumerate(fillers):
        rounds[min(i, len(rounds) - 1)].extend(group)
    for k in range(steps):
        if k == 0:
            raw_start(0, 0, state, offset, *scan)
            lax.fori_loop(0, count, descend, 0)
            raw_start(1, 0, state, offset, *scan)
            late_pool(count - 1)
            edge_start(0, length, padded, e_send, e_recv)
            for h in range(1, heads):
                for d in range(2):
                    raw_start(d, h, state, offset, *scan)
            for h in range(heads):
                for d in range(2):
                    raw_rest(d, h, *scan)
        for h in range(heads if k else 0):
            for d in range(2):
                scan_close(k - 1, d, h, leads[d] if k == 1 else always, *scan)
            for d in range(2):
                total_start(k, d, h, state, offset, *scan)
            if k == 1 and h == 0:
                pool_away(0)
        for filler in rounds[k]:
            filler()
    for h in range(heads):
        for d in range(2):
            scan_close(steps - 1, d, h, always, *scan)
            lanes = slice(d * DEPTH, (d + 1) * DEPTH)
            keep = before_keep[d, :, h * DEPTH : (h + 1) * DEPTH]
            turned[h, :, lanes] = keep * turned[h, :, lanes] + before[d, h]
        for k in range(2):
            away(k, h)
    for k in (2, 3):
        for h in range(heads):
            away(k, h)

    def all_heads(rows):
        return jnp.concatenate([rows(h) for h in range(heads)], axis=1)

    def far_part(h, lanes):
        rows = slice(h * DEPTH, (h + 1) * DEPTH)
        return dot(
            jnp.concatenate([taken[across, h], taken[opposite, h]], axis=1),
            jnp.concatenate([wfull[across, rows, lanes], wfull[opposite, rows, lanes]], axis=0),
        )

    wide_pool()
    recur_wait(1, heads, heads).wait_recv()
    home = pl.ds(pl.multiple_of(me * share, share), share)
    for j in range(tiles):
        lanes = slice(j * tile, (j + 1) * tile)
        y = total[:, lanes] + dot(
            all_heads(lambda h: given[h, home, :]), wfull[me, :depth, lanes]
        )
        total[:, lanes] = y + dot(
            all_heads(lambda h: taken[sibling, h]), wfull[sibling, :depth, lanes]
        )
    drain_scan()
    for h in range(heads):
        recur_wait(1, 2, h).wait_recv()
        for j in range(tiles):
            lanes = slice(j * tile, (j + 1) * tile)
            y = total[:, lanes] + far_part(h, lanes)
            if h == heads - 1:
                out[:, lanes] = y.astype(BF16)
            else:
                total[:, lanes] = y

    recur_wait(3, heads, 0).wait_send()


def shards(
    tokens, norm_gain, w_query, w_forget_fwd, w_forget_bwd, w_value, w_gate, w_pool_in,
    forget_gap, added_log_retention, initial_state, head_gain, pool_mix, pool_gain,
    w_out_recur, w_out_pool,
):
    weights = (w_query, w_forget_fwd, w_forget_bwd, w_value, w_gate, w_pool_in)
    length, width = tokens.shape
    features, columns = w_query.shape
    heads = columns // DEPTH
    count = length // CHUNK
    share = length // 4
    subs = share // CHUNK
    depth, out_width = w_out_recur.shape
    steps = 1 + len(group_strides())
    size = ring_size()
    events = size - 1
    slots = group_size() + steps - 1
    dma = pltpu.SemaphoreType.DMA
    operands = (
        tokens, norm_gain[None, :], *weights, forget_gap, added_log_retention.T, initial_state,
        head_gain[None, :], pool_mix, pool_gain[None, :], w_out_recur, w_out_pool,
    )

    def like(array):
        return pltpu.VMEM(array.shape, array.dtype)

    return pl.pallas_call(
        functools.partial(mixer_kernel, pool_mix.shape[0]),
        out_shape=pltpu.VMEM((share, out_width), BF16),
        in_specs=[ANY] * len(operands),
        out_specs=VM,
        scratch_shapes=[
            pltpu.VMEM((4, length, width), BF16),
            like(operands[1]),
            pltpu.VMEM((6, features, columns), BF16),
            like(operands[8]), like(operands[9]), like(operands[10]), like(operands[11]),
            like(operands[12]), like(operands[13]),
            pltpu.VMEM((4, 2 * depth, out_width), BF16),
            pltpu.VMEM((6, length, columns), F32),
            pltpu.VMEM((length, 1), F32),
            pltpu.VMEM((2, count, CHUNK, heads), F32),
            pltpu.VMEM((2, count, heads, CHUNK), F32),
            pltpu.VMEM((heads, DEPTH, 2 * DEPTH), F32),
            pltpu.VMEM((length, columns), BF16),
            pltpu.VMEM((length, columns), BF16),
            pltpu.VMEM((length, columns), F32),
            pltpu.VMEM((2, length, columns), BF16),
            pltpu.VMEM((2, length, columns), F32),
            pltpu.VMEM((length, columns), F32),
            pltpu.VMEM((heads, length, 2 * DEPTH), BF16),
            pltpu.VMEM((count, heads, DEPTH, 2 * DEPTH), F32),
            pltpu.VMEM((2, count, 1, columns), F32),
            pltpu.VMEM((count, heads, DEPTH, DEPTH), F32),
            pltpu.VMEM((count, 1, columns), F32),
            pltpu.VMEM((2, heads, DEPTH, DEPTH), F32),
            pltpu.VMEM((2, 1, columns), F32),
            pltpu.VMEM((length + 2 * RIM, columns), BF16),
            pltpu.VMEM((steps, 2, heads, DEPTH + 16, DEPTH), BF16),
            pltpu.VMEM((slots, 2, heads, DEPTH + 16, DEPTH), BF16),
            pltpu.VMEM((2, heads, DEPTH, DEPTH), F32),
            pltpu.VMEM((2, 1, columns), F32),
            pltpu.VMEM((heads, length, DEPTH), BF16),
            pltpu.VMEM((4, heads, share, DEPTH), BF16),
            pltpu.VMEM((4, share, columns), BF16),
            pltpu.VMEM((4, share, columns), BF16),
            pltpu.VMEM((share, out_width), F32),
            pltpu.VMEM((CHUNK, 2 * width), BF16),
            pltpu.VMEM((CHUNK, 1), F32),
            dma((10,)), dma((1,)), dma((1,)), dma((1,)), dma((count,)), dma((count,)),
            dma((1,)), dma((1,)), dma((events,)),
            dma((slots, 2)), dma((slots, 2, heads)), dma((2,)), dma((2,)),
            dma((1,)), dma((1,)), dma((1,)), dma((heads + 1,)),
        ],
        compiler_params=pltpu.CompilerParams(
            collective_id=0, has_side_effects=True, vmem_limit_bytes=VMEM_LIMIT
        ),
        name="mixer",
    )(*(pltpu.with_memory_space_constraint(x, pltpu.HBM) for x in operands))


def solution(mesh):
    in_specs = (
        P("sp", "tp"), P(), P(None, "tp"), P(None, "tp"), P(None, "tp"), P(None, "tp"),
        P(None, "tp"), P(None, "tp"), P(None, "tp"), P("sp", "tp"), P(None, "tp", None, None),
        P("tp"), P("tp", None, None), P("tp"), P("tp", None), P("tp", None),
    )
    out_specs = P(("sp", "tp"), None)
    return jax.shard_map(shards, mesh=mesh, in_specs=in_specs, out_specs=out_specs, check_vma=False)
```

```python
import functools

import jax
import jax.numpy as jnp
from jax import lax
from jax.experimental import pallas as pl
from jax.experimental.pallas import tpu as pltpu
from jax.sharding import PartitionSpec as P

DEPTH = 128
CHUNK = 128
EPSILON = 1e-06
RIM = 16
RING = 8
GROUP = 4
MESH = pl.DeviceIdType.MESH
F32 = jnp.float32
BF16 = jnp.bfloat16
VMEM_LIMIT = 52 * 1024 * 1024
ANY = pl.BlockSpec(memory_space=pl.ANY)
VM = pl.BlockSpec(memory_space=pltpu.VMEM)
EXACT = lax.Precision.HIGHEST


def dot(a, b, precision=None):
    return jnp.dot(a, b, preferred_element_type=F32, precision=precision)


def dot_t(a, b, precision=None):
    return lax.dot_general(
        a, b, (((1,), (1,)), ((), ())), preferred_element_type=F32, precision=precision
    )


def t_dot(a, b):
    return lax.dot_general(a, b, (((0,), (0,)), ((), ())), preferred_element_type=F32)


def peers():
    me = lax.axis_index("tp")
    sibling = me + 1 - 2 * lax.rem(me, 2)
    across = lax.rem(me + 2, 4)
    return me, sibling, across, lax.rem(sibling + 2, 4)


def partner(d, stride):
    me, count = lax.axis_index("sp"), lax.axis_size("sp")
    above, below = me + stride < count, me >= stride
    return (above, me + stride, below) if d == 0 else (below, me - stride, above)


def group_size():
    return min(GROUP, lax.axis_size("sp"))


def group_strides():
    count = lax.axis_size("sp") // group_size()
    return [1 << k for k in range(count.bit_length()) if 1 << k < count]


def group_place():
    me = lax.axis_index("sp")
    return me // group_size(), lax.rem(me, group_size())


def raw_partner(d, j):
    (_, place), me, size = group_place(), lax.axis_index("sp"), group_size()
    above, below = place + j < size, place >= j
    return (above, me + j, below) if d == 0 else (below, me - j, above)


def group_partner(d, stride):
    (group, place), size = group_place(), group_size()
    count = lax.axis_size("sp") // size
    above, below = group + stride < count, group >= stride
    if d == 0:
        return above & (place >= size - 2), group + stride, below
    return below & (place < 2), group - stride, above


def ring_size():
    return min(RING, lax.axis_size("sp"))


def ring_place():
    size = ring_size()
    me = lax.axis_index("sp")
    base, mine = me - lax.rem(me, size), lax.rem(me, size)
    place = jnp.where(lax.rem(mine, 2) == 0, mine // 2, size - 1 - mine // 2)

    def index(spot):
        spot = lax.rem(spot + size, size)
        return base + jnp.where(spot < size // 2, 2 * spot, 2 * (size - 1 - spot) + 1)

    return place, index(place + 1), index(place - 1)


def greet():
    barrier = pltpu.get_barrier_semaphore()
    _, sibling, across, opposite = peers()
    _, right, left = ring_place()
    for device in (sibling, across, opposite):
        pl.semaphore_signal(barrier, inc=1, device_id={"tp": device}, device_id_type=MESH)
    for device in (right, left):
        pl.semaphore_signal(barrier, inc=1, device_id={"sp": device}, device_id_type=MESH)
    size, (group, place) = group_size(), group_place()
    for j in range(1, size):
        target = group * size + lax.rem(place + j, size)
        pl.semaphore_signal(barrier, inc=1, device_id={"sp": target}, device_id_type=MESH)
    number = jnp.int32(5 + size - 1)
    for stride in group_strides():
        for d in range(2):
            sends, _, gets = group_partner(d, stride)
            source = (group - stride) * size + size - 2 if d == 0 else (group + stride) * size
            source = source + lax.rem(place, 2)

            @pl.when(gets)
            def _():
                pl.semaphore_signal(
                    barrier, inc=1, device_id={"sp": source}, device_id_type=MESH
                )

            number = number + jnp.where(sends, size // 2, 0)
    for d in range(2):
        exists, target, _ = partner(d, 1)
        outside = exists & (place == (size - 1 if d == 0 else 0))

        @pl.when(outside)
        def _():
            pl.semaphore_signal(barrier, inc=1, device_id={"sp": target}, device_id_type=MESH)

        number = number + jnp.where(outside, 1, 0)
    pl.semaphore_wait(barrier, number)


def edge_copy(d, length, padded, e_send, e_recv):
    _, target, _ = partner(d, 1)
    there = 0 if d == 0 else RIM + length
    return pltpu.make_async_remote_copy(
        padded.at[pl.ds(length if d == 0 else RIM, RIM)], padded.at[pl.ds(there, RIM)],
        e_send.at[d], e_recv.at[d], device_id={"sp": target}, device_id_type=MESH,
    )


def edge_start(d, length, padded, e_send, e_recv):
    exists, _, _ = partner(d, 1)

    @pl.when(exists)
    def _():
        edge_copy(d, length, padded, e_send, e_recv).start()


def edge_wait(d, length, padded, e_send, e_recv):
    _, _, source = partner(d, 1)

    @pl.when(source)
    def _():
        edge_copy(d, length, padded, e_send, e_recv).wait_recv()


def scan_copy(slot, k, d, h, target, sent, landed, p_send, p_recv):
    return pltpu.make_async_remote_copy(
        sent.at[k, d, h], landed.at[slot, d, h], p_send.at[slot, d], p_recv.at[slot, d, h],
        device_id={"sp": target}, device_id_type=MESH,
    )


def raw_sends(d):
    size, (_, place), me = group_size(), group_place(), lax.axis_index("sp")
    rows = []
    for j in range(size - 1, 0, -1):
        exists, target, _ = raw_partner(d, j)
        rows.append((j - 1, exists, target, place + j >= size - 2 if d == 0 else place - j < 2))
    if d == 0:
        extra = (size - 1, place == size - 1, me - 1, place >= 0)
    else:
        extra = (size - 1, place == 0, me + 1, place >= 0)
    return [extra] + rows


def raw_start(d, h, state, offset, sent, landed, before, before_keep, p_send, p_recv):
    lanes = slice(h * DEPTH, (h + 1) * DEPTH)
    sent[0, d, h, :DEPTH, :] = state[d, h].astype(BF16)
    sent[0, d, h, DEPTH:, :] = jnp.broadcast_to(
        jnp.exp(offset[d, :, lanes]), (16, DEPTH)
    ).astype(BF16)
    for slot, exists, target, boundary in raw_sends(d):
        @pl.when(exists & boundary)
        def _():
            scan_copy(slot, 0, d, h, target, sent, landed, p_send, p_recv).start()


def raw_rest(d, h, sent, landed, before, before_keep, p_send, p_recv):
    for slot, exists, target, boundary in raw_sends(d):
        @pl.when(exists & jnp.logical_not(boundary))
        def _():
            scan_copy(slot, 0, d, h, target, sent, landed, p_send, p_recv).start()


def total_start(k, d, h, state, offset, sent, landed, before, before_keep, p_send, p_recv):
    size, (_, place) = group_size(), group_place()
    sends, group, _ = group_partner(d, group_strides()[k - 1])
    inner = place == (size - 2 if d == 0 else 1)
    lanes = slice(h * DEPTH, (h + 1) * DEPTH)

    def send(values, keep):
        sent[k, d, h, :DEPTH, :] = values.astype(BF16)
        sent[k, d, h, DEPTH:, :] = jnp.broadcast_to(keep, (16, DEPTH)).astype(BF16)
        for pair in range(size // 2 - 1, -1, -1) if d == 0 else range(size // 2):
            target = group * size + 2 * pair + lax.rem(place, 2)
            scan_copy(size + k - 1, k, d, h, target, sent, landed, p_send, p_recv).start()

    @pl.when(sends & jnp.logical_not(inner))
    def _():
        keep = jnp.exp(offset[d, :, lanes])
        send(keep * before[d, h] + state[d, h], keep * before_keep[d, :, lanes])

    @pl.when(sends & inner)
    def _():
        if k == 1:
            scan_copy(size - 1, 0, d, h, 0, sent, landed, p_send, p_recv).wait_recv()
        last = landed[size - 1, d, h].astype(F32)
        keep = jnp.exp(offset[d, :, lanes])
        last_keep = last[DEPTH : DEPTH + 1]
        send(
            last_keep * (keep * before[d, h] + state[d, h]) + last[:DEPTH],
            last_keep * (keep * before_keep[d, :, lanes]),
        )

    if k == 1:
        @pl.when(inner & jnp.logical_not(sends))
        def _():
            scan_copy(size - 1, 0, d, h, 0, sent, landed, p_send, p_recv).wait_recv()


def scan_close(k, d, h, only, sent, landed, before, before_keep, p_send, p_recv):
    size = group_size()
    if k == 0:
        arrivals = [(j - 1, raw_partner(d, j)[2]) for j in range(1, size)]
    else:
        arrivals = [(size + k - 1, group_partner(d, group_strides()[k - 1])[2])]
    for slot, gets in arrivals:
        @pl.when(gets & only)
        def _():
            scan_copy(slot, k, d, h, 0, sent, landed, p_send, p_recv).wait_recv()
            lanes = slice(h * DEPTH, (h + 1) * DEPTH)
            keep = before_keep[d, :, lanes]
            early = landed[slot, d, h].astype(F32)
            before[d, h] = keep * early[:DEPTH] + before[d, h]
            before_keep[d, :, lanes] = keep * early[DEPTH : DEPTH + 1]


def scan_drain(k, d, sent, landed, p_send, p_recv):
    size = group_size()
    if k == 0:
        leaving = [(slot, exists, sent.at[0, d]) for slot, exists, _, _ in raw_sends(d)]
    else:
        sends = group_partner(d, group_strides()[k - 1])[0]
        leaving = [(size + k - 1, sends, landed.at[pl.ds(0, size // 4)])]
    for slot, sends, block in leaving:
        @pl.when(sends)
        def _():
            pltpu.make_async_remote_copy(
                block, block, p_send.at[slot, d], p_recv.at[slot, d, 0],
                device_id={"sp": 0}, device_id_type=MESH,
            ).wait_send()


def mixer_kernel(groups, *refs):
    (h_tokens, h_gain, *h_weights) = refs[:8]
    (h_gap, h_added, h_initial, h_head, h_mix, h_scale, h_recur, h_pool) = refs[8:16]
    out = refs[16]
    (
        held, gain, wide, gap, added, initial, head_gain, mix, pool_gain, wfull,
        acc, square, cols, rows_of, turned, query_pre, value, gated, ent, runs, inner, reach,
        starts, offsets, chunk_state, chunk_keep, state, offset, padded,
        sent, landed, before, before_keep, given, taken, passed, brought, total, kept_x, kept_scale,
        l_sem, t_send, w_send, s_recv, x_recv, f_recv, w_recv, q_recv, g_recv,
        p_send, p_recv, e_send, e_recv, a_send, a_recv, c_send, c_recv,
    ) = refs[17:]
    me, sibling, across, opposite = peers()
    length, width = held.shape[1:]
    columns = wide.shape[2]
    heads = columns // DEPTH
    count = length // CHUNK
    share = length // 4
    subs = share // CHUNK
    features = 4 * width
    depth = wfull.shape[1] // 2
    steps = 1 + len(group_strides())

    own_w = [
        pltpu.make_async_copy(h_recur, wfull.at[me, pl.ds(0, depth)], l_sem.at[0]),
        pltpu.make_async_copy(h_pool, wfull.at[me, pl.ds(depth, depth)], l_sem.at[0]),
    ]
    own_t = pltpu.make_async_copy(h_tokens, held.at[me], l_sem.at[1])
    small = [
        pltpu.make_async_copy(a, b, l_sem.at[3 + i])
        for i, (a, b) in enumerate((
            (h_gain, gain), (h_gap, gap), (h_added, added), (h_initial, initial),
            (h_head, head_gain), (h_mix, mix), (h_scale, pool_gain),
        ))
    ]
    loads = [
        pltpu.make_async_copy(w, wide.at[i], l_sem.at[2]) for i, w in enumerate(h_weights)
    ]
    for copy in own_w + [own_t] + small + loads:
        copy.start()
    greet()

    size = ring_size()
    slab = 2 * depth // size
    half = slab // 2
    place, right, left = ring_place()
    events = size - 1

    mine = pl.ds(pl.multiple_of(place * slab, slab), slab)
    w_across = pltpu.make_async_remote_copy(
        wfull.at[me, mine], wfull.at[me, mine], w_send.at[0], w_recv.at[0],
        device_id={"tp": across}, device_id_type=MESH,
    )
    w_beside = pltpu.make_async_remote_copy(
        wfull.at[me], wfull.at[me], w_send.at[0], q_recv.at[0],
        device_id={"tp": sibling}, device_id_type=MESH,
    )
    def w_pass(rows):
        return pltpu.make_async_remote_copy(
            wfull.at[across, rows], wfull.at[across, rows], w_send.at[0], q_recv.at[0],
            device_id={"tp": sibling}, device_id_type=MESH,
        )

    def ring_rows(way, e):
        spot = lax.rem(place + (e // 2 if way else size - e // 2), size)
        side = 1 - lax.rem(e, 2) if way else lax.rem(e, 2)
        return pl.ds(pl.multiple_of(spot * slab + side * half, half), half)

    def ring_copy(way, e):
        at = ring_rows(way, e)
        return pltpu.make_async_remote_copy(
            wfull.at[across, at], wfull.at[across, at], w_send.at[0], g_recv.at[e],
            device_id={"sp": left if way else right}, device_id_type=MESH,
        )

    def ring_turn(e):
        landed_slab = wfull.at[across, pl.ds(0, slab)]
        pltpu.make_async_remote_copy(
            landed_slab, landed_slab, w_send.at[0], g_recv.at[e],
            device_id={"sp": right}, device_id_type=MESH,
        ).wait_recv()
        for way in range(2):
            @pl.when(e + 2 < events)
            def _():
                ring_copy(way, e + 2).start()

            w_pass(ring_rows(way, e + 2)).start()

    beside = pltpu.make_async_remote_copy(
        held.at[me], held.at[me], t_send.at[0], s_recv.at[0],
        device_id={"tp": sibling}, device_id_type=MESH,
    )

    def piece(i):
        return pl.ds(pl.multiple_of(i * CHUNK, CHUNK), CHUNK)

    def crossing(i):
        return pltpu.make_async_remote_copy(
            held.at[me, piece(i)], held.at[me, piece(i)], t_send.at[0], x_recv.at[i],
            device_id={"tp": across}, device_id_type=MESH,
        )

    def relay(i):
        return pltpu.make_async_remote_copy(
            held.at[across, piece(i)], held.at[across, piece(i)], t_send.at[0], f_recv.at[i],
            device_id={"tp": sibling}, device_id_type=MESH,
        )

    pltpu.make_async_copy(wfull.at[across], wfull.at[me], l_sem.at[0]).wait()
    w_across.start()
    own_t.wait()
    beside.start()
    for i in range(count):
        crossing(i).start()
    w_beside.start()
    for copy in small:
        copy.wait()

    row = lax.broadcasted_iota(jnp.int32, (CHUNK, CHUNK), 0)
    col = lax.broadcasted_iota(jnp.int32, (CHUNK, CHUNK), 1)
    lower, upper = row >= col, row <= col
    lower_f, upper_f = lower.astype(F32), upper.astype(F32)
    lower_2 = jnp.concatenate([lower_f, lower_f], axis=1).astype(BF16)
    upper_2 = jnp.concatenate([upper_f, upper_f], axis=1).astype(BF16)

    def sums(c, _):
        add = added[:, piece(c)]
        cols[0, c] = dot_t(lower_f, add, EXACT)
        cols[1, c] = dot_t(upper_f, add, EXACT)
        rows_of[0, c] = dot(add, upper_f, EXACT)
        rows_of[1, c] = dot(add, lower_f, EXACT)
        return 0

    lax.fori_loop(0, count, sums, 0)
    for h in range(heads):
        for d in range(2):
            turned[h, :, d * DEPTH : (d + 1) * DEPTH] = initial[d, h].T
    state[...] = jnp.zeros_like(state)
    offset[...] = jnp.zeros_like(offset)
    before[...] = jnp.zeros_like(before)
    before_keep[...] = jnp.ones_like(before_keep)
    for d in range(2):
        _, _, source = partner(d, 1)
        begin = 0 if d == 0 else RIM + length

        @pl.when(jnp.logical_not(source))
        def _():
            padded[pl.ds(begin, RIM), :] = jnp.zeros((RIM, columns), BF16)

    pair = me // 2
    near, far = 2 * pair, 2 - 2 * pair

    def normed(first, at):
        parts, squares = [], 0.0
        for o in range(2):
            x = held[first + o, at, :].astype(F32)
            squares = squares + jnp.sum(x * x, axis=1, keepdims=True)
            lanes = pl.ds(pl.multiple_of((first + o) * width, width), width)
            parts.append((x * gain[:, lanes]).astype(BF16))
        return jnp.concatenate(parts, axis=1), squares

    def depth_of(first):
        return pl.ds(pl.multiple_of(first * width, 2 * width), 2 * width)

    pltpu.make_async_copy(wide, wide, l_sem.at[2]).wait()
    beside.wait_recv()

    def own(i, _):
        at = pl.ds(pl.multiple_of(i * share, share), share)
        x, squares = normed(near, at)
        square[at, :] = squares
        for j in range(6):
            acc[j, at, :] = dot(x, wide[j, depth_of(near), :])
        return 0

    lax.fori_loop(0, 4, own, 0)
    w_across.wait_recv()
    for e in range(min(2, events)):
        for way in range(2):
            ring_copy(way, e).start()
    w_pass(mine).start()

    def gates(pre, gap_row, sums):
        enter = gap_row * (1.0 / (1.0 + jnp.exp(pre)))
        keep = jnp.log1p(-enter)
        high = keep.astype(BF16)
        low = (keep - high.astype(F32)).astype(BF16)
        return enter, dot(sums, jnp.concatenate([high, low], axis=0))

    def local(c):
        at = piece(c)
        x = query_pre[at, :].astype(F32)
        query = x / (1.0 + jnp.exp(-x))
        q_f, q_b = query * jnp.exp(runs[0, at, :]), query * jnp.exp(runs[1, at, :])
        e_f, e_b = ent[0, at, :], ent[1, at, :]
        values = value[at, :]
        col_f, col_b = cols[0, c], cols[1, c]
        row_f, row_b = rows_of[0, c], rows_of[1, c]
        for h in range(heads):
            lanes = slice(h * DEPTH, (h + 1) * DEPTH)
            a_col, b_col = col_f[:, h : h + 1], col_b[:, h : h + 1]
            fade = jnp.exp(
                jnp.where(lower, a_col - row_f[h : h + 1, :], b_col - row_b[h : h + 1, :])
            )
            w_f = dot_t(q_f[:, lanes].astype(BF16), e_f[:, lanes])
            w_b = dot_t(q_b[:, lanes].astype(BF16), e_b[:, lanes])
            weight = (jnp.where(lower, w_f, 0.0) + jnp.where(upper, w_b, 0.0)) * fade
            inner[at, lanes] = dot(weight.astype(BF16), values[:, lanes])
            reach[h, at, :DEPTH] = (q_f[:, lanes] * jnp.exp(a_col)).astype(BF16)
            reach[h, at, DEPTH:] = (q_b[:, lanes] * jnp.exp(b_col)).astype(BF16)

    def project(j, x, scale, at):
        return ((acc[j, at, :] + dot(x, wide[j, depth_of(far), :])) * scale).astype(BF16)

    def late_pool(c, rows=None):
        slot = lax.rem(c, 2)
        if rows is None:
            rows = project(5, kept_x[slot], kept_scale[slot], piece(c))
        padded[pl.ds(pl.multiple_of(c * CHUNK + RIM, RIM), CHUNK), :] = rows

    def late(c, again=None):
        at, x, scale = piece(c), kept_x[lax.rem(c, 2)], kept_scale[lax.rem(c, 2)]
        again = again or (lambda j: project(j, x, scale, at))
        query_pre[at, :] = again(0)
        gate = again(4).astype(F32)
        gated[at, :] = head_gain[...] / (1.0 + jnp.exp(-gate))

    def step(i, _):
        at = piece(i)
        crossing(i).wait_recv()
        relay(i).start()
        @pl.when(i > 0)
        def _():
            late_pool(i - 1)
            late(i - 1)
            local(i - 1)

        @pl.when((i > 0) & (i <= events))
        def _():
            ring_turn(i - 1)

        @pl.when(i == 1)
        def _():
            edge_start(1, length, padded, e_send, e_recv)

        relay(i).wait_recv()
        x, squares = normed(far, at)
        scale = lax.rsqrt((square[at, :] + squares) / features + EPSILON)
        kept_x[lax.rem(i, 2)], kept_scale[lax.rem(i, 2)] = x, scale
        advance(i, *(project(j, x, scale, at) for j in (1, 2, 3)))
        return 0

    def last_step():
        i = count - 1
        at, slot = piece(i), i % 2

        def half(owner):
            x = held[owner, at, :].astype(F32)
            lanes = pl.ds(pl.multiple_of(owner * width, width), width)
            part = (x * gain[:, lanes]).astype(BF16)
            inside = pl.ds(pl.multiple_of((owner - far) * width, width), width)
            kept_x[slot, :, inside] = part
            return part, jnp.sum(x * x, axis=1, keepdims=True)

        def rows_of_w(owner):
            return pl.ds(pl.multiple_of(owner * width, width), width)

        crossing(i).wait_recv()
        relay(i).start()
        x, squares = half(across)
        square[at, :] = square[at, :] + squares
        for j in range(6):
            acc[j, at, :] = acc[j, at, :] + dot(x, wide[j, rows_of_w(across), :])
        relay(i).wait_recv()
        x, squares = half(opposite)
        scale = lax.rsqrt((square[at, :] + squares) / features + EPSILON)
        kept_scale[slot] = scale

        def project_half(j):
            y = acc[j, at, :] + dot(x, wide[j, rows_of_w(opposite), :])
            return (y * scale).astype(BF16)

        advance(i, *(project_half(j) for j in (1, 2, 3)))

    def advance(i, pre_f, pre_b, values):
        at = piece(i)
        value[at, :] = values
        enter_f, run_f = gates(pre_f.astype(F32), gap[0:1, :], lower_2)
        enter_b, run_b = gates(pre_b.astype(F32), gap[1:2, :], upper_2)
        runs[0, at, :], runs[1, at, :] = run_f, run_b
        e_f, e_b = enter_f * jnp.exp(-run_f), enter_b * jnp.exp(-run_b)
        ent[0, at, :], ent[1, at, :] = e_f.astype(BF16), e_b.astype(BF16)
        close_f, close_b = run_f[CHUNK - 1 : CHUNK, :], run_b[0:1, :]
        last_f, last_b = e_f * jnp.exp(close_f), e_b * jnp.exp(close_b)
        offsets[0, i] = offset[0]
        col_f, col_b = cols[0, i], cols[1, i]
        for h in range(heads):
            lanes = slice(h * DEPTH, (h + 1) * DEPTH)
            a_col, b_col = col_f[:, h : h + 1], col_b[:, h : h + 1]
            a_end, b_end = a_col[CHUNK - 1 : CHUNK, :], b_col[0:1, :]
            total_f = close_f[:, lanes] + a_end
            ends_f = (last_f[:, lanes] * jnp.exp(a_end - a_col)).astype(BF16)
            ends_b = (last_b[:, lanes] * jnp.exp(b_end - b_col)).astype(BF16)
            ends = t_dot(values[:, lanes], jnp.concatenate([ends_f, ends_b], axis=1))
            starts[i, h, :, :DEPTH] = state[0, h]
            state[0, h] = jnp.exp(total_f) * state[0, h] + ends[:, :DEPTH]
            chunk_state[i, h] = ends[:, DEPTH:]
            chunk_keep[i, :, lanes] = close_b[:, lanes] + b_end
            offset[0, :, lanes] = offset[0, :, lanes] + total_f

    lax.fori_loop(0, count - 1, step, 0)
    last_step()

    def descend(i, _):
        c = count - 1 - i
        offsets[1, c] = offset[1]
        for h in range(heads):
            lanes = slice(h * DEPTH, (h + 1) * DEPTH)
            starts[c, h, :, DEPTH:] = state[1, h]
            keep = chunk_keep[c, :, lanes]
            state[1, h] = jnp.exp(keep) * state[1, h] + chunk_state[c, h]
            offset[1, :, lanes] = offset[1, :, lanes] + keep
        return 0

    window = jnp.left_shift(jnp.int32(2), lax.axis_index("tp") * groups)
    sequence, first_row = length * lax.axis_size("sp"), lax.axis_index("sp") * length

    def pooled(owner):
        begin = pl.multiple_of(owner * share, share)
        span = share + 2 * RIM
        near_rows = padded[pl.ds(begin, span), :]
        target = first_row + begin + lax.broadcasted_iota(jnp.int32, (share, span), 0)
        source = first_row + begin - RIM + lax.broadcasted_iota(jnp.int32, (share, span), 1)
        low = target - window // 2
        inside = (source >= low) & (source < low + window) & (source >= 0) & (source < sequence)
        start = first_row + begin + lax.broadcasted_iota(jnp.int32, (share, 1), 0) - window // 2
        number = jnp.minimum(start + window, sequence) - jnp.maximum(start, 0)
        mean = dot(inside.astype(F32).astype(BF16), near_rows) / number.astype(F32)
        here = padded[pl.ds(pl.multiple_of(begin + RIM, RIM), share), :].astype(F32)
        return (dot((mean - here).astype(BF16), mix[0]) * pool_gain[...]).astype(BF16)

    def pool_copy(r):
        return pltpu.make_async_remote_copy(
            passed.at[r], brought.at[me], a_send.at[0], a_recv.at[0],
            device_id={"tp": jnp.int32(r)}, device_id_type=MESH,
        )

    pool_all = pltpu.make_async_remote_copy(
        passed.at[pl.ds(0, 3)], brought.at[pl.ds(0, 3)], a_send.at[0], a_recv.at[0],
        device_id={"tp": sibling}, device_id_type=MESH,
    )

    def pool_away(r):
        if r == 3:
            edge_wait(1, length, padded, e_send, e_recv)
        if r == 0:
            edge_wait(0, length, padded, e_send, e_recv)
        rows = pooled(r)
        passed[r] = rows

        @pl.when(me == r)
        def _():
            brought[r] = rows

        @pl.when(me != r)
        def _():
            pool_copy(r).start()

    def ring_end():
        for e in range(count - 2, events):
            ring_turn(e)

    def drain_gather():
        for block, sem in ((held, t_send), (wfull, w_send)):
            rows = block.at[pl.ds(0, 3)]
            pltpu.make_async_remote_copy(
                rows, rows, sem.at[0], s_recv.at[0],
                device_id={"tp": sibling}, device_id_type=MESH,
            ).wait_send()

    def drain_scan():
        for d in range(2):
            exists, _, _ = partner(d, 1)

            @pl.when(exists)
            def _():
                edge_copy(d, length, padded, e_send, e_recv).wait_send()

        for k in range(steps):
            for d in range(2):
                scan_drain(k, d, sent, landed, p_send, p_recv)

        pool_all.wait_send()

    def half_again(j):
        at = piece(count - 1)
        owner = pl.ds(pl.multiple_of(opposite * width, width), width)
        inside = pl.ds(pl.multiple_of((opposite - far) * width, width), width)
        slot = (count - 1) % 2
        y = acc[j, at, :] + dot(kept_x[slot, :, inside], wide[j, owner, :])
        return (y * kept_scale[slot]).astype(BF16)

    def late_last():
        late_pool(count - 2)
        late(count - 2)
        local(count - 2)
        for h in range(1, heads):
            for d in range(2):
                raw_start(d, h, state, offset, *scan)
        for h in range(heads):
            for d in range(2):
                raw_rest(d, h, *scan)
        late(count - 1, half_again)
        local(count - 1)

    tile = 512
    tiles = out.shape[1] // tile

    def wide_pool():
        pltpu.make_async_remote_copy(
            wfull.at[pl.ds(0, 2)], wfull.at[pl.ds(0, 2)], w_send.at[0], q_recv.at[0],
            device_id={"tp": sibling}, device_id_type=MESH,
        ).wait_recv()
        pool_all.wait_recv()
        for j in range(tiles):
            lanes = slice(j * tile, (j + 1) * tile)
            y = dot(brought[0], wfull[0, depth:, lanes])
            for r in range(1, 4):
                y = y + dot(brought[r], wfull[r, depth:, lanes])
            total[:, lanes] = y

    def finished(c, h):
        at, lanes = piece(c), slice(h * DEPTH, (h + 1) * DEPTH)
        ages = jnp.exp(jnp.concatenate([offsets[0, c, :, lanes], offsets[1, c, :, lanes]], axis=1))
        enter = (starts[c, h] + ages * turned[h]).astype(BF16)
        both = inner[at, lanes] + dot_t(reach[h, at, :], enter)
        both = both * lax.rsqrt(jnp.mean(both * both, axis=1, keepdims=True) + EPSILON)
        given[h, at, :] = (both * gated[at, lanes]).astype(BF16)

    relations = (across, opposite, sibling, me)

    def recur_copy(k, h):
        there = relations[k]
        at = pl.ds(pl.multiple_of(there * share, share), share)
        return pltpu.make_async_remote_copy(
            given.at[h, at], taken.at[me, h], c_send.at[0], c_recv.at[heads if k == 2 else h],
            device_id={"tp": there}, device_id_type=MESH,
        )

    def recur_wait(owners, count, sem):
        block = taken.at[pl.ds(0, owners), pl.ds(0, count)]
        return pltpu.make_async_remote_copy(
            block, block, c_send.at[0], c_recv.at[sem],
            device_id={"tp": sibling}, device_id_type=MESH,
        )

    def away(k, h):
        for sub in range(subs):
            finished(relations[k] * subs + sub, h)
        if k < 3:
            recur_copy(k, h).start()

    scan = (sent, landed, before, before_keep, p_send, p_recv)
    place_in_group = group_place()[1]
    always = place_in_group >= 0
    leads = (place_in_group >= group_size() // 2, place_in_group < group_size() // 2)

    def close_rest():
        for h in range(heads):
            for d in range(2):
                scan_close(0, d, h, leads[1 - d] if steps > 1 else always, *scan)

    fillers = [
        [late_last, ring_end] + [functools.partial(pool_away, r) for r in (1, 2, 3)]
        + ([] if steps > 1 else [lambda: pool_away(0), close_rest, drain_gather]),
        [close_rest, drain_gather] if steps > 1 else [],
    ]
    rounds = [[] for _ in range(steps)]
    for i, group in enumerate(fillers):
        rounds[min(i, len(rounds) - 1)].extend(group)
    for k in range(steps):
        if k == 0:
            raw_start(0, 0, state, offset, *scan)
            lax.fori_loop(0, count, descend, 0)
            raw_start(1, 0, state, offset, *scan)
            late_pool(count - 1, half_again(5))
            edge_start(0, length, padded, e_send, e_recv)
        for h in range(heads if k else 0):
            for d in range(2):
                scan_close(k - 1, d, h, leads[d] if k == 1 else always, *scan)
            for d in range(2):
                total_start(k, d, h, state, offset, *scan)
            if k == 1 and h == 0:
                pool_away(0)
        for filler in rounds[k]:
            filler()
    for h in range(heads):
        for d in range(2):
            scan_close(steps - 1, d, h, always, *scan)
            lanes = slice(d * DEPTH, (d + 1) * DEPTH)
            keep = before_keep[d, :, h * DEPTH : (h + 1) * DEPTH]
            turned[h, :, lanes] = keep * turned[h, :, lanes] + before[d, h]
        for k in range(2):
            away(k, h)
    for k in (2, 3):
        for h in range(heads):
            away(k, h)

    def all_heads(rows):
        return jnp.concatenate([rows(h) for h in range(heads)], axis=1)

    def far_part(h, lanes):
        rows = slice(h * DEPTH, (h + 1) * DEPTH)
        return dot(
            jnp.concatenate([taken[across, h], taken[opposite, h]], axis=1),
            jnp.concatenate([wfull[across, rows, lanes], wfull[opposite, rows, lanes]], axis=0),
        )

    wide_pool()
    recur_wait(1, heads, heads).wait_recv()
    home = pl.ds(pl.multiple_of(me * share, share), share)
    for j in range(tiles):
        lanes = slice(j * tile, (j + 1) * tile)
        y = total[:, lanes] + dot(
            all_heads(lambda h: given[h, home, :]), wfull[me, :depth, lanes]
        )
        total[:, lanes] = y + dot(
            all_heads(lambda h: taken[sibling, h]), wfull[sibling, :depth, lanes]
        )
    drain_scan()
    for h in range(heads - 1):
        recur_wait(1, 2, h).wait_recv()
        for j in range(tiles):
            lanes = slice(j * tile, (j + 1) * tile)
            total[:, lanes] = total[:, lanes] + far_part(h, lanes)
    recur_wait(1, 2, heads - 1).wait_recv()
    for j in range(tiles):
        lanes = slice(j * tile, (j + 1) * tile)
        out[:, lanes] = (total[:, lanes] + far_part(heads - 1, lanes)).astype(BF16)
    recur_wait(3, heads, 0).wait_send()


def shards(
    tokens, norm_gain, w_query, w_forget_fwd, w_forget_bwd, w_value, w_gate, w_pool_in,
    forget_gap, added_log_retention, initial_state, head_gain, pool_mix, pool_gain,
    w_out_recur, w_out_pool,
):
    weights = (w_query, w_forget_fwd, w_forget_bwd, w_value, w_gate, w_pool_in)
    length, width = tokens.shape
    features, columns = w_query.shape
    heads = columns // DEPTH
    count = length // CHUNK
    share = length // 4
    subs = share // CHUNK
    depth, out_width = w_out_recur.shape
    steps = 1 + len(group_strides())
    size = ring_size()
    events = size - 1
    slots = group_size() + steps - 1
    dma = pltpu.SemaphoreType.DMA
    operands = (
        tokens, norm_gain[None, :], *weights, forget_gap, added_log_retention.T, initial_state,
        head_gain[None, :], pool_mix, pool_gain[None, :], w_out_recur, w_out_pool,
    )

    def like(array):
        return pltpu.VMEM(array.shape, array.dtype)

    return pl.pallas_call(
        functools.partial(mixer_kernel, pool_mix.shape[0]),
        out_shape=pltpu.VMEM((share, out_width), BF16),
        in_specs=[ANY] * len(operands),
        out_specs=VM,
        scratch_shapes=[
            pltpu.VMEM((4, length, width), BF16),
            like(operands[1]),
            pltpu.VMEM((6, features, columns), BF16),
            like(operands[8]), like(operands[9]), like(operands[10]), like(operands[11]),
            like(operands[12]), like(operands[13]),
            pltpu.VMEM((4, 2 * depth, out_width), BF16),
            pltpu.VMEM((6, length, columns), F32),
            pltpu.VMEM((length, 1), F32),
            pltpu.VMEM((2, count, CHUNK, heads), F32),
            pltpu.VMEM((2, count, heads, CHUNK), F32),
            pltpu.VMEM((heads, DEPTH, 2 * DEPTH), F32),
            pltpu.VMEM((length, columns), BF16),
            pltpu.VMEM((length, columns), BF16),
            pltpu.VMEM((length, columns), F32),
            pltpu.VMEM((2, length, columns), BF16),
            pltpu.VMEM((2, length, columns), F32),
            pltpu.VMEM((length, columns), F32),
            pltpu.VMEM((heads, length, 2 * DEPTH), BF16),
            pltpu.VMEM((count, heads, DEPTH, 2 * DEPTH), F32),
            pltpu.VMEM((2, count, 1, columns), F32),
            pltpu.VMEM((count, heads, DEPTH, DEPTH), F32),
            pltpu.VMEM((count, 1, columns), F32),
            pltpu.VMEM((2, heads, DEPTH, DEPTH), F32),
            pltpu.VMEM((2, 1, columns), F32),
            pltpu.VMEM((length + 2 * RIM, columns), BF16),
            pltpu.VMEM((steps, 2, heads, DEPTH + 16, DEPTH), BF16),
            pltpu.VMEM((slots, 2, heads, DEPTH + 16, DEPTH), BF16),
            pltpu.VMEM((2, heads, DEPTH, DEPTH), F32),
            pltpu.VMEM((2, 1, columns), F32),
            pltpu.VMEM((heads, length, DEPTH), BF16),
            pltpu.VMEM((4, heads, share, DEPTH), BF16),
            pltpu.VMEM((4, share, columns), BF16),
            pltpu.VMEM((4, share, columns), BF16),
            pltpu.VMEM((share, out_width), F32),
            pltpu.VMEM((2, CHUNK, 2 * width), BF16),
            pltpu.VMEM((2, CHUNK, 1), F32),
            dma((10,)), dma((1,)), dma((1,)), dma((1,)), dma((count,)), dma((count,)),
            dma((1,)), dma((1,)), dma((events,)),
            dma((slots, 2)), dma((slots, 2, heads)), dma((2,)), dma((2,)),
            dma((1,)), dma((1,)), dma((1,)), dma((heads + 1,)),
        ],
        compiler_params=pltpu.CompilerParams(
            collective_id=0, has_side_effects=True, vmem_limit_bytes=VMEM_LIMIT
        ),
        name="mixer",
    )(*(pltpu.with_memory_space_constraint(x, pltpu.HBM) for x in operands))


def solution(mesh):
    in_specs = (
        P("sp", "tp"), P(), P(None, "tp"), P(None, "tp"), P(None, "tp"), P(None, "tp"),
        P(None, "tp"), P(None, "tp"), P(None, "tp"), P("sp", "tp"), P(None, "tp", None, None),
        P("tp"), P("tp", None, None), P("tp"), P("tp", None), P("tp", None),
    )
    out_specs = P(("sp", "tp"), None)
    return jax.shard_map(shards, mesh=mesh, in_specs=in_specs, out_specs=out_specs, check_vma=False)
```

```python
import functools

import jax
import jax.numpy as jnp
from jax import lax
from jax.experimental import pallas as pl
from jax.experimental.pallas import tpu as pltpu
from jax.sharding import PartitionSpec as P

DEPTH = 128
CHUNK = 128
EPSILON = 1e-06
RIM = 16
RING = 8
GROUP = 4
MESH = pl.DeviceIdType.MESH
F32 = jnp.float32
BF16 = jnp.bfloat16
VMEM_LIMIT = 52 * 1024 * 1024
ANY = pl.BlockSpec(memory_space=pl.ANY)
VM = pl.BlockSpec(memory_space=pltpu.VMEM)
EXACT = lax.Precision.HIGHEST


def dot(a, b, precision=None):
    return jnp.dot(a, b, preferred_element_type=F32, precision=precision)


def dot_t(a, b, precision=None):
    return lax.dot_general(
        a, b, (((1,), (1,)), ((), ())), preferred_element_type=F32, precision=precision
    )


def t_dot(a, b):
    return lax.dot_general(a, b, (((0,), (0,)), ((), ())), preferred_element_type=F32)


def peers():
    me = lax.axis_index("tp")
    sibling = me + 1 - 2 * lax.rem(me, 2)
    across = lax.rem(me + 2, 4)
    return me, sibling, across, lax.rem(sibling + 2, 4)


def partner(d, stride):
    me, count = lax.axis_index("sp"), lax.axis_size("sp")
    above, below = me + stride < count, me >= stride
    return (above, me + stride, below) if d == 0 else (below, me - stride, above)


def group_size():
    return min(GROUP, lax.axis_size("sp"))


def group_strides():
    count = lax.axis_size("sp") // group_size()
    return [1 << k for k in range(count.bit_length()) if 1 << k < count]


def group_place():
    me = lax.axis_index("sp")
    return me // group_size(), lax.rem(me, group_size())


def raw_partner(d, j):
    (_, place), me, size = group_place(), lax.axis_index("sp"), group_size()
    above, below = place + j < size, place >= j
    return (above, me + j, below) if d == 0 else (below, me - j, above)


def group_partner(d, stride):
    (group, place), size = group_place(), group_size()
    count = lax.axis_size("sp") // size
    above, below = group + stride < count, group >= stride
    if d == 0:
        return above & (place >= size - 2), group + stride, below
    return below & (place < 2), group - stride, above


def ring_size():
    return min(RING, lax.axis_size("sp"))


def ring_place():
    size = ring_size()
    me = lax.axis_index("sp")
    base, mine = me - lax.rem(me, size), lax.rem(me, size)
    place = jnp.where(lax.rem(mine, 2) == 0, mine // 2, size - 1 - mine // 2)

    def index(spot):
        spot = lax.rem(spot + size, size)
        return base + jnp.where(spot < size // 2, 2 * spot, 2 * (size - 1 - spot) + 1)

    return place, index(place + 1), index(place - 1)


def greet():
    barrier = pltpu.get_barrier_semaphore()
    _, sibling, across, opposite = peers()
    _, right, left = ring_place()
    for device in (sibling, across, opposite):
        pl.semaphore_signal(barrier, inc=1, device_id={"tp": device}, device_id_type=MESH)
    for device in (right, left):
        pl.semaphore_signal(barrier, inc=1, device_id={"sp": device}, device_id_type=MESH)
    size, (group, place) = group_size(), group_place()
    for j in range(1, size):
        target = group * size + lax.rem(place + j, size)
        pl.semaphore_signal(barrier, inc=1, device_id={"sp": target}, device_id_type=MESH)
    number = jnp.int32(5 + size - 1)
    for stride in group_strides():
        for d in range(2):
            sends, _, gets = group_partner(d, stride)
            source = (group - stride) * size + size - 2 if d == 0 else (group + stride) * size
            source = source + lax.rem(place, 2)

            @pl.when(gets)
            def _():
                pl.semaphore_signal(
                    barrier, inc=1, device_id={"sp": source}, device_id_type=MESH
                )

            number = number + jnp.where(sends, size // 2, 0)
    for d in range(2):
        exists, target, _ = partner(d, 1)
        outside = exists & (place == (size - 1 if d == 0 else 0))

        @pl.when(outside)
        def _():
            pl.semaphore_signal(barrier, inc=1, device_id={"sp": target}, device_id_type=MESH)

        number = number + jnp.where(outside, 1, 0)
    pl.semaphore_wait(barrier, number)


def edge_copy(d, length, padded, e_send, e_recv):
    _, target, _ = partner(d, 1)
    there = 0 if d == 0 else RIM + length
    return pltpu.make_async_remote_copy(
        padded.at[pl.ds(length if d == 0 else RIM, RIM)], padded.at[pl.ds(there, RIM)],
        e_send.at[d], e_recv.at[d], device_id={"sp": target}, device_id_type=MESH,
    )


def edge_start(d, length, padded, e_send, e_recv):
    exists, _, _ = partner(d, 1)

    @pl.when(exists)
    def _():
        edge_copy(d, length, padded, e_send, e_recv).start()


def edge_wait(d, length, padded, e_send, e_recv):
    _, _, source = partner(d, 1)

    @pl.when(source)
    def _():
        edge_copy(d, length, padded, e_send, e_recv).wait_recv()


def scan_copy(slot, k, d, h, target, sent, landed, p_send, p_recv):
    return pltpu.make_async_remote_copy(
        sent.at[k, d, h], landed.at[slot, d, h],
        p_send.at[2 * k - 1 + d if k else 0], p_recv.at[k, d, h],
        device_id={"sp": target}, device_id_type=MESH,
    )


def raw_sends(d):
    size, (_, place), me = group_size(), group_place(), lax.axis_index("sp")
    rows = []
    for j in range(size - 1, 0, -1):
        exists, target, _ = raw_partner(d, j)
        rows.append((j - 1, exists, target, place + j >= size - 2 if d == 0 else place - j < 2))
    if d == 0:
        extra = (size - 1, place == size - 1, me - 1, place >= 0)
    else:
        extra = (size - 1, place == 0, me + 1, place >= 0)
    return [extra] + rows


def raw_start(d, h, state, offset, sent, landed, before, before_keep, p_send, p_recv):
    lanes = slice(h * DEPTH, (h + 1) * DEPTH)
    sent[0, d, h, :DEPTH, :] = state[d, h].astype(BF16)
    sent[0, d, h, DEPTH:, :] = jnp.broadcast_to(
        jnp.exp(offset[d, :, lanes]), (16, DEPTH)
    ).astype(BF16)
    for slot, exists, target, boundary in raw_sends(d):
        @pl.when(exists & boundary)
        def _():
            scan_copy(slot, 0, d, h, target, sent, landed, p_send, p_recv).start()


def raw_rest(d, h, sent, landed, before, before_keep, p_send, p_recv):
    for slot, exists, target, boundary in raw_sends(d):
        @pl.when(exists & jnp.logical_not(boundary))
        def _():
            scan_copy(slot, 0, d, h, target, sent, landed, p_send, p_recv).start()


def total_start(k, d, h, state, offset, sent, landed, before, before_keep, p_send, p_recv):
    size, (_, place) = group_size(), group_place()
    sends, group, _ = group_partner(d, group_strides()[k - 1])
    inner = place == (size - 2 if d == 0 else 1)
    lanes = slice(h * DEPTH, (h + 1) * DEPTH)

    def send(values, keep):
        sent[k, d, h, :DEPTH, :] = values.astype(BF16)
        sent[k, d, h, DEPTH:, :] = jnp.broadcast_to(keep, (16, DEPTH)).astype(BF16)
        for pair in range(size // 2 - 1, -1, -1) if d == 0 else range(size // 2):
            target = group * size + 2 * pair + lax.rem(place, 2)
            scan_copy(size + k - 1, k, d, h, target, sent, landed, p_send, p_recv).start()

    @pl.when(sends & jnp.logical_not(inner))
    def _():
        keep = jnp.exp(offset[d, :, lanes])
        send(keep * before[d, h] + state[d, h], keep * before_keep[d, :, lanes])

    @pl.when(sends & inner)
    def _():
        last = landed[size - 1, d, h].astype(F32)
        keep = jnp.exp(offset[d, :, lanes])
        last_keep = last[DEPTH : DEPTH + 1]
        send(
            last_keep * (keep * before[d, h] + state[d, h]) + last[:DEPTH],
            last_keep * (keep * before_keep[d, :, lanes]),
        )


def scan_wait(block, send, recv):
    return pltpu.make_async_remote_copy(
        block, block, send, recv, device_id={"sp": 0}, device_id_type=MESH
    )


def scan_close(k, d, h, only, sent, landed, before, before_keep, p_send, p_recv):
    size, (_, place) = group_size(), group_place()

    def add(slot):
        lanes = slice(h * DEPTH, (h + 1) * DEPTH)
        keep = before_keep[d, :, lanes]
        early = landed[slot, d, h].astype(F32)
        before[d, h] = keep * early[:DEPTH] + before[d, h]
        before_keep[d, :, lanes] = keep * early[DEPTH : DEPTH + 1]

    def wait(block):
        scan_wait(block, p_send.at[0], p_recv.at[k, d, h]).wait_recv()

    if k:
        @pl.when(group_partner(d, group_strides()[k - 1])[2] & only)
        def _():
            wait(landed.at[0, d, h])
            add(size + k - 1)

        return
    boundary = place >= size - 2 if d == 0 else place < 2

    @pl.when(only & boundary)
    def _():
        wait(landed.at[pl.ds(0, size - 1), d, h])
        for j in range(1, size):
            pl.when(raw_partner(d, j)[2])(functools.partial(add, j - 1))

    @pl.when(only & jnp.logical_not(boundary) & raw_partner(d, 1)[2])
    def _():
        wait(landed.at[0, d, h])
        add(0)


def scan_drain(steps, landed, p_send, p_recv):
    size, (_, place) = group_size(), group_place()
    outer = (place == 0) | (place == size - 1)
    leaving = [
        (0, outer, landed.at[pl.ds(0, size // 2)]),
        (0, jnp.logical_not(outer), landed.at[pl.ds(0, size - 1), 0]),
    ]
    for k in range(1, steps):
        for d in range(2):
            sends = group_partner(d, group_strides()[k - 1])[0]
            leaving.append((2 * k - 1 + d, sends, landed.at[pl.ds(0, size // 4)]))
    for index, sends, block in leaving:
        @pl.when(sends)
        def _():
            scan_wait(block, p_send.at[index], p_recv.at[0, 0, 0]).wait_send()


def mixer_kernel(groups, *refs):
    (h_tokens, h_gain, *h_weights) = refs[:8]
    (h_gap, h_added, h_initial, h_head, h_mix, h_scale, h_recur, h_pool) = refs[8:16]
    out = refs[16]
    (
        held, gain, wide, gap, added, initial, head_gain, mix, pool_gain, wfull,
        acc, square, cols, rows_of, turned, query_pre, value, gated, ent, runs, inner, reach,
        starts, offsets, chunk_state, chunk_keep, state, offset, padded,
        sent, landed, before, before_keep, given, taken, passed, brought, total, kept_x, kept_scale,
        l_sem, t_send, w_send, s_recv, x_recv, f_recv, w_recv, q_recv, g_recv,
        p_send, p_recv, e_send, e_recv, a_send, a_recv, c_send, c_recv,
    ) = refs[17:]
    me, sibling, across, opposite = peers()
    length, width = held.shape[1:]
    columns = wide.shape[2]
    heads = columns // DEPTH
    count = length // CHUNK
    share = length // 4
    subs = share // CHUNK
    features = 4 * width
    depth = wfull.shape[1] // 2
    steps = 1 + len(group_strides())

    own_w = [
        pltpu.make_async_copy(h_recur, wfull.at[me, pl.ds(0, depth)], l_sem.at[0]),
        pltpu.make_async_copy(h_pool, wfull.at[me, pl.ds(depth, depth)], l_sem.at[0]),
    ]
    own_t = pltpu.make_async_copy(h_tokens, held.at[me], l_sem.at[1])
    small = [
        pltpu.make_async_copy(a, b, l_sem.at[3 + i])
        for i, (a, b) in enumerate((
            (h_gain, gain), (h_gap, gap), (h_added, added), (h_initial, initial),
            (h_head, head_gain), (h_mix, mix), (h_scale, pool_gain),
        ))
    ]
    loads = [
        pltpu.make_async_copy(w, wide.at[i], l_sem.at[2]) for i, w in enumerate(h_weights)
    ]
    for copy in own_w + [own_t] + small + loads:
        copy.start()
    greet()

    size = ring_size()
    slab = 2 * depth // size
    half = slab // 2
    place, right, left = ring_place()
    events = size - 1

    mine = pl.ds(pl.multiple_of(place * slab, slab), slab)
    w_across = pltpu.make_async_remote_copy(
        wfull.at[me, mine], wfull.at[me, mine], w_send.at[0], w_recv.at[0],
        device_id={"tp": across}, device_id_type=MESH,
    )
    w_beside = pltpu.make_async_remote_copy(
        wfull.at[me], wfull.at[me], w_send.at[0], q_recv.at[0],
        device_id={"tp": sibling}, device_id_type=MESH,
    )
    def w_pass(rows):
        return pltpu.make_async_remote_copy(
            wfull.at[across, rows], wfull.at[across, rows], w_send.at[0], q_recv.at[0],
            device_id={"tp": sibling}, device_id_type=MESH,
        )

    def ring_rows(way, e):
        spot = lax.rem(place + (e // 2 if way else size - e // 2), size)
        side = 1 - lax.rem(e, 2) if way else lax.rem(e, 2)
        return pl.ds(pl.multiple_of(spot * slab + side * half, half), half)

    def ring_copy(way, e):
        at = ring_rows(way, e)
        return pltpu.make_async_remote_copy(
            wfull.at[across, at], wfull.at[across, at], w_send.at[0], g_recv.at[e],
            device_id={"sp": left if way else right}, device_id_type=MESH,
        )

    def ring_turn(e):
        landed_slab = wfull.at[across, pl.ds(0, slab)]
        pltpu.make_async_remote_copy(
            landed_slab, landed_slab, w_send.at[0], g_recv.at[e],
            device_id={"sp": right}, device_id_type=MESH,
        ).wait_recv()
        for way in range(2):
            @pl.when(e + 2 < events)
            def _():
                ring_copy(way, e + 2).start()

            w_pass(ring_rows(way, e + 2)).start()

    beside = pltpu.make_async_remote_copy(
        held.at[me], held.at[me], t_send.at[0], s_recv.at[0],
        device_id={"tp": sibling}, device_id_type=MESH,
    )

    def piece(i):
        return pl.ds(pl.multiple_of(i * CHUNK, CHUNK), CHUNK)

    def crossing(i):
        return pltpu.make_async_remote_copy(
            held.at[me, piece(i)], held.at[me, piece(i)], t_send.at[0], x_recv.at[i],
            device_id={"tp": across}, device_id_type=MESH,
        )

    def relay(i):
        return pltpu.make_async_remote_copy(
            held.at[across, piece(i)], held.at[across, piece(i)], t_send.at[0], f_recv.at[i],
            device_id={"tp": sibling}, device_id_type=MESH,
        )

    pltpu.make_async_copy(wfull.at[across], wfull.at[me], l_sem.at[0]).wait()
    w_across.start()
    own_t.wait()
    beside.start()
    for i in range(count):
        crossing(i).start()
    w_beside.start()
    for copy in small:
        copy.wait()

    row = lax.broadcasted_iota(jnp.int32, (CHUNK, CHUNK), 0)
    col = lax.broadcasted_iota(jnp.int32, (CHUNK, CHUNK), 1)
    lower, upper = row >= col, row <= col
    lower_f, upper_f = lower.astype(F32), upper.astype(F32)
    lower_2 = jnp.concatenate([lower_f, lower_f], axis=1).astype(BF16)
    upper_2 = jnp.concatenate([upper_f, upper_f], axis=1).astype(BF16)

    def sums(c, _):
        add = added[:, piece(c)]
        cols[0, c] = dot_t(lower_f, add, EXACT)
        cols[1, c] = dot_t(upper_f, add, EXACT)
        rows_of[0, c] = dot(add, upper_f, EXACT)
        rows_of[1, c] = dot(add, lower_f, EXACT)
        return 0

    lax.fori_loop(0, count, sums, 0)
    for h in range(heads):
        for d in range(2):
            turned[h, :, d * DEPTH : (d + 1) * DEPTH] = initial[d, h].T
    state[...] = jnp.zeros_like(state)
    offset[...] = jnp.zeros_like(offset)
    before[...] = jnp.zeros_like(before)
    before_keep[...] = jnp.ones_like(before_keep)
    for d in range(2):
        _, _, source = partner(d, 1)
        begin = 0 if d == 0 else RIM + length

        @pl.when(jnp.logical_not(source))
        def _():
            padded[pl.ds(begin, RIM), :] = jnp.zeros((RIM, columns), BF16)

    pair = me // 2
    near, far = 2 * pair, 2 - 2 * pair

    def normed(first, at):
        parts, squares = [], 0.0
        for o in range(2):
            x = held[first + o, at, :].astype(F32)
            squares = squares + jnp.sum(x * x, axis=1, keepdims=True)
            lanes = pl.ds(pl.multiple_of((first + o) * width, width), width)
            parts.append((x * gain[:, lanes]).astype(BF16))
        return jnp.concatenate(parts, axis=1), squares

    def depth_of(first):
        return pl.ds(pl.multiple_of(first * width, 2 * width), 2 * width)

    pltpu.make_async_copy(wide, wide, l_sem.at[2]).wait()
    beside.wait_recv()

    def own(i, _):
        at = pl.ds(pl.multiple_of(i * share, share), share)
        x, squares = normed(near, at)
        square[at, :] = squares
        for j in range(6):
            acc[j, at, :] = dot(x, wide[j, depth_of(near), :])
        return 0

    lax.fori_loop(0, 4, own, 0)
    w_across.wait_recv()
    for e in range(min(2, events)):
        for way in range(2):
            ring_copy(way, e).start()
    w_pass(mine).start()

    def gates(pre, gap_row, sums):
        enter = gap_row * (1.0 / (1.0 + jnp.exp(pre)))
        keep = jnp.log1p(-enter)
        high = keep.astype(BF16)
        low = (keep - high.astype(F32)).astype(BF16)
        return enter, dot(sums, jnp.concatenate([high, low], axis=0))

    def local(c):
        at = piece(c)
        x = query_pre[at, :].astype(F32)
        query = x / (1.0 + jnp.exp(-x))
        q_f, q_b = query * jnp.exp(runs[0, at, :]), query * jnp.exp(runs[1, at, :])
        e_f, e_b = ent[0, at, :], ent[1, at, :]
        values = value[at, :]
        col_f, col_b = cols[0, c], cols[1, c]
        row_f, row_b = rows_of[0, c], rows_of[1, c]
        for h in range(heads):
            lanes = slice(h * DEPTH, (h + 1) * DEPTH)
            a_col, b_col = col_f[:, h : h + 1], col_b[:, h : h + 1]
            fade = jnp.exp(
                jnp.where(lower, a_col - row_f[h : h + 1, :], b_col - row_b[h : h + 1, :])
            )
            w_f = dot_t(q_f[:, lanes].astype(BF16), e_f[:, lanes])
            w_b = dot_t(q_b[:, lanes].astype(BF16), e_b[:, lanes])
            weight = (jnp.where(lower, w_f, 0.0) + jnp.where(upper, w_b, 0.0)) * fade
            inner[at, lanes] = dot(weight.astype(BF16), values[:, lanes])
            reach[h, at, :DEPTH] = (q_f[:, lanes] * jnp.exp(a_col)).astype(BF16)
            reach[h, at, DEPTH:] = (q_b[:, lanes] * jnp.exp(b_col)).astype(BF16)

    def project(j, x, scale, at):
        return ((acc[j, at, :] + dot(x, wide[j, depth_of(far), :])) * scale).astype(BF16)

    def late_pool(c, rows=None):
        slot = lax.rem(c, 2)
        if rows is None:
            rows = project(5, kept_x[slot], kept_scale[slot], piece(c))
        padded[pl.ds(pl.multiple_of(c * CHUNK + RIM, RIM), CHUNK), :] = rows

    def late(c, again=None):
        at, x, scale = piece(c), kept_x[lax.rem(c, 2)], kept_scale[lax.rem(c, 2)]
        again = again or (lambda j: project(j, x, scale, at))
        query_pre[at, :] = again(0)
        gate = again(4).astype(F32)
        gated[at, :] = head_gain[...] / (1.0 + jnp.exp(-gate))

    def step(i, _):
        at = piece(i)
        crossing(i).wait_recv()
        relay(i).start()
        @pl.when(i > 0)
        def _():
            late_pool(i - 1)
            late(i - 1)
            local(i - 1)

        @pl.when((i > 0) & (i <= events))
        def _():
            ring_turn(i - 1)

        @pl.when(i == 1)
        def _():
            edge_start(1, length, padded, e_send, e_recv)

        relay(i).wait_recv()
        x, squares = normed(far, at)
        scale = lax.rsqrt((square[at, :] + squares) / features + EPSILON)
        kept_x[lax.rem(i, 2)], kept_scale[lax.rem(i, 2)] = x, scale
        advance(i, *(project(j, x, scale, at) for j in (1, 2, 3)))
        return 0

    def last_step():
        i = count - 1
        at, slot = piece(i), i % 2

        def half(owner):
            x = held[owner, at, :].astype(F32)
            lanes = pl.ds(pl.multiple_of(owner * width, width), width)
            part = (x * gain[:, lanes]).astype(BF16)
            inside = pl.ds(pl.multiple_of((owner - far) * width, width), width)
            kept_x[slot, :, inside] = part
            return part, jnp.sum(x * x, axis=1, keepdims=True)

        def rows_of_w(owner):
            return pl.ds(pl.multiple_of(owner * width, width), width)

        crossing(i).wait_recv()
        relay(i).start()
        x, squares = half(across)
        square[at, :] = square[at, :] + squares
        for j in range(6):
            acc[j, at, :] = acc[j, at, :] + dot(x, wide[j, rows_of_w(across), :])
        relay(i).wait_recv()
        x, squares = half(opposite)
        scale = lax.rsqrt((square[at, :] + squares) / features + EPSILON)
        kept_scale[slot] = scale

        def project_half(j):
            y = acc[j, at, :] + dot(x, wide[j, rows_of_w(opposite), :])
            return (y * scale).astype(BF16)

        advance(i, *(project_half(j) for j in (1, 2, 3)))

    def advance(i, pre_f, pre_b, values):
        at = piece(i)
        value[at, :] = values
        enter_f, run_f = gates(pre_f.astype(F32), gap[0:1, :], lower_2)
        enter_b, run_b = gates(pre_b.astype(F32), gap[1:2, :], upper_2)
        runs[0, at, :], runs[1, at, :] = run_f, run_b
        e_f, e_b = enter_f * jnp.exp(-run_f), enter_b * jnp.exp(-run_b)
        ent[0, at, :], ent[1, at, :] = e_f.astype(BF16), e_b.astype(BF16)
        close_f, close_b = run_f[CHUNK - 1 : CHUNK, :], run_b[0:1, :]
        last_f, last_b = e_f * jnp.exp(close_f), e_b * jnp.exp(close_b)
        offsets[0, i] = offset[0]
        col_f, col_b = cols[0, i], cols[1, i]
        for h in range(heads):
            lanes = slice(h * DEPTH, (h + 1) * DEPTH)
            a_col, b_col = col_f[:, h : h + 1], col_b[:, h : h + 1]
            a_end, b_end = a_col[CHUNK - 1 : CHUNK, :], b_col[0:1, :]
            total_f = close_f[:, lanes] + a_end
            ends_f = (last_f[:, lanes] * jnp.exp(a_end - a_col)).astype(BF16)
            ends_b = (last_b[:, lanes] * jnp.exp(b_end - b_col)).astype(BF16)
            ends = t_dot(values[:, lanes], jnp.concatenate([ends_f, ends_b], axis=1))
            starts[i, h, :, :DEPTH] = state[0, h]
            state[0, h] = jnp.exp(total_f) * state[0, h] + ends[:, :DEPTH]
            chunk_state[i, h] = ends[:, DEPTH:]
            chunk_keep[i, :, lanes] = close_b[:, lanes] + b_end
            offset[0, :, lanes] = offset[0, :, lanes] + total_f

    lax.fori_loop(0, count - 1, step, 0)
    last_step()

    def descend(h):
        lanes = slice(h * DEPTH, (h + 1) * DEPTH)

        def one(i, _):
            c = count - 1 - i
            offsets[1, c, :, lanes] = offset[1, :, lanes]
            starts[c, h, :, DEPTH:] = state[1, h]
            keep = chunk_keep[c, :, lanes]
            state[1, h] = jnp.exp(keep) * state[1, h] + chunk_state[c, h]
            offset[1, :, lanes] = offset[1, :, lanes] + keep
            return 0

        lax.fori_loop(0, count, one, 0)

    window = jnp.left_shift(jnp.int32(2), lax.axis_index("tp") * groups)
    sequence, first_row = length * lax.axis_size("sp"), lax.axis_index("sp") * length

    def pooled(owner):
        begin = pl.multiple_of(owner * share, share)
        span = share + 2 * RIM
        near_rows = padded[pl.ds(begin, span), :]
        target = first_row + begin + lax.broadcasted_iota(jnp.int32, (share, span), 0)
        source = first_row + begin - RIM + lax.broadcasted_iota(jnp.int32, (share, span), 1)
        low = target - window // 2
        inside = (source >= low) & (source < low + window) & (source >= 0) & (source < sequence)
        start = first_row + begin + lax.broadcasted_iota(jnp.int32, (share, 1), 0) - window // 2
        number = jnp.minimum(start + window, sequence) - jnp.maximum(start, 0)
        mean = dot(inside.astype(F32).astype(BF16), near_rows) / number.astype(F32)
        here = padded[pl.ds(pl.multiple_of(begin + RIM, RIM), share), :].astype(F32)
        return (dot((mean - here).astype(BF16), mix[0]) * pool_gain[...]).astype(BF16)

    def pool_copy(r):
        return pltpu.make_async_remote_copy(
            passed.at[r], brought.at[me], a_send.at[0], a_recv.at[0],
            device_id={"tp": jnp.int32(r)}, device_id_type=MESH,
        )

    pool_all = pltpu.make_async_remote_copy(
        passed.at[pl.ds(0, 3)], brought.at[pl.ds(0, 3)], a_send.at[0], a_recv.at[0],
        device_id={"tp": sibling}, device_id_type=MESH,
    )

    def pool_away(r):
        if r == 3:
            edge_wait(1, length, padded, e_send, e_recv)
        if r == 0:
            edge_wait(0, length, padded, e_send, e_recv)
        rows = pooled(r)
        passed[r] = rows

        @pl.when(me == r)
        def _():
            brought[r] = rows

        @pl.when(me != r)
        def _():
            pool_copy(r).start()

    def ring_end():
        for e in range(count - 2, events):
            ring_turn(e)

    def drain_gather():
        for block, sem in ((held, t_send), (wfull, w_send)):
            rows = block.at[pl.ds(0, 3)]
            pltpu.make_async_remote_copy(
                rows, rows, sem.at[0], s_recv.at[0],
                device_id={"tp": sibling}, device_id_type=MESH,
            ).wait_send()

    def drain_scan():
        for d in range(2):
            exists, _, _ = partner(d, 1)

            @pl.when(exists)
            def _():
                edge_copy(d, length, padded, e_send, e_recv).wait_send()

        scan_drain(steps, landed, p_send, p_recv)
        pool_all.wait_send()

    def half_again(j):
        at = piece(count - 1)
        owner = pl.ds(pl.multiple_of(opposite * width, width), width)
        inside = pl.ds(pl.multiple_of((opposite - far) * width, width), width)
        slot = (count - 1) % 2
        y = acc[j, at, :] + dot(kept_x[slot, :, inside], wide[j, owner, :])
        return (y * kept_scale[slot]).astype(BF16)

    def late_last():
        late_pool(count - 2)
        late(count - 2)
        local(count - 2)
        for h in range(1, heads):
            for d in range(2):
                raw_start(d, h, state, offset, *scan)
        for h in range(heads):
            for d in range(2):
                raw_rest(d, h, *scan)
        late(count - 1, half_again)
        local(count - 1)

    tile = 512
    tiles = out.shape[1] // tile

    def wide_pool():
        pltpu.make_async_remote_copy(
            wfull.at[pl.ds(0, 2)], wfull.at[pl.ds(0, 2)], w_send.at[0], q_recv.at[0],
            device_id={"tp": sibling}, device_id_type=MESH,
        ).wait_recv()
        pool_all.wait_recv()
        for j in range(tiles):
            lanes = slice(j * tile, (j + 1) * tile)
            y = dot(brought[0], wfull[0, depth:, lanes])
            for r in range(1, 4):
                y = y + dot(brought[r], wfull[r, depth:, lanes])
            total[:, lanes] = y

    def finished(c, h):
        at, lanes = piece(c), slice(h * DEPTH, (h + 1) * DEPTH)
        ages = jnp.exp(jnp.concatenate([offsets[0, c, :, lanes], offsets[1, c, :, lanes]], axis=1))
        enter = (starts[c, h] + ages * turned[h]).astype(BF16)
        both = inner[at, lanes] + dot_t(reach[h, at, :], enter)
        both = both * lax.rsqrt(jnp.mean(both * both, axis=1, keepdims=True) + EPSILON)
        given[h, at, :] = (both * gated[at, lanes]).astype(BF16)

    relations = (across, opposite, sibling, me)

    def recur_copy(k, h):
        there = relations[k]
        at = pl.ds(pl.multiple_of(there * share, share), share)
        return pltpu.make_async_remote_copy(
            given.at[h, at], taken.at[me, h], c_send.at[0], c_recv.at[heads if k == 2 else h],
            device_id={"tp": there}, device_id_type=MESH,
        )

    def recur_wait(owners, count, sem):
        block = taken.at[pl.ds(0, owners), pl.ds(0, count)]
        return pltpu.make_async_remote_copy(
            block, block, c_send.at[0], c_recv.at[sem],
            device_id={"tp": sibling}, device_id_type=MESH,
        )

    def away(k, h):
        for sub in range(subs):
            finished(relations[k] * subs + sub, h)
        if k < 3:
            recur_copy(k, h).start()

    scan = (sent, landed, before, before_keep, p_send, p_recv)
    place_in_group = group_place()[1]
    always = place_in_group >= 0
    leads = (place_in_group >= group_size() // 2, place_in_group < group_size() // 2)

    def close_rest():
        for h in range(heads):
            for d in range(2):
                scan_close(0, d, h, leads[1 - d] if steps > 1 else always, *scan)

    fillers = [
        [late_last, ring_end] + [functools.partial(pool_away, r) for r in (1, 2, 3)]
        + ([] if steps > 1 else [lambda: pool_away(0), close_rest, drain_gather]),
        [close_rest, drain_gather] if steps > 1 else [],
    ]
    rounds = [[] for _ in range(steps)]
    for i, group in enumerate(fillers):
        rounds[min(i, len(rounds) - 1)].extend(group)
    for k in range(steps):
        if k == 0:
            raw_start(0, 0, state, offset, *scan)
            descend(0)
            raw_start(1, 0, state, offset, *scan)
            for h in range(1, heads):
                descend(h)
            late_pool(count - 1, half_again(5))
            edge_start(0, length, padded, e_send, e_recv)
        for h in range(heads if k else 0):
            for d in range(2):
                scan_close(k - 1, d, h, leads[d] if k == 1 else always, *scan)
            for d in range(2):
                total_start(k, d, h, state, offset, *scan)
            if k == 1 and h == 0:
                pool_away(0)
        for filler in rounds[k]:
            filler()
    for h in range(heads):
        for d in range(2):
            scan_close(steps - 1, d, h, always, *scan)
            lanes = slice(d * DEPTH, (d + 1) * DEPTH)
            keep = before_keep[d, :, h * DEPTH : (h + 1) * DEPTH]
            turned[h, :, lanes] = keep * turned[h, :, lanes] + before[d, h]
        for k in range(2):
            away(k, h)
    for k in (2, 3):
        for h in range(heads):
            away(k, h)

    def all_heads(rows):
        return jnp.concatenate([rows(h) for h in range(heads)], axis=1)

    def far_part(h, lanes):
        rows = slice(h * DEPTH, (h + 1) * DEPTH)
        return dot(
            jnp.concatenate([taken[across, h], taken[opposite, h]], axis=1),
            jnp.concatenate([wfull[across, rows, lanes], wfull[opposite, rows, lanes]], axis=0),
        )

    wide_pool()
    recur_wait(1, heads, heads).wait_recv()
    home = pl.ds(pl.multiple_of(me * share, share), share)
    for j in range(tiles):
        lanes = slice(j * tile, (j + 1) * tile)
        y = total[:, lanes] + dot(
            all_heads(lambda h: given[h, home, :]), wfull[me, :depth, lanes]
        )
        total[:, lanes] = y + dot(
            all_heads(lambda h: taken[sibling, h]), wfull[sibling, :depth, lanes]
        )
    drain_scan()
    for h in range(heads - 1):
        recur_wait(1, 2, h).wait_recv()
        for j in range(tiles):
            lanes = slice(j * tile, (j + 1) * tile)
            total[:, lanes] = total[:, lanes] + far_part(h, lanes)
    recur_wait(1, 2, heads - 1).wait_recv()
    for j in range(tiles):
        lanes = slice(j * tile, (j + 1) * tile)
        out[:, lanes] = (total[:, lanes] + far_part(heads - 1, lanes)).astype(BF16)
    recur_wait(3, heads, 0).wait_send()


def shards(
    tokens, norm_gain, w_query, w_forget_fwd, w_forget_bwd, w_value, w_gate, w_pool_in,
    forget_gap, added_log_retention, initial_state, head_gain, pool_mix, pool_gain,
    w_out_recur, w_out_pool,
):
    weights = (w_query, w_forget_fwd, w_forget_bwd, w_value, w_gate, w_pool_in)
    length, width = tokens.shape
    features, columns = w_query.shape
    heads = columns // DEPTH
    count = length // CHUNK
    share = length // 4
    subs = share // CHUNK
    depth, out_width = w_out_recur.shape
    steps = 1 + len(group_strides())
    size = ring_size()
    events = size - 1
    slots = group_size() + steps - 1
    dma = pltpu.SemaphoreType.DMA
    operands = (
        tokens, norm_gain[None, :], *weights, forget_gap, added_log_retention.T, initial_state,
        head_gain[None, :], pool_mix, pool_gain[None, :], w_out_recur, w_out_pool,
    )

    def like(array):
        return pltpu.VMEM(array.shape, array.dtype)

    return pl.pallas_call(
        functools.partial(mixer_kernel, pool_mix.shape[0]),
        out_shape=pltpu.VMEM((share, out_width), BF16),
        in_specs=[ANY] * len(operands),
        out_specs=VM,
        scratch_shapes=[
            pltpu.VMEM((4, length, width), BF16),
            like(operands[1]),
            pltpu.VMEM((6, features, columns), BF16),
            like(operands[8]), like(operands[9]), like(operands[10]), like(operands[11]),
            like(operands[12]), like(operands[13]),
            pltpu.VMEM((4, 2 * depth, out_width), BF16),
            pltpu.VMEM((6, length, columns), F32),
            pltpu.VMEM((length, 1), F32),
            pltpu.VMEM((2, count, CHUNK, heads), F32),
            pltpu.VMEM((2, count, heads, CHUNK), F32),
            pltpu.VMEM((heads, DEPTH, 2 * DEPTH), F32),
            pltpu.VMEM((length, columns), BF16),
            pltpu.VMEM((length, columns), BF16),
            pltpu.VMEM((length, columns), F32),
            pltpu.VMEM((2, length, columns), BF16),
            pltpu.VMEM((2, length, columns), F32),
            pltpu.VMEM((length, columns), F32),
            pltpu.VMEM((heads, length, 2 * DEPTH), BF16),
            pltpu.VMEM((count, heads, DEPTH, 2 * DEPTH), F32),
            pltpu.VMEM((2, count, 1, columns), F32),
            pltpu.VMEM((count, heads, DEPTH, DEPTH), F32),
            pltpu.VMEM((count, 1, columns), F32),
            pltpu.VMEM((2, heads, DEPTH, DEPTH), F32),
            pltpu.VMEM((2, 1, columns), F32),
            pltpu.VMEM((length + 2 * RIM, columns), BF16),
            pltpu.VMEM((steps, 2, heads, DEPTH + 16, DEPTH), BF16),
            pltpu.VMEM((slots, 2, heads, DEPTH + 16, DEPTH), BF16),
            pltpu.VMEM((2, heads, DEPTH, DEPTH), F32),
            pltpu.VMEM((2, 1, columns), F32),
            pltpu.VMEM((heads, length, DEPTH), BF16),
            pltpu.VMEM((4, heads, share, DEPTH), BF16),
            pltpu.VMEM((4, share, columns), BF16),
            pltpu.VMEM((4, share, columns), BF16),
            pltpu.VMEM((share, out_width), F32),
            pltpu.VMEM((2, CHUNK, 2 * width), BF16),
            pltpu.VMEM((2, CHUNK, 1), F32),
            dma((10,)), dma((1,)), dma((1,)), dma((1,)), dma((count,)), dma((count,)),
            dma((1,)), dma((1,)), dma((events,)),
            dma((2 * steps - 1,)), dma((steps, 2, heads)), dma((2,)), dma((2,)),
            dma((1,)), dma((1,)), dma((1,)), dma((heads + 1,)),
        ],
        compiler_params=pltpu.CompilerParams(
            collective_id=0, has_side_effects=True, vmem_limit_bytes=VMEM_LIMIT
        ),
        name="mixer",
    )(*(pltpu.with_memory_space_constraint(x, pltpu.HBM) for x in operands))


def solution(mesh):
    in_specs = (
        P("sp", "tp"), P(), P(None, "tp"), P(None, "tp"), P(None, "tp"), P(None, "tp"),
        P(None, "tp"), P(None, "tp"), P(None, "tp"), P("sp", "tp"), P(None, "tp", None, None),
        P("tp"), P("tp", None, None), P("tp"), P("tp", None), P("tp", None),
    )
    out_specs = P(("sp", "tp"), None)
    return jax.shard_map(shards, mesh=mesh, in_specs=in_specs, out_specs=out_specs, check_vma=False)
```

```python
import functools

import jax
import jax.numpy as jnp
from jax import lax
from jax.experimental import pallas as pl
from jax.experimental.pallas import tpu as pltpu
from jax.sharding import PartitionSpec as P

DEPTH = 128
CHUNK = 128
EPSILON = 1e-06
RIM = 16
RING = 8
GROUP = 4
MESH = pl.DeviceIdType.MESH
F32 = jnp.float32
BF16 = jnp.bfloat16
VMEM_LIMIT = 52 * 1024 * 1024
ANY = pl.BlockSpec(memory_space=pl.ANY)
VM = pl.BlockSpec(memory_space=pltpu.VMEM)
EXACT = lax.Precision.HIGHEST


def dot(a, b, precision=None):
    return jnp.dot(a, b, preferred_element_type=F32, precision=precision)


def dot_t(a, b, precision=None):
    return lax.dot_general(
        a, b, (((1,), (1,)), ((), ())), preferred_element_type=F32, precision=precision
    )


def t_dot(a, b):
    return lax.dot_general(a, b, (((0,), (0,)), ((), ())), preferred_element_type=F32)


def peers():
    me = lax.axis_index("tp")
    sibling = me + 1 - 2 * lax.rem(me, 2)
    across = lax.rem(me + 2, 4)
    return me, sibling, across, lax.rem(sibling + 2, 4)


def partner(d, stride):
    me, count = lax.axis_index("sp"), lax.axis_size("sp")
    above, below = me + stride < count, me >= stride
    return (above, me + stride, below) if d == 0 else (below, me - stride, above)


def group_size():
    return min(GROUP, lax.axis_size("sp"))


def group_strides():
    count = lax.axis_size("sp") // group_size()
    return [1 << k for k in range(count.bit_length()) if 1 << k < count]


def group_place():
    me = lax.axis_index("sp")
    return me // group_size(), lax.rem(me, group_size())


def raw_partner(d, j):
    (_, place), me, size = group_place(), lax.axis_index("sp"), group_size()
    above, below = place + j < size, place >= j
    return (above, me + j, below) if d == 0 else (below, me - j, above)


def group_partner(d, stride):
    (group, place), size = group_place(), group_size()
    count = lax.axis_size("sp") // size
    above, below = group + stride < count, group >= stride
    if d == 0:
        return above & (place >= size - 2), group + stride, below
    return below & (place < 2), group - stride, above


def ring_size():
    return min(RING, lax.axis_size("sp"))


def ring_place():
    size = ring_size()
    me = lax.axis_index("sp")
    base, mine = me - lax.rem(me, size), lax.rem(me, size)
    place = jnp.where(lax.rem(mine, 2) == 0, mine // 2, size - 1 - mine // 2)

    def index(spot):
        spot = lax.rem(spot + size, size)
        return base + jnp.where(spot < size // 2, 2 * spot, 2 * (size - 1 - spot) + 1)

    return place, index(place + 1), index(place - 1)


def greet():
    barrier = pltpu.get_barrier_semaphore()
    _, sibling, across, opposite = peers()
    _, right, left = ring_place()
    for device in (sibling, across, opposite):
        pl.semaphore_signal(barrier, inc=1, device_id={"tp": device}, device_id_type=MESH)
    for device in (right, left):
        pl.semaphore_signal(barrier, inc=1, device_id={"sp": device}, device_id_type=MESH)
    size, (group, place) = group_size(), group_place()
    for j in range(1, size):
        target = group * size + lax.rem(place + j, size)
        pl.semaphore_signal(barrier, inc=1, device_id={"sp": target}, device_id_type=MESH)
    number = jnp.int32(5 + size - 1)
    for stride in group_strides():
        for d in range(2):
            sends, _, gets = group_partner(d, stride)
            source = (group - stride) * size + size - 2 if d == 0 else (group + stride) * size
            source = source + lax.rem(place, 2)

            @pl.when(gets)
            def _():
                pl.semaphore_signal(
                    barrier, inc=1, device_id={"sp": source}, device_id_type=MESH
                )

            number = number + jnp.where(sends, size // 2, 0)
    for d in range(2):
        exists, target, _ = partner(d, 1)
        outside = exists & (place == (size - 1 if d == 0 else 0))

        @pl.when(outside)
        def _():
            pl.semaphore_signal(barrier, inc=1, device_id={"sp": target}, device_id_type=MESH)

        number = number + jnp.where(outside, 1, 0)
    pl.semaphore_wait(barrier, number)


def edge_copy(d, length, padded, e_send, e_recv):
    _, target, _ = partner(d, 1)
    there = 0 if d == 0 else RIM + length
    return pltpu.make_async_remote_copy(
        padded.at[pl.ds(length if d == 0 else RIM, RIM)], padded.at[pl.ds(there, RIM)],
        e_send.at[d], e_recv.at[d], device_id={"sp": target}, device_id_type=MESH,
    )


def edge_start(d, length, padded, e_send, e_recv):
    exists, _, _ = partner(d, 1)

    @pl.when(exists)
    def _():
        edge_copy(d, length, padded, e_send, e_recv).start()


def edge_wait(d, length, padded, e_send, e_recv):
    _, _, source = partner(d, 1)

    @pl.when(source)
    def _():
        edge_copy(d, length, padded, e_send, e_recv).wait_recv()


def scan_copy(slot, k, d, h, target, sent, landed, p_send, p_recv):
    return pltpu.make_async_remote_copy(
        sent.at[k, d, h], landed.at[slot, d, h],
        p_send.at[2 * k - 1 + d if k else 0], p_recv.at[k, d, h],
        device_id={"sp": target}, device_id_type=MESH,
    )


def raw_sends(d):
    size, (_, place), me = group_size(), group_place(), lax.axis_index("sp")
    rows = []
    for j in range(size - 1, 0, -1):
        exists, target, _ = raw_partner(d, j)
        rows.append((j - 1, exists, target, place + j >= size - 2 if d == 0 else place - j < 2))
    if d == 0:
        extra = (size - 1, place == size - 1, me - 1, place >= 0)
    else:
        extra = (size - 1, place == 0, me + 1, place >= 0)
    return [extra] + rows


def raw_start(d, h, state, offset, sent, landed, before, before_keep, p_send, p_recv):
    lanes = slice(h * DEPTH, (h + 1) * DEPTH)
    sent[0, d, h, :DEPTH, :] = state[d, h].astype(BF16)
    sent[0, d, h, DEPTH:, :] = jnp.broadcast_to(
        jnp.exp(offset[d, :, lanes]), (16, DEPTH)
    ).astype(BF16)
    for slot, exists, target, boundary in raw_sends(d):
        @pl.when(exists & boundary)
        def _():
            scan_copy(slot, 0, d, h, target, sent, landed, p_send, p_recv).start()


def raw_rest(d, h, sent, landed, before, before_keep, p_send, p_recv):
    for slot, exists, target, boundary in raw_sends(d):
        @pl.when(exists & jnp.logical_not(boundary))
        def _():
            scan_copy(slot, 0, d, h, target, sent, landed, p_send, p_recv).start()


def total_start(k, d, h, state, offset, sent, landed, before, before_keep, p_send, p_recv):
    size, (_, place) = group_size(), group_place()
    sends, group, _ = group_partner(d, group_strides()[k - 1])
    inner = place == (size - 2 if d == 0 else 1)
    lanes = slice(h * DEPTH, (h + 1) * DEPTH)

    def send(values, keep):
        sent[k, d, h, :DEPTH, :] = values.astype(BF16)
        sent[k, d, h, DEPTH:, :] = jnp.broadcast_to(keep, (16, DEPTH)).astype(BF16)
        for pair in range(size // 2 - 1, -1, -1) if d == 0 else range(size // 2):
            target = group * size + 2 * pair + lax.rem(place, 2)
            scan_copy(size + k - 1, k, d, h, target, sent, landed, p_send, p_recv).start()

    @pl.when(sends & jnp.logical_not(inner))
    def _():
        keep = jnp.exp(offset[d, :, lanes])
        send(keep * before[d, h] + state[d, h], keep * before_keep[d, :, lanes])

    @pl.when(sends & inner)
    def _():
        last = landed[size - 1, d, h].astype(F32)
        keep = jnp.exp(offset[d, :, lanes])
        last_keep = last[DEPTH : DEPTH + 1]
        send(
            last_keep * (keep * before[d, h] + state[d, h]) + last[:DEPTH],
            last_keep * (keep * before_keep[d, :, lanes]),
        )


def scan_wait(block, send, recv):
    return pltpu.make_async_remote_copy(
        block, block, send, recv, device_id={"sp": 0}, device_id_type=MESH
    )


def scan_close(k, d, h, only, sent, landed, before, before_keep, p_send, p_recv):
    size, (_, place) = group_size(), group_place()

    def add(slot):
        lanes = slice(h * DEPTH, (h + 1) * DEPTH)
        keep = before_keep[d, :, lanes]
        early = landed[slot, d, h].astype(F32)
        before[d, h] = keep * early[:DEPTH] + before[d, h]
        before_keep[d, :, lanes] = keep * early[DEPTH : DEPTH + 1]

    def wait(block):
        scan_wait(block, p_send.at[0], p_recv.at[k, d, h]).wait_recv()

    if k:
        @pl.when(group_partner(d, group_strides()[k - 1])[2] & only)
        def _():
            wait(landed.at[0, d, h])
            add(size + k - 1)

        return
    boundary = place >= size - 2 if d == 0 else place < 2

    @pl.when(only & boundary)
    def _():
        wait(landed.at[pl.ds(0, size - 1), d, h])
        for j in range(1, size):
            pl.when(raw_partner(d, j)[2])(functools.partial(add, j - 1))

    @pl.when(only & jnp.logical_not(boundary) & raw_partner(d, 1)[2])
    def _():
        wait(landed.at[0, d, h])
        add(0)


def scan_drain(steps, landed, p_send, p_recv):
    size, (_, place) = group_size(), group_place()
    outer = (place == 0) | (place == size - 1)
    leaving = [
        (0, outer, landed.at[pl.ds(0, size // 2)]),
        (0, jnp.logical_not(outer), landed.at[pl.ds(0, size - 1), 0]),
    ]
    for k in range(1, steps):
        for d in range(2):
            sends = group_partner(d, group_strides()[k - 1])[0]
            leaving.append((2 * k - 1 + d, sends, landed.at[pl.ds(0, size // 4)]))
    for index, sends, block in leaving:
        @pl.when(sends)
        def _():
            scan_wait(block, p_send.at[index], p_recv.at[0, 0, 0]).wait_send()


def mixer_kernel(groups, *refs):
    (h_tokens, h_gain, *h_weights) = refs[:8]
    (h_gap, h_added, h_initial, h_head, h_mix, h_scale, h_recur, h_pool) = refs[8:16]
    out = refs[16]
    (
        held, gain, wide, gap, added, initial, head_gain, mix, pool_gain, wfull,
        acc, square, cols, rows_of, turned, query_pre, value, gated, ent, runs, inner, reach,
        starts, offsets, chunk_state, chunk_keep, state, offset, padded,
        sent, landed, before, before_keep, given, taken, passed, brought, total, kept_x, kept_scale,
        l_sem, t_send, w_send, s_recv, x_recv, f_recv, w_recv, q_recv, g_recv,
        p_send, p_recv, e_send, e_recv, a_send, a_recv, c_send, c_recv,
    ) = refs[17:]
    me, sibling, across, opposite = peers()
    length, width = held.shape[1:]
    columns = wide.shape[2]
    heads = columns // DEPTH
    count = length // CHUNK
    share = length // 4
    subs = share // CHUNK
    features = 4 * width
    depth = wfull.shape[1] // 2
    steps = 1 + len(group_strides())

    own_w = [
        pltpu.make_async_copy(h_recur, wfull.at[me, pl.ds(0, depth)], l_sem.at[0]),
        pltpu.make_async_copy(h_pool, wfull.at[me, pl.ds(depth, depth)], l_sem.at[0]),
    ]
    own_t = pltpu.make_async_copy(h_tokens, held.at[me], l_sem.at[1])
    small = [
        pltpu.make_async_copy(a, b, l_sem.at[3 + i])
        for i, (a, b) in enumerate((
            (h_gain, gain), (h_gap, gap), (h_added, added), (h_initial, initial),
            (h_head, head_gain), (h_mix, mix), (h_scale, pool_gain),
        ))
    ]
    loads = [
        pltpu.make_async_copy(w, wide.at[i], l_sem.at[2]) for i, w in enumerate(h_weights)
    ]
    for copy in own_w + [own_t] + small + loads:
        copy.start()
    greet()

    size = ring_size()
    slab = 2 * depth // size
    half = slab // 2
    place, right, left = ring_place()
    events = size - 1

    mine = pl.ds(pl.multiple_of(place * slab, slab), slab)
    w_across = pltpu.make_async_remote_copy(
        wfull.at[me, mine], wfull.at[me, mine], w_send.at[0], w_recv.at[0],
        device_id={"tp": across}, device_id_type=MESH,
    )
    w_beside = pltpu.make_async_remote_copy(
        wfull.at[me], wfull.at[me], w_send.at[0], q_recv.at[0],
        device_id={"tp": sibling}, device_id_type=MESH,
    )
    def w_pass(rows):
        return pltpu.make_async_remote_copy(
            wfull.at[across, rows], wfull.at[across, rows], w_send.at[0], q_recv.at[0],
            device_id={"tp": sibling}, device_id_type=MESH,
        )

    def ring_rows(way, e):
        spot = lax.rem(place + (e // 2 if way else size - e // 2), size)
        side = 1 - lax.rem(e, 2) if way else lax.rem(e, 2)
        return pl.ds(pl.multiple_of(spot * slab + side * half, half), half)

    def ring_copy(way, e):
        at = ring_rows(way, e)
        return pltpu.make_async_remote_copy(
            wfull.at[across, at], wfull.at[across, at], w_send.at[0], g_recv.at[e],
            device_id={"sp": left if way else right}, device_id_type=MESH,
        )

    def ring_turn(e):
        landed_slab = wfull.at[across, pl.ds(0, slab)]
        pltpu.make_async_remote_copy(
            landed_slab, landed_slab, w_send.at[0], g_recv.at[e],
            device_id={"sp": right}, device_id_type=MESH,
        ).wait_recv()
        for way in range(2):
            @pl.when(e + 2 < events)
            def _():
                ring_copy(way, e + 2).start()

            w_pass(ring_rows(way, e + 2)).start()

    beside = pltpu.make_async_remote_copy(
        held.at[me], held.at[me], t_send.at[0], s_recv.at[0],
        device_id={"tp": sibling}, device_id_type=MESH,
    )

    def piece(i):
        return pl.ds(pl.multiple_of(i * CHUNK, CHUNK), CHUNK)

    def crossing(i):
        return pltpu.make_async_remote_copy(
            held.at[me, piece(i)], held.at[me, piece(i)], t_send.at[0], x_recv.at[i],
            device_id={"tp": across}, device_id_type=MESH,
        )

    def relay(i):
        return pltpu.make_async_remote_copy(
            held.at[across, piece(i)], held.at[across, piece(i)], t_send.at[0], f_recv.at[i],
            device_id={"tp": sibling}, device_id_type=MESH,
        )

    pltpu.make_async_copy(wfull.at[across], wfull.at[me], l_sem.at[0]).wait()
    w_across.start()
    own_t.wait()
    beside.start()
    for i in range(count):
        crossing(i).start()
    w_beside.start()
    for copy in small:
        copy.wait()

    row = lax.broadcasted_iota(jnp.int32, (CHUNK, CHUNK), 0)
    col = lax.broadcasted_iota(jnp.int32, (CHUNK, CHUNK), 1)
    lower, upper = row >= col, row <= col
    lower_f, upper_f = lower.astype(F32), upper.astype(F32)
    lower_2 = jnp.concatenate([lower_f, lower_f], axis=1).astype(BF16)
    upper_2 = jnp.concatenate([upper_f, upper_f], axis=1).astype(BF16)

    def sums(c, _):
        add = added[:, piece(c)]
        cols[0, c] = dot_t(lower_f, add, EXACT)
        cols[1, c] = dot_t(upper_f, add, EXACT)
        rows_of[0, c] = dot(add, upper_f, EXACT)
        rows_of[1, c] = dot(add, lower_f, EXACT)
        return 0

    lax.fori_loop(0, count, sums, 0)
    for h in range(heads):
        for d in range(2):
            turned[h, :, d * DEPTH : (d + 1) * DEPTH] = initial[d, h].T
    state[...] = jnp.zeros_like(state)
    offset[...] = jnp.zeros_like(offset)
    before[...] = jnp.zeros_like(before)
    before_keep[...] = jnp.ones_like(before_keep)
    for d in range(2):
        _, _, source = partner(d, 1)
        begin = 0 if d == 0 else RIM + length

        @pl.when(jnp.logical_not(source))
        def _():
            padded[pl.ds(begin, RIM), :] = jnp.zeros((RIM, columns), BF16)

    pair = me // 2
    near, far = 2 * pair, 2 - 2 * pair

    def normed(first, at):
        parts, squares = [], 0.0
        for o in range(2):
            x = held[first + o, at, :].astype(F32)
            squares = squares + jnp.sum(x * x, axis=1, keepdims=True)
            lanes = pl.ds(pl.multiple_of((first + o) * width, width), width)
            parts.append((x * gain[:, lanes]).astype(BF16))
        return jnp.concatenate(parts, axis=1), squares

    def depth_of(first):
        return pl.ds(pl.multiple_of(first * width, 2 * width), 2 * width)

    pltpu.make_async_copy(wide, wide, l_sem.at[2]).wait()
    beside.wait_recv()

    def own(i, _):
        at = pl.ds(pl.multiple_of(i * share, share), share)
        x, squares = normed(near, at)
        square[at, :] = squares
        for j in range(6):
            acc[j, at, :] = dot(x, wide[j, depth_of(near), :])
        return 0

    lax.fori_loop(0, 4, own, 0)
    w_across.wait_recv()
    for e in range(min(2, events)):
        for way in range(2):
            ring_copy(way, e).start()
    w_pass(mine).start()

    def gates(pre, gap_row, sums):
        enter = gap_row * (1.0 / (1.0 + jnp.exp(pre)))
        keep = jnp.log1p(-enter)
        high = keep.astype(BF16)
        low = (keep - high.astype(F32)).astype(BF16)
        return enter, dot(sums, jnp.concatenate([high, low], axis=0))

    def local(c):
        at = piece(c)
        x = query_pre[at, :].astype(F32)
        query = x / (1.0 + jnp.exp(-x))
        q_f, q_b = query * jnp.exp(runs[0, at, :]), query * jnp.exp(runs[1, at, :])
        e_f, e_b = ent[0, at, :], ent[1, at, :]
        values = value[at, :]
        col_f, col_b = cols[0, c], cols[1, c]
        row_f, row_b = rows_of[0, c], rows_of[1, c]
        for h in range(heads):
            lanes = slice(h * DEPTH, (h + 1) * DEPTH)
            a_col, b_col = col_f[:, h : h + 1], col_b[:, h : h + 1]
            fade = jnp.exp(
                jnp.where(lower, a_col - row_f[h : h + 1, :], b_col - row_b[h : h + 1, :])
            )
            w_f = dot_t(q_f[:, lanes].astype(BF16), e_f[:, lanes])
            w_b = dot_t(q_b[:, lanes].astype(BF16), e_b[:, lanes])
            weight = (jnp.where(lower, w_f, 0.0) + jnp.where(upper, w_b, 0.0)) * fade
            inner[at, lanes] = dot(weight.astype(BF16), values[:, lanes])
            reach[h, at, :DEPTH] = (q_f[:, lanes] * jnp.exp(a_col)).astype(BF16)
            reach[h, at, DEPTH:] = (q_b[:, lanes] * jnp.exp(b_col)).astype(BF16)

    def project(j, x, scale, at):
        return ((acc[j, at, :] + dot(x, wide[j, depth_of(far), :])) * scale).astype(BF16)

    def late_pool(c, rows=None):
        slot = lax.rem(c, 2)
        if rows is None:
            rows = project(5, kept_x[slot], kept_scale[slot], piece(c))
        padded[pl.ds(pl.multiple_of(c * CHUNK + RIM, RIM), CHUNK), :] = rows

    def late(c, again=None):
        at, x, scale = piece(c), kept_x[lax.rem(c, 2)], kept_scale[lax.rem(c, 2)]
        again = again or (lambda j: project(j, x, scale, at))
        query_pre[at, :] = again(0)
        gate = again(4).astype(F32)
        gated[at, :] = head_gain[...] / (1.0 + jnp.exp(-gate))

    def step(i, _):
        at = piece(i)
        crossing(i).wait_recv()
        relay(i).start()
        @pl.when(i > 0)
        def _():
            late_pool(i - 1)
            late(i - 1)
            local(i - 1)

        @pl.when((i > 0) & (i <= events))
        def _():
            ring_turn(i - 1)

        @pl.when(i == 1)
        def _():
            edge_start(1, length, padded, e_send, e_recv)

        relay(i).wait_recv()
        x, squares = normed(far, at)
        scale = lax.rsqrt((square[at, :] + squares) / features + EPSILON)
        kept_x[lax.rem(i, 2)], kept_scale[lax.rem(i, 2)] = x, scale
        advance(i, *(project(j, x, scale, at) for j in (1, 2, 3)))
        return 0

    def last_step():
        i = count - 1
        at, slot = piece(i), i % 2

        def half(owner):
            x = held[owner, at, :].astype(F32)
            lanes = pl.ds(pl.multiple_of(owner * width, width), width)
            part = (x * gain[:, lanes]).astype(BF16)
            inside = pl.ds(pl.multiple_of((owner - far) * width, width), width)
            kept_x[slot, :, inside] = part
            return part, jnp.sum(x * x, axis=1, keepdims=True)

        def rows_of_w(owner):
            return pl.ds(pl.multiple_of(owner * width, width), width)

        crossing(i).wait_recv()
        relay(i).start()
        x, squares = half(across)
        square[at, :] = square[at, :] + squares
        for j in range(6):
            acc[j, at, :] = acc[j, at, :] + dot(x, wide[j, rows_of_w(across), :])
        relay(i).wait_recv()
        x, squares = half(opposite)
        scale = lax.rsqrt((square[at, :] + squares) / features + EPSILON)
        kept_scale[slot] = scale

        def project_half(j):
            y = acc[j, at, :] + dot(x, wide[j, rows_of_w(opposite), :])
            return (y * scale).astype(BF16)

        advance(i, *(project_half(j) for j in (1, 2, 3)))

    def advance(i, pre_f, pre_b, values):
        at = piece(i)
        value[at, :] = values
        enter_f, run_f = gates(pre_f.astype(F32), gap[0:1, :], lower_2)
        enter_b, run_b = gates(pre_b.astype(F32), gap[1:2, :], upper_2)
        runs[0, at, :], runs[1, at, :] = run_f, run_b
        e_f, e_b = enter_f * jnp.exp(-run_f), enter_b * jnp.exp(-run_b)
        ent[0, at, :], ent[1, at, :] = e_f.astype(BF16), e_b.astype(BF16)
        close_f, close_b = run_f[CHUNK - 1 : CHUNK, :], run_b[0:1, :]
        last_f, last_b = e_f * jnp.exp(close_f), e_b * jnp.exp(close_b)
        offsets[0, i] = offset[0]
        col_f, col_b = cols[0, i], cols[1, i]
        for h in range(heads):
            lanes = slice(h * DEPTH, (h + 1) * DEPTH)
            a_col, b_col = col_f[:, h : h + 1], col_b[:, h : h + 1]
            a_end, b_end = a_col[CHUNK - 1 : CHUNK, :], b_col[0:1, :]
            total_f = close_f[:, lanes] + a_end
            ends_f = (last_f[:, lanes] * jnp.exp(a_end - a_col)).astype(BF16)
            ends_b = (last_b[:, lanes] * jnp.exp(b_end - b_col)).astype(BF16)
            ends = t_dot(values[:, lanes], jnp.concatenate([ends_f, ends_b], axis=1))
            starts[i, h, :, :DEPTH] = state[0, h]
            state[0, h] = jnp.exp(total_f) * state[0, h] + ends[:, :DEPTH]
            chunk_state[i, h] = ends[:, DEPTH:]
            chunk_keep[i, :, lanes] = close_b[:, lanes] + b_end
            offset[0, :, lanes] = offset[0, :, lanes] + total_f

    lax.fori_loop(0, count - 1, step, 0)
    last_step()

    def descend(h):
        lanes = slice(h * DEPTH, (h + 1) * DEPTH)

        def one(i, _):
            c = count - 1 - i
            offsets[1, c, :, lanes] = offset[1, :, lanes]
            starts[c, h, :, DEPTH:] = state[1, h]
            keep = chunk_keep[c, :, lanes]
            state[1, h] = jnp.exp(keep) * state[1, h] + chunk_state[c, h]
            offset[1, :, lanes] = offset[1, :, lanes] + keep
            return 0

        lax.fori_loop(0, count, one, 0)

    window = jnp.left_shift(jnp.int32(2), lax.axis_index("tp") * groups)
    sequence, first_row = length * lax.axis_size("sp"), lax.axis_index("sp") * length

    def pooled(owner):
        begin = pl.multiple_of(owner * share, share)
        span = share + 2 * RIM
        near_rows = padded[pl.ds(begin, span), :]
        target = first_row + begin + lax.broadcasted_iota(jnp.int32, (share, span), 0)
        source = first_row + begin - RIM + lax.broadcasted_iota(jnp.int32, (share, span), 1)
        low = target - window // 2
        inside = (source >= low) & (source < low + window) & (source >= 0) & (source < sequence)
        start = first_row + begin + lax.broadcasted_iota(jnp.int32, (share, 1), 0) - window // 2
        number = jnp.minimum(start + window, sequence) - jnp.maximum(start, 0)
        mean = dot(inside.astype(F32).astype(BF16), near_rows) / number.astype(F32)
        here = padded[pl.ds(pl.multiple_of(begin + RIM, RIM), share), :].astype(F32)
        return (dot((mean - here).astype(BF16), mix[0]) * pool_gain[...]).astype(BF16)

    def pool_copy(r):
        return pltpu.make_async_remote_copy(
            passed.at[r], brought.at[me], a_send.at[0], a_recv.at[0],
            device_id={"tp": jnp.int32(r)}, device_id_type=MESH,
        )

    pool_all = pltpu.make_async_remote_copy(
        passed.at[pl.ds(0, 3)], brought.at[pl.ds(0, 3)], a_send.at[0], a_recv.at[0],
        device_id={"tp": sibling}, device_id_type=MESH,
    )

    def pool_away(r):
        if r == 3:
            edge_wait(1, length, padded, e_send, e_recv)
        if r == 0:
            edge_wait(0, length, padded, e_send, e_recv)
        rows = pooled(r)
        passed[r] = rows

        @pl.when(me == r)
        def _():
            brought[r] = rows

        @pl.when(me != r)
        def _():
            pool_copy(r).start()

    def ring_end():
        for e in range(count - 2, events):
            ring_turn(e)

    def drain_gather():
        for block, sem in ((held, t_send), (wfull, w_send)):
            rows = block.at[pl.ds(0, 3)]
            pltpu.make_async_remote_copy(
                rows, rows, sem.at[0], s_recv.at[0],
                device_id={"tp": sibling}, device_id_type=MESH,
            ).wait_send()

    def drain_scan():
        for d in range(2):
            exists, _, _ = partner(d, 1)

            @pl.when(exists)
            def _():
                edge_copy(d, length, padded, e_send, e_recv).wait_send()

        scan_drain(steps, landed, p_send, p_recv)
        pool_all.wait_send()

    def half_again(j):
        at = piece(count - 1)
        owner = pl.ds(pl.multiple_of(opposite * width, width), width)
        inside = pl.ds(pl.multiple_of((opposite - far) * width, width), width)
        slot = (count - 1) % 2
        y = acc[j, at, :] + dot(kept_x[slot, :, inside], wide[j, owner, :])
        return (y * kept_scale[slot]).astype(BF16)

    def late_last():
        late_pool(count - 2)
        late(count - 2)
        local(count - 2)
        for h in range(1, heads):
            for d in range(2):
                raw_start(d, h, state, offset, *scan)
        for h in range(heads):
            for d in range(2):
                raw_rest(d, h, *scan)
        late(count - 1, half_again)
        local(count - 1)

    tile = 512
    tiles = out.shape[1] // tile

    def wide_pool():
        pltpu.make_async_remote_copy(
            wfull.at[pl.ds(0, 2)], wfull.at[pl.ds(0, 2)], w_send.at[0], q_recv.at[0],
            device_id={"tp": sibling}, device_id_type=MESH,
        ).wait_recv()
        pool_all.wait_recv()
        for j in range(tiles):
            lanes = slice(j * tile, (j + 1) * tile)
            y = dot(brought[0], wfull[0, depth:, lanes])
            for r in range(1, 4):
                y = y + dot(brought[r], wfull[r, depth:, lanes])
            total[:, lanes] = y

    def finished(c, h):
        at, lanes = piece(c), slice(h * DEPTH, (h + 1) * DEPTH)
        ages = jnp.exp(jnp.concatenate([offsets[0, c, :, lanes], offsets[1, c, :, lanes]], axis=1))
        enter = (starts[c, h] + ages * turned[h]).astype(BF16)
        both = inner[at, lanes] + dot_t(reach[h, at, :], enter)
        both = both * lax.rsqrt(jnp.mean(both * both, axis=1, keepdims=True) + EPSILON)
        given[h, at, :] = (both * gated[at, lanes]).astype(BF16)

    relations = (across, opposite, sibling, me)

    def recur_copy(k, h):
        there = relations[k]
        at = pl.ds(pl.multiple_of(there * share, share), share)
        return pltpu.make_async_remote_copy(
            given.at[h, at], taken.at[me, h], c_send.at[0], c_recv.at[heads if k == 2 else h],
            device_id={"tp": there}, device_id_type=MESH,
        )

    def recur_wait(owners, count, sem):
        block = taken.at[pl.ds(0, owners), pl.ds(0, count)]
        return pltpu.make_async_remote_copy(
            block, block, c_send.at[0], c_recv.at[sem],
            device_id={"tp": sibling}, device_id_type=MESH,
        )

    def away(k, h):
        for sub in range(subs):
            finished(relations[k] * subs + sub, h)
        if k < 3:
            recur_copy(k, h).start()

    scan = (sent, landed, before, before_keep, p_send, p_recv)
    place_in_group = group_place()[1]
    always = place_in_group >= 0
    leads = (place_in_group >= group_size() // 2, place_in_group < group_size() // 2)

    def close_rest():
        for h in range(heads):
            for d in range(2):
                scan_close(0, d, h, leads[1 - d] if steps > 1 else always, *scan)

    fillers = [
        [late_last, ring_end] + [functools.partial(pool_away, r) for r in (1, 2, 3)]
        + ([] if steps > 1 else [lambda: pool_away(0), close_rest, drain_gather]),
        [close_rest, drain_gather] if steps > 1 else [],
    ]
    rounds = [[] for _ in range(steps)]
    for i, group in enumerate(fillers):
        rounds[min(i, len(rounds) - 1)].extend(group)
    for k in range(steps):
        if k == 0:
            raw_start(0, 0, state, offset, *scan)
            descend(0)
            raw_start(1, 0, state, offset, *scan)
            for h in range(1, heads):
                descend(h)
            late_pool(count - 1, half_again(5))
            edge_start(0, length, padded, e_send, e_recv)
        for h in range(heads if k else 0):
            for d in range(2):
                scan_close(k - 1, d, h, leads[d] if k == 1 else always, *scan)
            for d in range(2):
                total_start(k, d, h, state, offset, *scan)
            if k == 1 and h == heads - 1:
                pool_away(0)
        for filler in rounds[k]:
            filler()
    for h in range(heads):
        for d in range(2):
            scan_close(steps - 1, d, h, always, *scan)
            lanes = slice(d * DEPTH, (d + 1) * DEPTH)
            keep = before_keep[d, :, h * DEPTH : (h + 1) * DEPTH]
            turned[h, :, lanes] = keep * turned[h, :, lanes] + before[d, h]
        for k in range(2):
            away(k, h)
    for k in (2, 3):
        for h in range(heads):
            away(k, h)

    def all_heads(rows):
        return jnp.concatenate([rows(h) for h in range(heads)], axis=1)

    def far_part(h, lanes):
        rows = slice(h * DEPTH, (h + 1) * DEPTH)
        return dot(
            jnp.concatenate([taken[across, h], taken[opposite, h]], axis=1),
            jnp.concatenate([wfull[across, rows, lanes], wfull[opposite, rows, lanes]], axis=0),
        )

    wide_pool()
    recur_wait(1, heads, heads).wait_recv()
    home = pl.ds(pl.multiple_of(me * share, share), share)
    for j in range(tiles):
        lanes = slice(j * tile, (j + 1) * tile)
        y = total[:, lanes] + dot(
            all_heads(lambda h: given[h, home, :]), wfull[me, :depth, lanes]
        )
        total[:, lanes] = y + dot(
            all_heads(lambda h: taken[sibling, h]), wfull[sibling, :depth, lanes]
        )
    drain_scan()
    for h in range(heads - 1):
        recur_wait(1, 2, h).wait_recv()
        for j in range(tiles):
            lanes = slice(j * tile, (j + 1) * tile)
            total[:, lanes] = total[:, lanes] + far_part(h, lanes)
    recur_wait(1, 2, heads - 1).wait_recv()
    for j in range(tiles):
        lanes = slice(j * tile, (j + 1) * tile)
        out[:, lanes] = (total[:, lanes] + far_part(heads - 1, lanes)).astype(BF16)
    recur_wait(3, heads, 0).wait_send()


def shards(
    tokens, norm_gain, w_query, w_forget_fwd, w_forget_bwd, w_value, w_gate, w_pool_in,
    forget_gap, added_log_retention, initial_state, head_gain, pool_mix, pool_gain,
    w_out_recur, w_out_pool,
):
    weights = (w_query, w_forget_fwd, w_forget_bwd, w_value, w_gate, w_pool_in)
    length, width = tokens.shape
    features, columns = w_query.shape
    heads = columns // DEPTH
    count = length // CHUNK
    share = length // 4
    subs = share // CHUNK
    depth, out_width = w_out_recur.shape
    steps = 1 + len(group_strides())
    size = ring_size()
    events = size - 1
    slots = group_size() + steps - 1
    dma = pltpu.SemaphoreType.DMA
    operands = (
        tokens, norm_gain[None, :], *weights, forget_gap, added_log_retention.T, initial_state,
        head_gain[None, :], pool_mix, pool_gain[None, :], w_out_recur, w_out_pool,
    )

    def like(array):
        return pltpu.VMEM(array.shape, array.dtype)

    return pl.pallas_call(
        functools.partial(mixer_kernel, pool_mix.shape[0]),
        out_shape=pltpu.VMEM((share, out_width), BF16),
        in_specs=[ANY] * len(operands),
        out_specs=VM,
        scratch_shapes=[
            pltpu.VMEM((4, length, width), BF16),
            like(operands[1]),
            pltpu.VMEM((6, features, columns), BF16),
            like(operands[8]), like(operands[9]), like(operands[10]), like(operands[11]),
            like(operands[12]), like(operands[13]),
            pltpu.VMEM((4, 2 * depth, out_width), BF16),
            pltpu.VMEM((6, length, columns), F32),
            pltpu.VMEM((length, 1), F32),
            pltpu.VMEM((2, count, CHUNK, heads), F32),
            pltpu.VMEM((2, count, heads, CHUNK), F32),
            pltpu.VMEM((heads, DEPTH, 2 * DEPTH), F32),
            pltpu.VMEM((length, columns), BF16),
            pltpu.VMEM((length, columns), BF16),
            pltpu.VMEM((length, columns), F32),
            pltpu.VMEM((2, length, columns), BF16),
            pltpu.VMEM((2, length, columns), F32),
            pltpu.VMEM((length, columns), F32),
            pltpu.VMEM((heads, length, 2 * DEPTH), BF16),
            pltpu.VMEM((count, heads, DEPTH, 2 * DEPTH), F32),
            pltpu.VMEM((2, count, 1, columns), F32),
            pltpu.VMEM((count, heads, DEPTH, DEPTH), F32),
            pltpu.VMEM((count, 1, columns), F32),
            pltpu.VMEM((2, heads, DEPTH, DEPTH), F32),
            pltpu.VMEM((2, 1, columns), F32),
            pltpu.VMEM((length + 2 * RIM, columns), BF16),
            pltpu.VMEM((steps, 2, heads, DEPTH + 16, DEPTH), BF16),
            pltpu.VMEM((slots, 2, heads, DEPTH + 16, DEPTH), BF16),
            pltpu.VMEM((2, heads, DEPTH, DEPTH), F32),
            pltpu.VMEM((2, 1, columns), F32),
            pltpu.VMEM((heads, length, DEPTH), BF16),
            pltpu.VMEM((4, heads, share, DEPTH), BF16),
            pltpu.VMEM((4, share, columns), BF16),
            pltpu.VMEM((4, share, columns), BF16),
            pltpu.VMEM((share, out_width), F32),
            pltpu.VMEM((2, CHUNK, 2 * width), BF16),
            pltpu.VMEM((2, CHUNK, 1), F32),
            dma((10,)), dma((1,)), dma((1,)), dma((1,)), dma((count,)), dma((count,)),
            dma((1,)), dma((1,)), dma((events,)),
            dma((2 * steps - 1,)), dma((steps, 2, heads)), dma((2,)), dma((2,)),
            dma((1,)), dma((1,)), dma((1,)), dma((heads + 1,)),
        ],
        compiler_params=pltpu.CompilerParams(
            collective_id=0, has_side_effects=True, vmem_limit_bytes=VMEM_LIMIT
        ),
        name="mixer",
    )(*(pltpu.with_memory_space_constraint(x, pltpu.HBM) for x in operands))


def solution(mesh):
    in_specs = (
        P("sp", "tp"), P(), P(None, "tp"), P(None, "tp"), P(None, "tp"), P(None, "tp"),
        P(None, "tp"), P(None, "tp"), P(None, "tp"), P("sp", "tp"), P(None, "tp", None, None),
        P("tp"), P("tp", None, None), P("tp"), P("tp", None), P("tp", None),
    )
    out_specs = P(("sp", "tp"), None)
    return jax.shard_map(shards, mesh=mesh, in_specs=in_specs, out_specs=out_specs, check_vma=False)
```
